256 devices in a mesh: kv: 32 (over z, y), tp: 8 (over x, core).
Axes of the slice: x: 4, y: 4, z: 8, core: 2. Of those that a mesh axis runs over, the one named last changes fastest.
Arguments:
- tokens: bfloat16 [32768, 1024], P('kv', 'tp'), may hold values from -6 to 6
- query_weight: bfloat16 [1024, 2048], P(None, 'tp'), may hold values from -0.1875 to 0.1875
- latent_weight: bfloat16 [1024, 128], replicated, may hold values from -0.1875 to 0.1875
- query_gain: float32 [128], replicated, may hold values from 0.5 to 1.5
- key_gain: float32 [128], replicated, may hold values from 0.5 to 1.5
- value_up: bfloat16 [16, 128, 64], P('tp'), may hold values from -0.5 to 0.5
- out_weight: bfloat16 [1024, 1024], P('tp'), may hold values from -0.25 to 0.25
- out_gain: float32 [1024], replicated, may hold values from 0.5 to 1.5
- chosen: int32 [256, 32], P('kv'), may hold values from -1 to 255, as said below
Outputs:
- mixed_out: bfloat16 [32768, 1024], P('kv', 'tp')
The draws below stay inside these ranges and needn't reach their ends.
Inputs may be any that keep to these rules, and one draw needn't show every extreme that they name: Row b lists the key blocks chosen for query block b: entry 0 is b itself, then distinct blocks before b, then -1 in every unused place. Block j is held by index j // 8 of kv. All query blocks of one index of kv together choose at most 2 distinct blocks held by any one other index, and some pair of indices reaches that bound; blocks held by the same index are chosen freely.
All inputs are finite; a program needn't handle non-finite values.
Results may differ from the reference program's by a relative error of at most 0.02.
Values may be sent and summed in bfloat16 or wider, within the bound.
A program may use at most 64 MiB of HBM per device.

```python
import jax
import jax.numpy as jnp
from jax import lax

D = 1024
HEADS = 16
LATENT = 128
VDIM = 64
BLOCK = 128
PICKS = 32
PER_OWNER = 2
TOKENS = 32768
BLOCKS_DEV = 8
BLOCKS = 256


def draw_chosen(key, part):
    per_dev = BLOCKS_DEV
    block_count = BLOCKS
    devices = block_count // per_dev
    level_key = jax.random.fold_in(key, 11)
    order_key = jax.random.fold_in(key, 12)
    pick_key = jax.random.fold_in(key, 13)
    classes = jax.random.randint(level_key, (devices,), 0, 4)
    levels = jnp.where(classes == 0, PER_OWNER, jnp.where(classes == 1, 1, 0)).astype(jnp.int32)
    levels = jnp.minimum(levels, PER_OWNER)
    levels = levels.at[0].set(PER_OWNER)
    block_ids = jnp.arange(block_count, dtype=jnp.int32)
    owner_ids = block_ids // per_dev
    local_ids = block_ids % per_dev
    raw_order = jax.random.randint(order_key, (devices, block_count), 0, 1 << 16)
    distinct = raw_order * per_dev + local_ids[None, :]
    grouped = distinct.reshape(devices, devices, per_dev)
    ranking = jnp.argsort(jnp.argsort(grouped, axis=2), axis=2).reshape(devices, block_count)
    requester = jnp.arange(devices, dtype=jnp.int32)
    allowed = (ranking < levels[owner_ids][None, :]) & (owner_ids[None, :] < requester[:, None])
    local_before = (owner_ids[None, :] == owner_ids[:, None]) & (block_ids[None, :] < block_ids[:, None])
    candidate = allowed[owner_ids] | local_before
    raw_pick = jax.random.randint(pick_key, (block_count, block_count), 0, 1 << 16)
    scores = jnp.where(candidate, raw_pick * block_count + block_ids[None, :], -1)
    best_scores, where_best = lax.top_k(scores, PICKS - 1)
    others = jnp.where(best_scores >= 0, where_best, -1).astype(jnp.int32)
    return jnp.concatenate([block_ids[:, None], others], axis=1).astype(jnp.int32)


def with_spikes(result, rng, source, target, shards_of, factor):
    def block_of(dim):
        return (jnp.arange(result.shape[dim]) // (result.shape[dim] // shards_of)).reshape((-1,) + (1,) * (result.ndim - 1 - dim))

    one_side = jax.random.permutation(rng, shards_of)[block_of(target)]
    far = (block_of(target) + shards_of // 2) % shards_of
    return jnp.where((block_of(source) == one_side) | (block_of(source) == far), factor * result, result)


def block_scale(stream_key, dims, cuts, smallest, high):
    gain = 1.0
    for position, shards_of in cuts:
        draws = jax.random.uniform(jax.random.fold_in(jax.random.fold_in(stream_key, 6), position), (shards_of,), jnp.float32, smallest / len(cuts), high / len(cuts))
        gain = gain * jnp.repeat(jnp.exp(draws), dims[position] // shards_of).reshape((-1,) + (1,) * (len(dims) - 1 - position))
    return gain


def bell_draw(own_key, dims, width, most, shards=(), kind=jnp.bfloat16):
    array = width * jax.random.normal(own_key, dims, jnp.float32)
    if shards:
        array = array * block_scale(own_key, dims, shards, -0.22, 0.18)
    return jnp.clip(array, -most, most).astype(kind)


def bell_draw_with(key, extent, width, limit, pieces, heavy, kind=jnp.bfloat16):
    drawn = width * jax.random.normal(key, extent, jnp.float32)
    if pieces:
        drawn = drawn * block_scale(key, extent, pieces, -0.22, 0.18)
    return jnp.clip(with_spikes(drawn, jax.random.fold_in(key, 3), *heavy), -limit, limit).astype(kind)


def setup_inputs(seed: int = 0) -> dict:
    splits = jax.random.split(jax.random.key(seed), 10)
    tokens = bell_draw(splits[0], (TOKENS, D), 1.0, 6.0, ((0, 32), (1, 8)))
    query_weight = bell_draw(splits[1], (D, HEADS * LATENT), D ** -0.5, 0.1875, ((1, 8),))
    latent_weight = bell_draw(splits[2], (D, LATENT), D ** -0.5, 0.1875)
    query_gain = jnp.clip(1.0 + 0.1 * jax.random.normal(splits[3], (LATENT,), jnp.float32), 0.5, 1.5)
    key_gain = jnp.clip(1.0 + 0.1 * jax.random.normal(splits[4], (LATENT,), jnp.float32), 0.5, 1.5)
    value_up = bell_draw(splits[5], (HEADS, LATENT, VDIM), LATENT ** -0.5, 0.5, ((0, 8),))
    out_weight = bell_draw_with(splits[6], (HEADS * VDIM, D), (HEADS * VDIM) ** -0.5, 0.25, ((0, 8),), (0, 1, 8, 2.0))
    out_gain = jnp.clip(1.0 + 0.1 * jax.random.normal(splits[7], (D,), jnp.float32), 0.5, 1.5)
    chosen = draw_chosen(jax.random.fold_in(splits[9], 71), 0)
    return {"tokens": tokens, "query_weight": query_weight, "latent_weight": latent_weight, "query_gain": query_gain, "key_gain": key_gain, "value_up": value_up, "out_weight": out_weight, "out_gain": out_gain, "chosen": chosen}


epsilon = 1e-06
masked_score = -1e+30

def rms_scale(values, gain_row):
    widened = values.astype(jnp.float32)
    mean_sq = lax.optimization_barrier(jnp.mean(widened * widened, axis=-1, keepdims=True))
    return (widened * lax.rsqrt(mean_sq + epsilon) * gain_row).astype(jnp.bfloat16)

def reference(tokens, query_weight, latent_weight, query_gain, key_gain, value_up, out_weight, out_gain, chosen):
    queries = jnp.dot(tokens, query_weight, preferred_element_type=jnp.float32).astype(jnp.bfloat16)
    queries = rms_scale(queries.reshape(TOKENS, HEADS, LATENT), query_gain)
    latent = jnp.dot(tokens, latent_weight, preferred_element_type=jnp.float32).astype(jnp.bfloat16)
    normed_keys = rms_scale(latent, key_gain)
    key_blocks = normed_keys.reshape(BLOCKS, BLOCK, LATENT)
    value_blocks = latent.reshape(BLOCKS, BLOCK, LATENT)
    query_blocks = queries.reshape(BLOCKS, BLOCK, HEADS, LATENT)
    offsets = jnp.arange(BLOCK, dtype=jnp.int32)

    def attend(packed):
        query_block, chosen_row, start_pos = packed
        clamped = jnp.maximum(chosen_row, 0).astype(jnp.int32)
        picked_keys = key_blocks[clamped].astype(jnp.float32)
        picked_values = value_blocks[clamped].astype(jnp.float32)
        scores = jnp.einsum('qhl,ckl->qhck', query_block.astype(jnp.float32), picked_keys) * LATENT ** (-0.5)
        key_pos = clamped[:, None] * BLOCK + offsets[None, :]
        query_pos = start_pos + offsets
        allowed = (chosen_row[:, None] >= 0)[None] & (key_pos[None] <= query_pos[:, None, None])
        allowed = allowed[:, None]
        scores = jnp.where(allowed, scores, masked_score)
        row_max = lax.optimization_barrier(jnp.max(scores, axis=(2, 3), keepdims=True))
        exp_scores = jnp.where(allowed, jnp.exp(scores - row_max), 0.0)
        weights = (exp_scores / lax.optimization_barrier(jnp.sum(exp_scores, axis=(2, 3), keepdims=True))).astype(jnp.bfloat16)
        attended = jnp.einsum('qhck,ckl->qhl', weights.astype(jnp.float32), picked_values)
        return attended.astype(jnp.bfloat16)
    block_starts = jnp.arange(BLOCKS, dtype=jnp.int32) * BLOCK
    attended = lax.map(attend, (query_blocks, chosen, block_starts))
    attended = attended.reshape(TOKENS, HEADS, LATENT)
    heads_out = jnp.einsum('thl,hlv->thv', attended.astype(jnp.float32), value_up.astype(jnp.float32))
    heads_out = heads_out.astype(jnp.bfloat16).reshape(TOKENS, HEADS * VDIM)
    projected = jnp.dot(heads_out, out_weight, preferred_element_type=jnp.float32)
    return rms_scale(projected, out_gain)
```

```python
import functools

import jax
import jax.numpy as jnp
from jax import lax
from jax.experimental import pallas as pl
from jax.experimental.pallas import tpu as pltpu
from jax.sharding import PartitionSpec as P

BLOCK = 128
PER_OWNER = 2
CHUNKS = 4
GROUP = 1
STEP = 8
LANES = 128
ONES = 16
MESH = pl.DeviceIdType.MESH

epsilon = 1e-06
masked_score = -1e30


def rms_scale(values, gain_row):
    widened = values.astype(jnp.float32)
    mean_sq = jnp.mean(widened * widened, axis=-1, keepdims=True)
    return (widened * lax.rsqrt(mean_sq + epsilon) * gain_row).astype(jnp.bfloat16)


def prefix_in_owner(values, lane, blocks, inclusive):
    total = values if inclusive else jnp.zeros_like(values)
    for s in range(1, blocks):
        total = total + jnp.where(lane % blocks >= s, pltpu.roll(values, s, 1), 0)
    return total


def send(src, dst, sems, where):
    return pltpu.make_async_remote_copy(
        src_ref=src, dst_ref=dst, send_sem=sems[0], recv_sem=sems[1], device_id=where, device_id_type=MESH
    )


def kernel(
    kv_n, tp_n,
    tok_ref, wq_ref, wl_ref, qgain_ref, kgain_ref, vu_ref, w_ref, ogain_ref, chosen_ref, chosen_s,
    o_ref,
    tk_ref, q_ref, own_ref, pool_ref, out_ref, kn_ref, vt_ref, bd_ref,
    map_ref, req_ref, chs_ref, map_s, chs_s,
    ho_ref, wc_ref, proj_ref, ss_ref, rs_ref,
    lc, ch_s, ch_r, ts_s, ts_r, tx_s, tx_r, tr_s, tr_r, b_s, b_r, f_s, f_r,
    hs_s, hs_r, hx_s, hx_r, hr_s, hr_r, w_s, w_r, s_s, s_r,
):
    kv, tp = lax.axis_index("kv"), lax.axis_index("tp")
    core = lax.rem(tp, 2)
    sib = tp + 1 - 2 * core
    far = tp_n // 2 - 1
    toks, feat = tok_ref.shape
    width = wl_ref.shape[1]
    heads = wq_ref.shape[1] // width
    vdim = vu_ref.shape[1]
    blocks = toks // BLOCK
    slots = blocks + pool_ref.shape[0]
    picks = chosen_ref.shape[1]
    cols = o_ref.shape[1]
    crows = toks // CHUNKS
    per_row = LANES // blocks

    def at_kv(other):
        return {"kv": other, "tp": tp}

    def at_tp(other):
        return {"kv": kv, "tp": other}

    def across(i, sign):
        return lax.rem(tp + sign * 2 * (i + 1) + tp_n, tp_n)

    barrier = pltpu.get_barrier_semaphore()
    for d in range(1, kv_n):
        pl.semaphore_signal(barrier, inc=1, device_id=at_kv(lax.rem(kv + d, kv_n)), device_id_type=MESH)
    for d in range(1, tp_n):
        pl.semaphore_signal(barrier, inc=1, device_id=at_tp(lax.rem(tp + d, tp_n)), device_id_type=MESH)

    lane = lax.broadcasted_iota(jnp.int32, (blocks, LANES), 1)
    halves = map_ref.shape[0]
    table = chosen_ref[...]
    for g in range(halves):
        hit = jnp.zeros((blocks, LANES), jnp.int32)
        for c in range(picks):
            hit = jnp.where(table[:, c : c + 1] == lane + g * LANES, 1, hit)
        need = jnp.broadcast_to(jnp.max(hit, axis=0, keepdims=True), (blocks, LANES))
        rank = prefix_in_owner(need, lane, blocks, False)
        local = lane % blocks
        dist = kv - (lane // blocks + g * per_row)
        slot = jnp.where(dist == 0, local, blocks + (dist - 1) * PER_OWNER + rank)
        map_ref[g] = jnp.clip(slot, 0, slots - 1)[0:1]
        code = jnp.zeros((blocks, LANES), jnp.int32)
        for k in range(PER_OWNER):
            code = code + jnp.where((need > 0) & (rank == k), local * blocks**k, 0)
        req_ref[g] = prefix_in_owner(code, lane, blocks, True)[0:1]

    pltpu.make_async_copy(map_ref, map_s, lc.at[0]).start()
    pl.semaphore_wait(barrier, kv_n - 1 + tp_n - 1)

    def rows_of(c, n):
        return pl.ds(pl.multiple_of(c * n, n), n)

    def to_sib(src, buf, c, n, sems):
        return send(src.at[rows_of(c, n)], buf.at[tp, rows_of(c, n)], [s.at[c] for s in sems], at_tp(sib))

    def to_far(src, buf, c, n, i, sems):
        return send(
            src.at[rows_of(c, n)], buf.at[tp, rows_of(c, n)], [s.at[i, c] for s in sems], at_tp(across(i, 1))
        )

    def relay(buf, c, n, i, sems):
        part = buf.at[across(i, -1), rows_of(c, n)]
        return send(part, part, [s.at[i, c] for s in sems], at_tp(sib))

    def from_far(buf, c, n, i, sems):
        part = buf.at[across(i, -1), rows_of(c, n)]
        return send(part, part, [s.at[i, c] for s in sems], at_tp(sib))

    for c in range(CHUNKS):
        for i in range(far):
            to_far(tok_ref, tk_ref, c, crows, i, (tx_s, tx_r)).start()
        to_sib(tok_ref, tk_ref, c, crows, (ts_s, ts_r)).start()

    def ask(d):
        owner = kv - d
        return send(
            req_ref.at[jnp.maximum(owner, 0) // per_row], chs_ref.at[d - 1],
            (ch_s.at[d - 1], ch_r.at[d - 1]), at_kv(lax.rem(owner + kv_n, kv_n)),
        )

    def asks(d):
        return kv - d >= 0

    def serves(d):
        return kv + d < kv_n

    for d in range(1, kv_n):

        @pl.when(asks(d))
        def _(d=d):
            ask(d).start()

    tk_ref[tp] = tok_ref[...]
    null = slots
    kn_ref[null] = jnp.zeros((BLOCK, width), jnp.bfloat16)
    vt_ref[null] = jnp.zeros((width + ONES, BLOCK), jnp.bfloat16)
    bd_ref[...] = jnp.zeros_like(bd_ref)
    for h in range(heads):
        bd_ref[h // 2, (h % 2) * vdim : (h % 2 + 1) * vdim, (h % 2) * width : (h % 2 + 1) * width] = vu_ref[h]

    gain = qgain_ref[...] * (width**-0.5 * 1.4426950408889634)

    def project(c):
        rows = slice(c * crows, (c + 1) * crows)
        x = jnp.concatenate([tk_ref[t, rows, :] for t in range(tp_n)], axis=1)
        lat = jnp.dot(x, wl_ref[...], preferred_element_type=jnp.float32).astype(jnp.bfloat16)
        for j in range(crows // BLOCK):
            own_ref[c * (crows // BLOCK) + j] = lat[j * BLOCK : (j + 1) * BLOCK]
        qs = jnp.dot(x, wq_ref[...], preferred_element_type=jnp.float32).astype(jnp.bfloat16)
        for h in range(heads):
            hc = slice(h * width, (h + 1) * width)
            q_ref[rows, hc] = rms_scale(qs[:, hc], gain)

    def arrive(c):
        to_sib(tok_ref, tk_ref, c, crows, (ts_s, ts_r)).wait()
        for i in range(far):
            relay(tk_ref, c, crows, i, (tr_s, tr_r)).wait()
            to_far(tok_ref, tk_ref, c, crows, i, (tx_s, tx_r)).wait_send()
        project(c)

    for c in range(CHUNKS):
        for i in range(far):
            from_far(tk_ref, c, crows, i, (tx_s, tx_r)).wait_recv()
            relay(tk_ref, c, crows, i, (tr_s, tr_r)).start()
        if c:
            arrive(c - 1)

    for d in range(1, kv_n):

        @pl.when(asks(d))
        def _(d=d):
            ask(d).wait_send()

        @pl.when(serves(d))
        def _(d=d):
            ask(d).wait_recv()

    pltpu.make_async_copy(map_ref, map_s, lc.at[0]).wait()
    to_smem = pltpu.make_async_copy(chs_ref, chs_s, lc.at[1])
    to_smem.start()
    arrive(CHUNKS - 1)
    to_smem.wait()

    def weight(d):
        other = lax.rem(tp + d, tp_n)
        part = w_ref.at[:, pl.ds(pl.multiple_of(other * cols, cols), cols)]
        return send(part, wc_ref.at[tp], (w_s.at[d - 1], w_r.at[d - 1]), at_tp(other))

    def slot_of(d, c):
        return (d - 1) * PER_OWNER + c

    def give(d):
        return send(
            out_ref.at[d - 1], pool_ref.at[slot_of(d, core)], (b_s.at[d - 1], b_r.at[d - 1]), at_kv(lax.rem(kv + d, kv_n))
        )

    def forward(d):
        part = pool_ref.at[slot_of(d, core)]
        return send(part, part, (f_s.at[d - 1], f_r.at[d - 1]), at_tp(sib))

    mine = lax.rem(kv, per_row) * blocks + blocks - 1
    for d in range(1, kv_n):

        @pl.when(serves(d))
        def _(d=d):
            code = chs_s[d - 1, 0, mine]
            want = jnp.where(core == 0, code, code >> 3) & (blocks - 1)
            out_ref[d - 1] = own_ref[want]
            give(d).start()

    for d in range(1, tp_n):
        weight(d).start()

    def norm(lat, slot):
        kn_ref[slot] = rms_scale(lat, kgain_ref[...])
        vt_ref[slot, 0:width, :] = lat.T
        vt_ref[slot, width:, :] = jnp.ones((ONES, BLOCK), jnp.bfloat16)

    @pl.loop(0, blocks)
    def _(b):
        norm(own_ref[b], b)

    wc_ref[tp] = w_ref[:, pl.ds(pl.multiple_of(tp * cols, cols), cols)]

    for d in range(1, kv_n):

        @pl.when(asks(d))
        def _(d=d):
            give(d).wait_recv()
            forward(d).start()

    for d in range(1, kv_n):

        @pl.when(asks(d))
        def _(d=d):
            forward(d).wait()
            for k in range(PER_OWNER):
                norm(pool_ref[slot_of(d, k)], blocks + slot_of(d, k))

    for d in range(1, kv_n):

        @pl.when(serves(d))
        def _(d=d):
            give(d).wait_send()

    def hand_on(b):
        for i in range(far):
            from_far(ho_ref, b, BLOCK, i, (hx_s, hx_r)).wait_recv()
            relay(ho_ref, b, BLOCK, i, (hr_s, hr_r)).start()

    def listed(b, c):
        block = chosen_s[b, c]
        known = jnp.maximum(block, 0)
        return jnp.where(block < 0, null, map_s[known >> 7, 0, known & (LANES - 1)])

    def attend_block(b):
        rows = rows_of(b, BLOCK)
        q = jnp.concatenate([q_ref[rows, h * width : (h + 1) * width] for h in range(heads)], axis=0)
        qt = q.T
        acc = jnp.zeros((width + ONES, heads * BLOCK), jnp.float32)
        for i in range(0, picks, STEP):
            at = [listed(b, i + k) for k in range(STEP)]
            keys = jnp.concatenate([kn_ref[s] for s in at], axis=0)
            s = jnp.dot(keys, qt, preferred_element_type=jnp.float32)
            if i == 0:
                key_row = lax.broadcasted_iota(jnp.int32, s.shape, 0)
                query_row = lax.broadcasted_iota(jnp.int32, s.shape, 1) % BLOCK
                s = jnp.where((key_row <= query_row) | (key_row >= BLOCK), s, masked_score)
            p = jnp.exp2(s).astype(jnp.bfloat16)
            values = jnp.concatenate([vt_ref[s] for s in at], axis=1)
            acc = acc + jnp.dot(values, p, preferred_element_type=jnp.float32)
        att = (acc[:width] / acc[width : width + 1]).astype(jnp.bfloat16).T
        out = []
        for h in range(0, heads, 2):
            two = jnp.concatenate([att[h * BLOCK : (h + 1) * BLOCK], att[(h + 1) * BLOCK : (h + 2) * BLOCK]], axis=1)
            out.append(
                lax.dot_general(two, bd_ref[h // 2], (((1,), (1,)), ((), ())), preferred_element_type=jnp.float32)
            )
        return jnp.concatenate(out, axis=1).astype(jnp.bfloat16)

    @pl.loop(0, blocks // GROUP)
    def _(g):
        done = [attend_block(g * GROUP + u) for u in range(GROUP)]
        for u in range(GROUP):
            b = g * GROUP + u
            ho_ref[tp, rows_of(b, BLOCK), :] = done[u]
            for i in range(far):
                to_far(ho_ref.at[tp], ho_ref, b, BLOCK, i, (hx_s, hx_r)).start()
            to_sib(ho_ref.at[tp], ho_ref, b, BLOCK, (hs_s, hs_r)).start()

        @pl.when(g >= 1)
        def _():
            for u in range(GROUP):
                hand_on((g - 1) * GROUP + u)

    for d in range(1, tp_n):
        weight(d).wait()

    def finish(b):
        rows = rows_of(b, BLOCK)
        to_sib(ho_ref.at[tp], ho_ref, b, BLOCK, (hs_s, hs_r)).wait()
        for i in range(far):
            to_far(ho_ref.at[tp], ho_ref, b, BLOCK, i, (hx_s, hx_r)).wait_send()
            relay(ho_ref, b, BLOCK, i, (hr_s, hr_r)).wait()
        total = jnp.zeros((BLOCK, cols), jnp.float32)
        for t in range(tp_n):
            total = total + jnp.dot(ho_ref[t, rows, :], wc_ref[t], preferred_element_type=jnp.float32)
        proj_ref[rows, :] = total
        squares = jnp.sum(total * total, axis=1, keepdims=True)
        ss_ref[tp, pl.ds(b, 1), :] = jnp.broadcast_to(squares, (BLOCK, BLOCK)).T[0:1]

    for b in range(blocks - GROUP, blocks):
        hand_on(b)
    pl.loop(0, blocks)(finish)

    def sums(d):
        return send(ss_ref.at[tp], ss_ref.at[tp], (s_s.at[d - 1], s_r.at[d - 1]), at_tp(lax.rem(tp + d, tp_n)))

    for d in range(1, tp_n):
        sums(d).start()
    for d in range(1, tp_n):
        sums(d).wait()
    total = ss_ref[0]
    for t in range(1, tp_n):
        total = total + ss_ref[t]
    rs_ref[...] = lax.rsqrt(total / (cols * tp_n) + epsilon)
    gains = ogain_ref[:, pl.ds(pl.multiple_of(tp * cols, cols), cols)]

    @pl.loop(0, blocks)
    def _(b):
        rows = rows_of(b, BLOCK)
        scale = jnp.broadcast_to(rs_ref[pl.ds(b, 1), :], (BLOCK, BLOCK)).T
        scale = jnp.concatenate([scale] * (cols // BLOCK), axis=1)
        o_ref[rows, :] = (proj_ref[rows, :] * scale * gains).astype(jnp.bfloat16)


def on_device(
    tokens,
    query_weight,
    latent_weight,
    query_gain,
    key_gain,
    value_up,
    out_weight,
    out_gain,
    chosen,
):
    toks, feat = tokens.shape
    width = latent_weight.shape[1]
    heads = query_weight.shape[1] // width
    blocks = toks // BLOCK
    kv_n, tp_n = lax.axis_size("kv"), lax.axis_size("tp")
    cols = out_weight.shape[1] // tp_n
    hv = out_weight.shape[0]
    far = tp_n // 2 - 1
    slots = blocks + (kv_n - 1) * PER_OWNER
    halves = kv_n * blocks // LANES
    bf, f32, i32 = jnp.bfloat16, jnp.float32, jnp.int32
    dma = pltpu.SemaphoreType.DMA
    kvs, tps = [dma((kv_n - 1,))] * 2, [dma((tp_n - 1,))] * 2
    cs, cf = [dma((CHUNKS,))] * 2, [dma((far, CHUNKS))] * 2
    bs, bfar = [dma((blocks,))] * 2, [dma((far, blocks))] * 2
    vmem = pl.BlockSpec(memory_space=pltpu.VMEM)
    return pl.pallas_call(
        functools.partial(kernel, kv_n, tp_n),
        out_shape=jax.ShapeDtypeStruct((toks, cols), bf),
        in_specs=[vmem] * 9 + [pl.BlockSpec(memory_space=pltpu.SMEM)],
        out_specs=vmem,
        scratch_shapes=[
            pltpu.VMEM((tp_n, toks, feat), bf),
            pltpu.VMEM((toks, heads * width), bf),
            pltpu.VMEM((blocks, BLOCK, width), bf),
            pltpu.VMEM((slots - blocks, BLOCK, width), bf),
            pltpu.VMEM((kv_n - 1, BLOCK, width), bf),
            pltpu.VMEM((slots + 1, BLOCK, width), bf),
            pltpu.VMEM((slots + 1, width + ONES, BLOCK), bf),
            pltpu.VMEM((heads // 2, 2 * hv // heads, 2 * width), bf),
            pltpu.VMEM((halves, 1, LANES), i32),
            pltpu.VMEM((halves, 1, LANES), i32),
            pltpu.VMEM((kv_n - 1, 1, LANES), i32),
            pltpu.SMEM((halves, 1, LANES), i32),
            pltpu.SMEM((kv_n - 1, 1, LANES), i32),
            pltpu.VMEM((tp_n, toks, hv), bf),
            pltpu.VMEM((tp_n, hv, cols), bf),
            pltpu.VMEM((toks, cols), f32),
            pltpu.VMEM((tp_n, blocks, BLOCK), f32),
            pltpu.VMEM((blocks, BLOCK), f32),
            dma((2,)), *kvs, *cs, *cf, *cf, *kvs, *kvs, *bs, *bfar, *bfar, *tps, *tps,
        ],
        compiler_params=pltpu.CompilerParams(
            collective_id=0, has_side_effects=True, vmem_limit_bytes=60 << 20
        ),
    )(
        tokens, query_weight, latent_weight, query_gain[None, :], key_gain[None, :],
        jnp.swapaxes(value_up, 1, 2), out_weight, out_gain[None, :], chosen, chosen,
    )


def solution(mesh):
    in_specs = (
        P("kv", "tp"),
        P(None, "tp"),
        P(),
        P(),
        P(),
        P("tp", None, None),
        P("tp", None),
        P(),
        P("kv", None),
    )
    out_specs = P("kv", "tp")
    return jax.shard_map(
        on_device, mesh=mesh, in_specs=in_specs, out_specs=out_specs, check_vma=False
    )
```

```python
import functools

import jax
import jax.numpy as jnp
from jax import lax
from jax.experimental import pallas as pl
from jax.experimental.pallas import tpu as pltpu
from jax.sharding import PartitionSpec as P

BLOCK = 128
PER_OWNER = 2
RING = 4
OWNERS = 8
STEP = 8
LANES = 128
ONES = 16
MESH = pl.DeviceIdType.MESH

epsilon = 1e-06
masked_score = -1e30


def rms_scale(values, gain_row):
    widened = values.astype(jnp.float32)
    mean_sq = jnp.mean(widened * widened, axis=-1, keepdims=True)
    return (widened * lax.rsqrt(mean_sq + epsilon) * gain_row).astype(jnp.bfloat16)


def prefix_in_owner(values, lane, blocks, inclusive):
    total = values if inclusive else jnp.zeros_like(values)
    for s in range(1, blocks):
        total = total + jnp.where(lane % blocks >= s, pltpu.roll(values, s, 1), 0)
    return total


def send(src, dst, sems, where):
    return pltpu.make_async_remote_copy(
        src_ref=src, dst_ref=dst, send_sem=sems[0], recv_sem=sems[1], device_id=where, device_id_type=MESH
    )


def owner_groups(kv_n):
    return [(d, min(d + OWNERS, kv_n)) for d in range(1, kv_n, OWNERS)]


def kernel(
    kv_n, tp_n,
    tok_ref, wq_ref, wl_ref, qgain_ref, kgain_ref, vu_ref, w_ref, ogain_ref, chosen_ref, chosen_s,
    o_ref,
    tk_ref, wqs_ref, vus_ref, q_ref, lat_ref, out_ref, kvp_ref, kn_ref, vt_ref, bd_ref,
    map_ref, req_ref, chs_ref, map_s, chs_s,
    ho_ref, wc_ref, proj_ref, px_ref, ss_ref,
    lc, t_s, t_r, c_s, c_r, ch_s, ch_r, b_s, b_r, k_s, k_r, kr_s, kr_r,
    w_s, w_r, y_s, y_r, h_s, h_r, p_s, p_r, s_s, s_r,
):
    kv, tp = lax.axis_index("kv"), lax.axis_index("tp")
    core, x = lax.rem(tp, 2), tp // 2
    sib = tp + 1 - 2 * core
    blocks, _, xs, piece, feat = tok_ref.shape
    far = xs - 1
    width = wl_ref.shape[1]
    heads = wq_ref.shape[1] // width
    vdim = vu_ref.shape[1]
    slots = kvp_ref.shape[1]
    picks = chosen_ref.shape[1]
    cols = o_ref.shape[1]
    half = BLOCK // 2
    mine = blocks * piece
    per_row = LANES // blocks
    wrows = w_ref.shape[0] // RING
    y = lax.rem(kv, RING)

    def at_kv(other):
        return {"kv": other, "tp": tp}

    def at_tp(other):
        return {"kv": kv, "tp": other}

    def other_tp(d):
        return lax.rem(tp + d + tp_n, tp_n)

    barrier = pltpu.get_barrier_semaphore()
    for d in range(1, kv_n):
        pl.semaphore_signal(barrier, inc=1, device_id=at_kv(lax.rem(kv + d, kv_n)), device_id_type=MESH)
    for d in range(1, tp_n):
        pl.semaphore_signal(barrier, inc=1, device_id=at_tp(other_tp(d)), device_id_type=MESH)

    lane = lax.broadcasted_iota(jnp.int32, (blocks, LANES), 1)
    halves = map_ref.shape[0]
    table = chosen_ref[...]
    for g in range(halves):
        hit = jnp.zeros((blocks, LANES), jnp.int32)
        for c in range(picks):
            hit = jnp.where(table[:, c : c + 1] == lane + g * LANES, 1, hit)
        need = jnp.broadcast_to(jnp.max(hit, axis=0, keepdims=True), (blocks, LANES))
        rank = prefix_in_owner(need, lane, blocks, False)
        local = lane % blocks
        dist = kv - (lane // blocks + g * per_row)
        slot = jnp.where(dist == 0, local, blocks + (dist - 1) * PER_OWNER + rank)
        map_ref[g] = jnp.clip(slot, 0, slots - 1)[0:1]
        code = jnp.zeros((blocks, LANES), jnp.int32)
        for k in range(PER_OWNER):
            code = code + jnp.where((need > 0) & (rank == k), local * blocks**k, 0)
        req_ref[g] = prefix_in_owner(code, lane, blocks, True)[0:1]

    pltpu.make_async_copy(map_ref, map_s, lc.at[0]).start()
    pl.semaphore_wait(barrier, kv_n - 1 + tp_n - 1)

    def tokens_to(d, j):
        other = other_tp(d)
        part = lax.rem(other // 2 + j, xs)
        return send(
            tok_ref.at[:, lax.rem(other, 2), part], tk_ref.at[tp, part], (t_s.at[j, d - 1], t_r.at[j, d - 1]), at_tp(other)
        )

    def ask(d):
        owner = kv - d
        return send(
            req_ref.at[jnp.maximum(owner, 0) // per_row], chs_ref.at[d - 1],
            (ch_s.at[d - 1], ch_r.at[d - 1]), at_kv(lax.rem(owner + kv_n, kv_n)),
        )

    def asks(d):
        return kv - d >= 0

    def serves(d):
        return kv + d < kv_n

    def weights_to(d):
        other = other_tp(d)
        part = w_ref.at[
            pl.ds(pl.multiple_of(y * wrows, wrows), wrows),
            pl.ds(pl.multiple_of(other // 2 * 2 * cols, 2 * cols), 2 * cols),
        ]
        return send(part, wc_ref.at[tp, y], (w_s.at[d - 1], w_r.at[d - 1]), at_tp(other))

    def weights_on(e):
        part = wc_ref.at[:, y]
        other = kv - y + lax.rem(y + e, RING)
        return send(part, part, (y_s.at[e - 1], y_r.at[e - 1]), at_kv(other))

    to_sib = [
        send(wq_ref, wqs_ref, (c_s.at[0], c_r.at[0]), at_tp(sib)),
        send(vu_ref, vus_ref, (c_s.at[1], c_r.at[1]), at_tp(sib)),
    ]

    for d in range(1, tp_n):
        tokens_to(d, 0).start()
    for d in range(1, kv_n):

        @pl.when(asks(d))
        def _(d=d):
            ask(d).start()

    for j in range(1, xs):
        for d in range(1, tp_n):
            tokens_to(d, j).start()
    for copy in to_sib:
        copy.start()
    for d in range(1, tp_n):
        weights_to(d).start()

    for p in range(xs):
        tk_ref[tp, p] = tok_ref[:, core, p]
    wc_ref[tp, y] = w_ref[
        pl.ds(pl.multiple_of(y * wrows, wrows), wrows), pl.ds(pl.multiple_of(x * 2 * cols, 2 * cols), 2 * cols)
    ]
    null = slots
    kn_ref[null] = jnp.zeros((BLOCK, width), jnp.bfloat16)
    vt_ref[null] = jnp.zeros((width + ONES, BLOCK), jnp.bfloat16)
    bd_ref[...] = jnp.zeros_like(bd_ref)

    def features(p):
        return jnp.concatenate([tk_ref[t, p].reshape(mine, feat) for t in range(tp_n)], axis=1)

    for d in range(1, tp_n):
        tokens_to(d, 0).wait_recv()
    lat = jnp.dot(features(x), wl_ref[...], preferred_element_type=jnp.float32).astype(jnp.bfloat16)
    lat_ref[...] = lat.reshape(blocks, piece, width)
    kvp_ref[tp, 0:blocks] = lat.reshape(blocks, piece, width)

    for d in range(1, kv_n):

        @pl.when(asks(d))
        def _(d=d):
            ask(d).wait_send()

        @pl.when(serves(d))
        def _(d=d):
            ask(d).wait_recv()

    to_smem = pltpu.make_async_copy(chs_ref, chs_s, lc.at[1])
    to_smem.start()
    pltpu.make_async_copy(map_ref, map_s, lc.at[0]).wait()
    to_smem.wait()

    def slots_of(d):
        return pl.ds(blocks + (d - 1) * PER_OWNER, PER_OWNER)

    def give(d):
        return send(
            out_ref.at[d - 1], kvp_ref.at[tp, slots_of(d)], (b_s.at[d - 1], b_r.at[d - 1]), at_kv(lax.rem(kv + d, kv_n))
        )

    at_lane = lax.rem(kv, per_row) * blocks + blocks - 1
    for d in range(1, kv_n):

        @pl.when(serves(d))
        def _(d=d):
            code = chs_s[d - 1, 0, at_lane]
            for k in range(PER_OWNER):
                out_ref[d - 1, k] = lat_ref[(code >> (3 * k)) & (blocks - 1)]
            give(d).start()

    remote = owner_groups(kv_n)
    groups = [(0, blocks)] + [
        (blocks + (a - 1) * PER_OWNER, (b - a) * PER_OWNER) for a, b in remote
    ]

    def spread(g, i):
        part = kvp_ref.at[tp, pl.ds(*groups[g])]
        where = sib if i == far else other_tp(2 * (i + 1))
        return send(part, part, (k_s.at[g, i], k_r.at[g, i]), at_tp(where))

    def relay(g, i):
        part = kvp_ref.at[other_tp(-2 * (i + 1)), pl.ds(*groups[g])]
        return send(part, part, (kr_s.at[g, i], kr_r.at[g, i]), at_tp(sib))

    def when_group(g, body):
        if g == 0:
            body()
        else:
            pl.when(kv >= remote[g - 1][0])(body)

    def spread_group(g):
        def body():
            if g:
                for d in range(*remote[g - 1]):

                    @pl.when(asks(d))
                    def _(d=d):
                        give(d).wait_recv()

            for i in range(far + 1):
                spread(g, i).start()

        when_group(g, body)

    def relay_group(g):
        def body():
            for i in range(far):
                spread(g, i).wait_recv()
                relay(g, i).start()

        when_group(g, body)

    gain_k = kgain_ref[...]

    def norm_group(g):
        def body():
            spread(g, far).wait_recv()
            for i in range(far):
                relay(g, i).wait_recv()

            @pl.loop(groups[g][0], groups[g][0] + groups[g][1])
            def _(slot):
                rows = jnp.concatenate(
                    [kvp_ref[p * 2 + c, slot] for c in range(2) for p in range(xs)], axis=0
                )
                kn_ref[slot] = rms_scale(rows, gain_k)
                vt_ref[slot, 0:width, :] = rows.T
                vt_ref[slot, width:, :] = jnp.ones((ONES, BLOCK), jnp.bfloat16)

        when_group(g, body)

    gain_q = qgain_ref[...] * (width**-0.5 * 1.4426950408889634)

    def project(j):
        for d in range(1, tp_n):
            if j:
                tokens_to(d, j).wait_recv()
        p = lax.rem(x + j, xs)
        rows = features(p)
        for w, at in ((wq_ref, core), (wqs_ref, 1 - core)):
            qs = jnp.dot(rows, w[...], preferred_element_type=jnp.float32).astype(jnp.bfloat16)
            for h in range(heads):
                part = rms_scale(qs[:, h * width : (h + 1) * width], gain_q)
                q_ref[at * heads + h, p] = part.reshape(blocks, piece, width)

    spread_group(0)
    for copy in to_sib:
        copy.wait()
    for v, at in ((vu_ref, core), (vus_ref, 1 - core)):
        for h in range(heads):
            bd_ref[at, h * vdim : (h + 1) * vdim, h * width : (h + 1) * width] = v[h]
    project(0)
    count = len(groups)
    for g in range(1, count):
        spread_group(g)
        relay_group(g - 1)
        if g < xs:
            project(g)
        if g >= 2:
            norm_group(g - 2)
    for j in range(count, xs):
        project(j)
    for d in range(1, tp_n):
        weights_to(d).wait_recv()
    for e in range(1, RING):
        weights_on(e).start()
    relay_group(count - 1)
    if count >= 2:
        norm_group(count - 2)
    norm_group(count - 1)

    def listed(b, c):
        block = chosen_s[b, c]
        known = jnp.maximum(block, 0)
        return jnp.where(block < 0, null, map_s[known >> 7, 0, known & (LANES - 1)])

    def attend_block(b):
        q = jnp.concatenate([q_ref[h, p, b] for h in range(2 * heads) for p in range(xs)], axis=0)
        qt = q.T
        acc = jnp.zeros((width + ONES, 2 * heads * half), jnp.float32)
        for i in range(0, picks, STEP):
            at = [listed(b, i + k) for k in range(STEP)]
            keys = jnp.concatenate([kn_ref[s] for s in at], axis=0)
            s = jnp.dot(keys, qt, preferred_element_type=jnp.float32)
            if i == 0:
                key_row = lax.broadcasted_iota(jnp.int32, s.shape, 0)
                query_row = lax.broadcasted_iota(jnp.int32, s.shape, 1) % half + core * half
                s = jnp.where((key_row <= query_row) | (key_row >= BLOCK), s, masked_score)
            p = jnp.exp2(s).astype(jnp.bfloat16)
            values = jnp.concatenate([vt_ref[s] for s in at], axis=1)
            acc = acc + jnp.dot(values, p, preferred_element_type=jnp.float32)
        att = (acc[:width] / acc[width : width + 1]).astype(jnp.bfloat16).T
        out = []
        for h in range(0, 2 * heads, 2):
            two = jnp.concatenate([att[h * half : (h + 1) * half], att[(h + 1) * half : (h + 2) * half]], axis=1)
            out.append(
                lax.dot_general(two, bd_ref[h // 2], (((1,), (1,)), ((), ())), preferred_element_type=jnp.float32)
            )
        return jnp.concatenate(out, axis=1).astype(jnp.bfloat16)

    def heads_to(b, i):
        part = ho_ref.at[x, b]
        return send(part, part, (h_s.at[b, i], h_r.at[b, i]), at_tp(other_tp(2 * (i + 1))))

    def finish(g):
        for u in range(2):
            for i in range(far):
                heads_to(2 * g + u, i).wait_recv()
        total = jnp.zeros((BLOCK, 2 * cols), jnp.float32)
        for p in range(xs):
            rows = ho_ref[p, pl.ds(2 * g, 2)].reshape(BLOCK, 2 * cols)
            w = jnp.concatenate([wc_ref[2 * p + c].reshape(RING * wrows, 2 * cols) for c in range(2)], axis=0)
            total = total + jnp.dot(rows, w, preferred_element_type=jnp.float32)
        left, right = total[:, :cols], total[:, cols:]
        px_ref[g] = jnp.where(core == 0, right, left)
        proj_ref[g, core] = jnp.where(core == 0, left, right)
        squares = jnp.sum(total * total, axis=1, keepdims=True)
        ss_ref[tp, pl.ds(g, 1), :] = jnp.broadcast_to(squares, (BLOCK, BLOCK)).T[0:1]
        swap(g).start()

    def swap(g):
        return send(px_ref.at[g], proj_ref.at[g, core], (p_s.at[g], p_r.at[g]), at_tp(sib))

    pairs = blocks // 2
    for e in range(1, RING):
        weights_on(e).wait_recv()

    @pl.loop(0, blocks)
    def _(b):
        ho_ref[x, b] = attend_block(b)
        for i in range(far):
            heads_to(b, i).start()

        @pl.when((b >= 5) & (lax.rem(b, 2) == 1))
        def _():
            finish((b - 5) // 2)

    for g in range(max(pairs - 2, 0), pairs):
        finish(g)

    def sums(d):
        return send(ss_ref.at[tp], ss_ref.at[tp], (s_s.at[d - 1], s_r.at[d - 1]), at_tp(other_tp(d)))

    for d in range(1, tp_n):
        sums(d).start()

    for d in range(1, tp_n):
        for j in range(xs):
            tokens_to(d, j).wait_send()
        weights_to(d).wait_send()
    for e in range(1, RING):
        weights_on(e).wait_send()
    for d in range(1, kv_n):

        @pl.when(serves(d))
        def _(d=d):
            give(d).wait_send()

    for g in range(count):

        def drain(g=g):
            for i in range(far + 1):
                spread(g, i).wait_send()
            for i in range(far):
                relay(g, i).wait_send()

        when_group(g, drain)

    @pl.loop(0, blocks)
    def _(b):
        for i in range(far):
            heads_to(b, i).wait_send()

    for g in range(pairs):
        swap(g).wait()
    for d in range(1, tp_n):
        sums(d).wait()
    gains = ogain_ref[:, pl.ds(pl.multiple_of(tp * cols, cols), cols)]
    for c in range(2):
        total = ss_ref[c]
        for p in range(1, xs):
            total = total + ss_ref[2 * p + c]
        inverse = lax.rsqrt(total / (cols * tp_n) + epsilon)
        for g in range(pairs):
            scale = jnp.broadcast_to(inverse[g : g + 1], (BLOCK, BLOCK)).T
            scale = jnp.concatenate([scale] * (cols // BLOCK), axis=1)
            rows = (proj_ref[g, c] * scale * gains).astype(jnp.bfloat16)
            for u in range(2):
                o_ref[pl.ds((2 * g + u) * BLOCK + c * half, half), :] = rows[u * half : (u + 1) * half]


def on_device(
    tokens,
    query_weight,
    latent_weight,
    query_gain,
    key_gain,
    value_up,
    out_weight,
    out_gain,
    chosen,
):
    toks, feat = tokens.shape
    width = latent_weight.shape[1]
    heads = query_weight.shape[1] // width
    blocks = toks // BLOCK
    kv_n, tp_n = lax.axis_size("kv"), lax.axis_size("tp")
    cols = out_weight.shape[1] // tp_n
    hv = out_weight.shape[0]
    xs = tp_n // 2
    far = xs - 1
    piece = BLOCK // tp_n
    slots = blocks + (kv_n - 1) * PER_OWNER
    halves = max(1, kv_n * blocks // LANES)
    count = 1 + len(owner_groups(kv_n))
    bf, f32, i32 = jnp.bfloat16, jnp.float32, jnp.int32
    dma = pltpu.SemaphoreType.DMA
    vmem = pl.BlockSpec(memory_space=pltpu.VMEM)
    sems = [
        (xs, tp_n - 1), (2,), (kv_n - 1,), (kv_n - 1,), (count, far + 1), (count, far),
        (tp_n - 1,), (RING - 1,), (blocks, far), (blocks // 2,), (tp_n - 1,),
    ]
    return pl.pallas_call(
        functools.partial(kernel, kv_n, tp_n),
        out_shape=jax.ShapeDtypeStruct((toks, cols), bf),
        in_specs=[vmem] * 9 + [pl.BlockSpec(memory_space=pltpu.SMEM)],
        out_specs=vmem,
        scratch_shapes=[
            pltpu.VMEM((tp_n, xs, blocks, piece, feat), bf),
            pltpu.VMEM(query_weight.shape, bf),
            pltpu.VMEM((value_up.shape[0], value_up.shape[2], value_up.shape[1]), bf),
            pltpu.VMEM((2 * heads, xs, blocks, piece, width), bf),
            pltpu.VMEM((blocks, piece, width), bf),
            pltpu.VMEM((kv_n - 1, PER_OWNER, piece, width), bf),
            pltpu.VMEM((tp_n, slots, piece, width), bf),
            pltpu.VMEM((slots + 1, BLOCK, width), bf),
            pltpu.VMEM((slots + 1, width + ONES, BLOCK), bf),
            pltpu.VMEM((2, hv, 2 * width), bf),
            pltpu.VMEM((halves, 1, LANES), i32),
            pltpu.VMEM((halves, 1, LANES), i32),
            pltpu.VMEM((kv_n - 1, 1, LANES), i32),
            pltpu.SMEM((halves, 1, LANES), i32),
            pltpu.SMEM((kv_n - 1, 1, LANES), i32),
            pltpu.VMEM((xs, blocks, BLOCK // 2, 2 * hv), bf),
            pltpu.VMEM((tp_n, RING, hv // RING, 2 * cols), bf),
            pltpu.VMEM((blocks // 2, 2, BLOCK, cols), f32),
            pltpu.VMEM((blocks // 2, BLOCK, cols), f32),
            pltpu.VMEM((tp_n, blocks // 2, BLOCK), f32),
            dma((2,)), *[dma(shape) for shape in sems for _ in range(2)],
        ],
        compiler_params=pltpu.CompilerParams(
            collective_id=0, has_side_effects=True, vmem_limit_bytes=60 << 20
        ),
    )(
        tokens.reshape(blocks, 2, xs, piece, feat), query_weight, latent_weight, query_gain[None, :],
        key_gain[None, :], jnp.swapaxes(value_up, 1, 2), out_weight, out_gain[None, :], chosen, chosen,
    )


def solution(mesh):
    in_specs = (
        P("kv", "tp"),
        P(None, "tp"),
        P(),
        P(),
        P(),
        P("tp", None, None),
        P("tp", None),
        P(),
        P("kv", None),
    )
    out_specs = P("kv", "tp")
    return jax.shard_map(
        on_device, mesh=mesh, in_specs=in_specs, out_specs=out_specs, check_vma=False
    )
```

```python
import functools

import jax
import jax.numpy as jnp
from jax import lax
from jax.experimental import pallas as pl
from jax.experimental.pallas import tpu as pltpu
from jax.sharding import PartitionSpec as P

BLOCK = 128
PER_OWNER = 2
RING = 4
OWNERS = 8
STEP = 8
LANES = 128
ONES = 16
MESH = pl.DeviceIdType.MESH

epsilon = 1e-06
masked_score = -1e30


def rms_scale(values, gain_row):
    widened = values.astype(jnp.float32)
    mean_sq = jnp.mean(widened * widened, axis=-1, keepdims=True)
    return (widened * lax.rsqrt(mean_sq + epsilon) * gain_row).astype(jnp.bfloat16)


def prefix_in_owner(values, lane, blocks, inclusive):
    total = values if inclusive else jnp.zeros_like(values)
    for s in range(1, blocks):
        total = total + jnp.where(lane % blocks >= s, pltpu.roll(values, s, 1), 0)
    return total


def send(src, dst, sems, where):
    return pltpu.make_async_remote_copy(
        src_ref=src, dst_ref=dst, send_sem=sems[0], recv_sem=sems[1], device_id=where, device_id_type=MESH
    )


def owner_groups(kv_n):
    return [(d, min(d + OWNERS, kv_n)) for d in range(1, kv_n, OWNERS)]


def kernel(
    kv_n, tp_n,
    tok_ref, wq_ref, wl_ref, qgain_ref, kgain_ref, vu_ref, w_ref, ogain_ref, chosen_ref, chosen_s,
    o_ref,
    tk_ref, wqs_ref, vus_ref, q_ref, lat_ref, out_ref, kvp_ref, kn_ref, vt_ref, bd_ref,
    map_ref, req_ref, chs_ref, map_s, chs_s,
    ho_ref, wc_ref, proj_ref, px_ref, ss_ref,
    lc, t_s, t_r, tf_s, tf_r, c_s, c_r, ch_s, ch_r, b_s, b_r, k_s, k_r, kf_s, kf_r, kr_s, kr_r,
    w_s, w_r, y_s, y_r, h_s, h_r, hf_s, hf_r, p_s, p_r, s_s, s_r,
):
    kv, tp = lax.axis_index("kv"), lax.axis_index("tp")
    core, x = lax.rem(tp, 2), tp // 2
    sib = tp + 1 - 2 * core
    blocks, _, xs, piece, feat = tok_ref.shape
    width = wl_ref.shape[1]
    heads = wq_ref.shape[1] // width
    vdim = vu_ref.shape[1]
    slots = kvp_ref.shape[1]
    picks = chosen_ref.shape[1]
    cols = o_ref.shape[1]
    half = BLOCK // 2
    mine = blocks * piece
    per_row = LANES // blocks
    wrows = w_ref.shape[0] // RING
    y = lax.rem(kv, RING)

    def at_kv(other):
        return {"kv": other, "tp": tp}

    def at_tp(other):
        return {"kv": kv, "tp": other}

    def other_tp(d):
        return lax.rem(tp + d + tp_n, tp_n)

    barrier = pltpu.get_barrier_semaphore()
    for d in range(1, kv_n):
        pl.semaphore_signal(barrier, inc=1, device_id=at_kv(lax.rem(kv + d, kv_n)), device_id_type=MESH)
    for d in range(1, tp_n):
        pl.semaphore_signal(barrier, inc=1, device_id=at_tp(other_tp(d)), device_id_type=MESH)

    lane = lax.broadcasted_iota(jnp.int32, (blocks, LANES), 1)
    halves = map_ref.shape[0]
    table = chosen_ref[...]
    for g in range(halves):
        hit = jnp.zeros((blocks, LANES), jnp.int32)
        for c in range(picks):
            hit = jnp.where(table[:, c : c + 1] == lane + g * LANES, 1, hit)
        need = jnp.broadcast_to(jnp.max(hit, axis=0, keepdims=True), (blocks, LANES))
        rank = prefix_in_owner(need, lane, blocks, False)
        local = lane % blocks
        dist = kv - (lane // blocks + g * per_row)
        slot = jnp.where(dist == 0, local, blocks + (dist - 1) * PER_OWNER + rank)
        map_ref[g] = jnp.clip(slot, 0, slots - 1)[0:1]
        code = jnp.zeros((blocks, LANES), jnp.int32)
        for k in range(PER_OWNER):
            code = code + jnp.where((need > 0) & (rank == k), local * blocks**k, 0)
        req_ref[g] = prefix_in_owner(code, lane, blocks, True)[0:1]

    pltpu.make_async_copy(map_ref, map_s, lc.at[0]).start()
    pl.semaphore_wait(barrier, kv_n - 1 + tp_n - 1)

    def chip(i):
        return lax.rem(x + i + xs, xs)

    def same_core(i):
        return 2 * chip(i) + core

    def tokens_to(e, j):
        c = lax.rem(core + e % 2, 2)
        part = chip(e // 2 + j)
        return send(
            tok_ref.at[:, c, part], tk_ref.at[tp, part], (t_s.at[j, e - 1], t_r.at[j, e - 1]), at_tp(2 * chip(e // 2) + c)
        )

    beside = [e for e in range(1, tp_n) if e // 2 != 2]

    def tokens_on(j, way):
        step = 1 - 2 * way
        part = tk_ref.at[2 * chip(-step) + way, chip(step + j)]
        return send(part, part, (tf_s.at[j, way], tf_r.at[j, way]), at_tp(same_core(step)))

    def ask(d):
        owner = kv - d
        return send(
            req_ref.at[jnp.maximum(owner, 0) // per_row], chs_ref.at[d - 1],
            (ch_s.at[d - 1], ch_r.at[d - 1]), at_kv(lax.rem(owner + kv_n, kv_n)),
        )

    def asks(d):
        return kv - d >= 0

    def serves(d):
        return kv + d < kv_n

    def weights_to(d):
        other = other_tp(d)
        part = w_ref.at[
            pl.ds(pl.multiple_of(y * wrows, wrows), wrows),
            pl.ds(pl.multiple_of(other // 2 * 2 * cols, 2 * cols), 2 * cols),
        ]
        return send(part, wc_ref.at[tp, y], (w_s.at[d - 1], w_r.at[d - 1]), at_tp(other))

    def weights_on(e):
        part = wc_ref.at[:, y]
        other = kv - y + lax.rem(y + e, RING)
        return send(part, part, (y_s.at[e - 1], y_r.at[e - 1]), at_kv(other))

    to_sib = [
        send(wq_ref, wqs_ref, (c_s.at[0], c_r.at[0]), at_tp(sib)),
        send(vu_ref, vus_ref, (c_s.at[1], c_r.at[1]), at_tp(sib)),
    ]

    for e in range(1, tp_n):
        tokens_to(e, 0).start()
    for d in range(1, kv_n):

        @pl.when(asks(d))
        def _(d=d):
            ask(d).start()

    for j in range(1, xs):
        for e in beside:
            tokens_to(e, j).start()
    for copy in to_sib:
        copy.start()
    for d in range(1, tp_n):
        weights_to(d).start()

    for p in range(xs):
        tk_ref[tp, p] = tok_ref[:, core, p]
    wc_ref[tp, y] = w_ref[
        pl.ds(pl.multiple_of(y * wrows, wrows), wrows), pl.ds(pl.multiple_of(x * 2 * cols, 2 * cols), 2 * cols)
    ]
    null = slots
    kn_ref[null] = jnp.zeros((BLOCK, width), jnp.bfloat16)
    vt_ref[null] = jnp.zeros((width + ONES, BLOCK), jnp.bfloat16)
    bd_ref[...] = jnp.zeros_like(bd_ref)

    def features(p):
        return jnp.concatenate([tk_ref[t, p].reshape(mine, feat) for t in range(tp_n)], axis=1)

    def hand_tokens(j):
        if j:
            for e in beside:
                tokens_to(e, j).wait_recv()
        if j != 1:
            tokens_on((j - 1) % xs, 0).start()
        if j < xs - 1:
            tokens_on(j + 1, 1).start()

    for d in range(1, kv_n):

        @pl.when(asks(d))
        def _(d=d):
            ask(d).wait_send()

        @pl.when(serves(d))
        def _(d=d):
            ask(d).wait_recv()

    to_smem = pltpu.make_async_copy(chs_ref, chs_s, lc.at[1])
    to_smem.start()
    for e in range(1, tp_n):
        tokens_to(e, 0).wait_recv()
    hand_tokens(0)
    lat = jnp.dot(features(x), wl_ref[...], preferred_element_type=jnp.float32).astype(jnp.bfloat16)
    lat_ref[...] = lat.reshape(blocks, piece, width)
    kvp_ref[tp, 0:blocks] = lat.reshape(blocks, piece, width)

    pltpu.make_async_copy(map_ref, map_s, lc.at[0]).wait()
    to_smem.wait()

    def slots_of(d):
        return pl.ds(blocks + (d - 1) * PER_OWNER, PER_OWNER)

    def give(d):
        return send(
            out_ref.at[d - 1], kvp_ref.at[tp, slots_of(d)], (b_s.at[d - 1], b_r.at[d - 1]), at_kv(lax.rem(kv + d, kv_n))
        )

    at_lane = lax.rem(kv, per_row) * blocks + blocks - 1
    for d in range(1, kv_n):

        @pl.when(serves(d))
        def _(d=d):
            code = chs_s[d - 1, 0, at_lane]
            for k in range(PER_OWNER):
                out_ref[d - 1, k] = lat_ref[(code >> (3 * k)) & (blocks - 1)]
            give(d).start()

    remote = owner_groups(kv_n)
    groups = [(0, blocks)] + [
        (blocks + (a - 1) * PER_OWNER, (b - a) * PER_OWNER) for a, b in remote
    ]

    def halves_of(g):
        first, size = groups[g]
        cut = (size + 1) // 2
        return [pl.ds(first, cut), pl.ds(first + cut, size - cut)]

    def spread(g, i):
        part = kvp_ref.at[tp, pl.ds(*groups[g])]
        where = sib if i == 2 else same_core(1 - 2 * i)
        return send(part, part, (k_s.at[g, i], k_r.at[g, i]), at_tp(where))

    def pass_on(g, way):
        step = 1 - 2 * way
        part = kvp_ref.at[same_core(-step), halves_of(g)[way]]
        return send(part, part, (kf_s.at[g, way], kf_r.at[g, way]), at_tp(same_core(step)))

    def relay(g, i):
        if i < 2:
            part = kvp_ref.at[same_core(2 * i - 1), pl.ds(*groups[g])]
        else:
            part = kvp_ref.at[same_core(2), halves_of(g)[i - 2]]
        return send(part, part, (kr_s.at[g, i], kr_r.at[g, i]), at_tp(sib))

    def when_group(g, body):
        if g == 0:
            body()
        else:
            pl.when(kv >= remote[g - 1][0])(body)

    def spread_group(g):
        def body():
            if g:
                for d in range(*remote[g - 1]):

                    @pl.when(asks(d))
                    def _(d=d):
                        give(d).wait_recv()

            for i in range(3):
                spread(g, i).start()

        when_group(g, body)

    def pass_group(g):
        def body():
            for i in range(2):
                spread(g, i).wait_recv()
                pass_on(g, i).start()
                relay(g, i).start()

        when_group(g, body)

    def relay_group(g):
        def body():
            for i in range(2):
                pass_on(g, i).wait_recv()
                relay(g, i + 2).start()

        when_group(g, body)

    gain_k = kgain_ref[...]

    def norm_group(g):
        def body():
            spread(g, 2).wait_recv()
            for i in range(4):
                relay(g, i).wait_recv()

            @pl.loop(groups[g][0], groups[g][0] + groups[g][1])
            def _(slot):
                rows = jnp.concatenate(
                    [kvp_ref[p * 2 + c, slot] for c in range(2) for p in range(xs)], axis=0
                )
                kn_ref[slot] = rms_scale(rows, gain_k)
                vt_ref[slot, 0:width, :] = rows.T
                vt_ref[slot, width:, :] = jnp.ones((ONES, BLOCK), jnp.bfloat16)

        when_group(g, body)

    gain_q = qgain_ref[...] * (width**-0.5 * 1.4426950408889634)

    def project(j):
        if j:
            for way in range(2):
                tokens_on(j, way).wait_recv()
        p = lax.rem(x + j, xs)
        rows = features(p)
        for w, at in ((wq_ref, core), (wqs_ref, 1 - core)):
            qs = jnp.dot(rows, w[...], preferred_element_type=jnp.float32).astype(jnp.bfloat16)
            for h in range(heads):
                part = rms_scale(qs[:, h * width : (h + 1) * width], gain_q)
                q_ref[at * heads + h, p] = part.reshape(blocks, piece, width)

    spread_group(0)
    for copy in to_sib:
        copy.wait()
    for v, at in ((vu_ref, core), (vus_ref, 1 - core)):
        for h in range(heads):
            bd_ref[at, h * vdim : (h + 1) * vdim, h * width : (h + 1) * width] = v[h]
    count = len(groups)
    for step in range(count + 3):
        if step and step < count:
            spread_group(step)
        if 1 <= step <= count:
            pass_group(step - 1)
        if step + 1 < xs:
            hand_tokens(step + 1)
        if 2 <= step <= count + 1:
            relay_group(step - 2)
        if step < xs:
            project(step)
        if step >= 3:
            norm_group(step - 3)
        if step == 3:
            for d in range(1, tp_n):
                weights_to(d).wait_recv()
            for e in range(1, RING):
                weights_on(e).start()

    def listed(b, c):
        block = chosen_s[b, c]
        known = jnp.maximum(block, 0)
        return jnp.where(block < 0, null, map_s[known >> 7, 0, known & (LANES - 1)])

    def attend_block(b):
        q = jnp.concatenate([q_ref[h, p, b] for h in range(2 * heads) for p in range(xs)], axis=0)
        qt = q.T
        acc = jnp.zeros((width + ONES, 2 * heads * half), jnp.float32)
        for i in range(0, picks, STEP):
            at = [listed(b, i + k) for k in range(STEP)]
            keys = jnp.concatenate([kn_ref[s] for s in at], axis=0)
            s = jnp.dot(keys, qt, preferred_element_type=jnp.float32)
            if i == 0:
                key_row = lax.broadcasted_iota(jnp.int32, s.shape, 0)
                query_row = lax.broadcasted_iota(jnp.int32, s.shape, 1) % half + core * half
                s = jnp.where((key_row <= query_row) | (key_row >= BLOCK), s, masked_score)
            p = jnp.exp2(s).astype(jnp.bfloat16)
            values = jnp.concatenate([vt_ref[s] for s in at], axis=1)
            acc = acc + jnp.dot(values, p, preferred_element_type=jnp.float32)
        att = (acc[:width] / acc[width : width + 1]).astype(jnp.bfloat16).T
        out = []
        for h in range(0, 2 * heads, 2):
            two = jnp.concatenate([att[h * half : (h + 1) * half], att[(h + 1) * half : (h + 2) * half]], axis=1)
            out.append(
                lax.dot_general(two, bd_ref[h // 2], (((1,), (1,)), ((), ())), preferred_element_type=jnp.float32)
            )
        return jnp.concatenate(out, axis=1).astype(jnp.bfloat16)

    last = blocks - 1
    pairs = blocks // 2

    def heads_to(b, i):
        part = ho_ref.at[x, b]
        return send(part, part, (h_s.at[b, i], h_r.at[b, i]), at_tp(same_core((1, -1, 2)[i])))

    def heads_on(b, way):
        step = 1 - 2 * way
        part = ho_ref.at[chip(-step), b, pl.ds(way * half // 2, half // 2)]
        return send(part, part, (hf_s.at[b, way], hf_r.at[b, way]), at_tp(same_core(step)))

    def pass_heads(b):
        for way in range(2):
            heads_to(b, way).wait_recv()
            heads_on(b, way).start()

    def finish(g):
        for u in range(2):
            if not isinstance(g, jax.Array) and 2 * g + u == last:
                for i in range(3):
                    heads_to(last, i).wait_recv()
            else:
                for way in range(2):
                    heads_on(2 * g + u, way).wait_recv()
        total = jnp.zeros((BLOCK, 2 * cols), jnp.float32)
        for p in range(xs):
            rows = ho_ref[p, pl.ds(2 * g, 2)].reshape(BLOCK, 2 * cols)
            w = jnp.concatenate([wc_ref[2 * p + c].reshape(RING * wrows, 2 * cols) for c in range(2)], axis=0)
            total = total + jnp.dot(rows, w, preferred_element_type=jnp.float32)
        left, right = total[:, :cols], total[:, cols:]
        px_ref[g] = jnp.where(core == 0, right, left)
        proj_ref[g, core] = jnp.where(core == 0, left, right)
        squares = jnp.sum(total * total, axis=1, keepdims=True)
        ss_ref[tp, pl.ds(g, 1), :] = jnp.broadcast_to(squares, (BLOCK, BLOCK)).T[0:1]
        swap(g).start()

    def swap(g):
        return send(px_ref.at[g], proj_ref.at[g, core], (p_s.at[g], p_r.at[g]), at_tp(sib))

    @pl.loop(0, blocks)
    def _(b):
        ho_ref[x, b] = attend_block(b)
        for i in range(2):
            heads_to(b, i).start()

        @pl.when(b == last)
        def _():
            heads_to(last, 2).start()

        @pl.when(b >= 2)
        def _():
            pass_heads(b - 2)

        @pl.when(b == 4)
        def _():
            for e in range(1, RING):
                weights_on(e).wait_recv()

        @pl.when((b >= 5) & (lax.rem(b, 2) == 1))
        def _():
            finish((b - 5) // 2)

    pass_heads(last - 1)
    for g in range(max(pairs - 2, 0), pairs):
        finish(g)

    def sums(d):
        return send(ss_ref.at[tp], ss_ref.at[tp], (s_s.at[d - 1], s_r.at[d - 1]), at_tp(other_tp(d)))

    for d in range(1, tp_n):
        sums(d).start()

    for j in range(xs):
        for e in range(1, tp_n) if j == 0 else beside:
            tokens_to(e, j).wait_send()
        if j:
            for way in range(2):
                tokens_on(j, way).wait_send()
    for d in range(1, tp_n):
        weights_to(d).wait_send()
    for e in range(1, RING):
        weights_on(e).wait_send()
    for d in range(1, kv_n):

        @pl.when(serves(d))
        def _(d=d):
            give(d).wait_send()

    for g in range(count):

        def drain(g=g):
            for i in range(3):
                spread(g, i).wait_send()
            for i in range(2):
                pass_on(g, i).wait_send()
            for i in range(4):
                relay(g, i).wait_send()

        when_group(g, drain)

    @pl.loop(0, last)
    def _(b):
        for i in range(2):
            heads_to(b, i).wait_send()
            heads_on(b, i).wait_send()

    for i in range(3):
        heads_to(last, i).wait_send()
    for g in range(pairs):
        swap(g).wait()
    for d in range(1, tp_n):
        sums(d).wait()
    gains = ogain_ref[:, pl.ds(pl.multiple_of(tp * cols, cols), cols)]
    for c in range(2):
        total = ss_ref[c]
        for p in range(1, xs):
            total = total + ss_ref[2 * p + c]
        inverse = lax.rsqrt(total / (cols * tp_n) + epsilon)
        for g in range(pairs):
            scale = jnp.broadcast_to(inverse[g : g + 1], (BLOCK, BLOCK)).T
            scale = jnp.concatenate([scale] * (cols // BLOCK), axis=1)
            rows = (proj_ref[g, c] * scale * gains).astype(jnp.bfloat16)
            for u in range(2):
                o_ref[pl.ds((2 * g + u) * BLOCK + c * half, half), :] = rows[u * half : (u + 1) * half]


def on_device(
    tokens,
    query_weight,
    latent_weight,
    query_gain,
    key_gain,
    value_up,
    out_weight,
    out_gain,
    chosen,
):
    toks, feat = tokens.shape
    width = latent_weight.shape[1]
    heads = query_weight.shape[1] // width
    blocks = toks // BLOCK
    kv_n, tp_n = lax.axis_size("kv"), lax.axis_size("tp")
    cols = out_weight.shape[1] // tp_n
    hv = out_weight.shape[0]
    xs = tp_n // 2
    piece = BLOCK // tp_n
    slots = blocks + (kv_n - 1) * PER_OWNER
    halves = max(1, kv_n * blocks // LANES)
    count = 1 + len(owner_groups(kv_n))
    bf, f32, i32 = jnp.bfloat16, jnp.float32, jnp.int32
    dma = pltpu.SemaphoreType.DMA
    vmem = pl.BlockSpec(memory_space=pltpu.VMEM)
    sems = [
        (xs, tp_n - 1), (xs, 2), (2,), (kv_n - 1,), (kv_n - 1,), (count, 3), (count, 2), (count, 4),
        (tp_n - 1,), (RING - 1,), (blocks, 3), (blocks, 2), (blocks // 2,), (tp_n - 1,),
    ]
    return pl.pallas_call(
        functools.partial(kernel, kv_n, tp_n),
        out_shape=jax.ShapeDtypeStruct((toks, cols), bf),
        in_specs=[vmem] * 9 + [pl.BlockSpec(memory_space=pltpu.SMEM)],
        out_specs=vmem,
        scratch_shapes=[
            pltpu.VMEM((tp_n, xs, blocks, piece, feat), bf),
            pltpu.VMEM(query_weight.shape, bf),
            pltpu.VMEM((value_up.shape[0], value_up.shape[2], value_up.shape[1]), bf),
            pltpu.VMEM((2 * heads, xs, blocks, piece, width), bf),
            pltpu.VMEM((blocks, piece, width), bf),
            pltpu.VMEM((kv_n - 1, PER_OWNER, piece, width), bf),
            pltpu.VMEM((tp_n, slots, piece, width), bf),
            pltpu.VMEM((slots + 1, BLOCK, width), bf),
            pltpu.VMEM((slots + 1, width + ONES, BLOCK), bf),
            pltpu.VMEM((2, hv, 2 * width), bf),
            pltpu.VMEM((halves, 1, LANES), i32),
            pltpu.VMEM((halves, 1, LANES), i32),
            pltpu.VMEM((kv_n - 1, 1, LANES), i32),
            pltpu.SMEM((halves, 1, LANES), i32),
            pltpu.SMEM((kv_n - 1, 1, LANES), i32),
            pltpu.VMEM((xs, blocks, BLOCK // 2, 2 * hv), bf),
            pltpu.VMEM((tp_n, RING, hv // RING, 2 * cols), bf),
            pltpu.VMEM((blocks // 2, 2, BLOCK, cols), f32),
            pltpu.VMEM((blocks // 2, BLOCK, cols), f32),
            pltpu.VMEM((tp_n, blocks // 2, BLOCK), f32),
            dma((2,)), *[dma(shape) for shape in sems for _ in range(2)],
        ],
        compiler_params=pltpu.CompilerParams(
            collective_id=0, has_side_effects=True, vmem_limit_bytes=60 << 20
        ),
    )(
        tokens.reshape(blocks, 2, xs, piece, feat), query_weight, latent_weight, query_gain[None, :],
        key_gain[None, :], jnp.swapaxes(value_up, 1, 2), out_weight, out_gain[None, :], chosen, chosen,
    )


def solution(mesh):
    in_specs = (
        P("kv", "tp"),
        P(None, "tp"),
        P(),
        P(),
        P(),
        P("tp", None, None),
        P("tp", None),
        P(),
        P("kv", None),
    )
    out_specs = P("kv", "tp")
    return jax.shard_map(
        on_device, mesh=mesh, in_specs=in_specs, out_specs=out_specs, check_vma=False
    )
```

```python
import functools

import jax
import jax.numpy as jnp
from jax import lax
from jax.experimental import pallas as pl
from jax.experimental.pallas import tpu as pltpu
from jax.sharding import PartitionSpec as P

BLOCK = 128
PER_OWNER = 2
RING = 4
OWNERS = 8
STEP = 8
LANES = 128
ONES = 16
MESH = pl.DeviceIdType.MESH

epsilon = 1e-06
masked_score = -1e30


def rms_scale(values, gain_row):
    widened = values.astype(jnp.float32)
    mean_sq = jnp.mean(widened * widened, axis=-1, keepdims=True)
    return (widened * lax.rsqrt(mean_sq + epsilon) * gain_row).astype(jnp.bfloat16)


def prefix_in_owner(values, lane, blocks, inclusive):
    total = values if inclusive else jnp.zeros_like(values)
    for s in range(1, blocks):
        total = total + jnp.where(lane % blocks >= s, pltpu.roll(values, s, 1), 0)
    return total


def send(src, dst, sems, where):
    return pltpu.make_async_remote_copy(
        src_ref=src, dst_ref=dst, send_sem=sems[0], recv_sem=sems[1], device_id=where, device_id_type=MESH
    )


def owner_groups(kv_n):
    return [(d, min(d + OWNERS, kv_n)) for d in range(1, kv_n, OWNERS)]


def kernel(
    kv_n, tp_n,
    tok_ref, wq_ref, wl_ref, qgain_ref, kgain_ref, vu_ref, w_ref, ogain_ref, chosen_ref, chosen_s,
    out_hbm,
    o_ref, tk_ref, wqs_ref, vus_ref, q_ref, lat_ref, out_ref, kvp_ref, kn_ref, vt_ref, bd_ref,
    map_ref, req_ref, chs_ref, map_s, chs_s,
    ho_ref, wc_ref, proj_ref, px_ref, ss_ref,
    lc, oc, t_s, t_r, tf_s, tf_r, c_s, c_r, ch_s, ch_r, b_s, b_r, k_s, k_r, kf_s, kf_r, kr_s, kr_r,
    w_s, w_r, y_s, y_r, h_s, h_r, p_s, p_r, s_s, s_r,
):
    kv, tp = lax.axis_index("kv"), lax.axis_index("tp")
    core, x = lax.rem(tp, 2), tp // 2
    sib = tp + 1 - 2 * core
    blocks, _, xs, piece, feat = tok_ref.shape
    width = wl_ref.shape[1]
    heads = wq_ref.shape[1] // width
    vdim = vu_ref.shape[1]
    slots = kvp_ref.shape[1]
    picks = chosen_ref.shape[1]
    cols = o_ref.shape[1]
    half = BLOCK // 2
    mine = blocks * piece
    per_row = LANES // blocks
    wrows = w_ref.shape[0] // RING
    y = lax.rem(kv, RING)

    def at_kv(other):
        return {"kv": other, "tp": tp}

    def at_tp(other):
        return {"kv": kv, "tp": other}

    def other_tp(d):
        return lax.rem(tp + d + tp_n, tp_n)

    barrier = pltpu.get_barrier_semaphore()
    for d in range(1, kv_n):
        pl.semaphore_signal(barrier, inc=1, device_id=at_kv(lax.rem(kv + d, kv_n)), device_id_type=MESH)
    for d in range(1, tp_n):
        pl.semaphore_signal(barrier, inc=1, device_id=at_tp(other_tp(d)), device_id_type=MESH)

    lane = lax.broadcasted_iota(jnp.int32, (blocks, LANES), 1)
    halves = map_ref.shape[0]
    table = chosen_ref[...]
    for g in range(halves):
        hit = jnp.zeros((blocks, LANES), jnp.int32)
        for c in range(picks):
            hit = jnp.where(table[:, c : c + 1] == lane + g * LANES, 1, hit)
        need = jnp.broadcast_to(jnp.max(hit, axis=0, keepdims=True), (blocks, LANES))
        rank = prefix_in_owner(need, lane, blocks, False)
        local = lane % blocks
        dist = kv - (lane // blocks + g * per_row)
        slot = jnp.where(dist == 0, local, blocks + (dist - 1) * PER_OWNER + rank)
        map_ref[g] = jnp.clip(slot, 0, slots - 1)[0:1]
        code = jnp.zeros((blocks, LANES), jnp.int32)
        for k in range(PER_OWNER):
            code = code + jnp.where((need > 0) & (rank == k), local * blocks**k, 0)
        req_ref[g] = prefix_in_owner(code, lane, blocks, True)[0:1]

    pltpu.make_async_copy(map_ref, map_s, lc.at[0]).start()
    pl.semaphore_wait(barrier, kv_n - 1 + tp_n - 1)

    def chip(i):
        return lax.rem(x + i + xs, xs)

    def same_core(i):
        return 2 * chip(i) + core

    def tokens_to(e, j):
        c = lax.rem(core + e % 2, 2)
        part = chip(e // 2 + j)
        return send(
            tok_ref.at[:, c, part], tk_ref.at[tp, part], (t_s.at[j, e - 1], t_r.at[j, e - 1]), at_tp(2 * chip(e // 2) + c)
        )

    beside = [e for e in range(1, tp_n) if e // 2 != 2]

    def tokens_on(j, way):
        step = 1 - 2 * way
        part = tk_ref.at[2 * chip(-step) + way, chip(step + j)]
        return send(part, part, (tf_s.at[j, way], tf_r.at[j, way]), at_tp(same_core(step)))

    def ask(d):
        owner = kv - d
        return send(
            req_ref.at[jnp.maximum(owner, 0) // per_row], chs_ref.at[d - 1],
            (ch_s.at[d - 1], ch_r.at[d - 1]), at_kv(lax.rem(owner + kv_n, kv_n)),
        )

    def asks(d):
        return kv - d >= 0

    def serves(d):
        return kv + d < kv_n

    def weights_to(d):
        other = other_tp(d)
        part = w_ref.at[
            pl.ds(pl.multiple_of(y * wrows, wrows), wrows),
            pl.ds(pl.multiple_of(other // 2 * 2 * cols, 2 * cols), 2 * cols),
        ]
        return send(part, wc_ref.at[tp, y], (w_s.at[d - 1], w_r.at[d - 1]), at_tp(other))

    def weights_on(e):
        part = wc_ref.at[:, y]
        other = kv - y + lax.rem(y + e, RING)
        return send(part, part, (y_s.at[e - 1], y_r.at[e - 1]), at_kv(other))

    to_sib = [
        send(wq_ref, wqs_ref, (c_s.at[0], c_r.at[0]), at_tp(sib)),
        send(vu_ref, vus_ref, (c_s.at[1], c_r.at[1]), at_tp(sib)),
    ]

    for e in range(1, tp_n):
        tokens_to(e, 0).start()
    for d in range(1, kv_n):

        @pl.when(asks(d))
        def _(d=d):
            ask(d).start()

    for j in range(1, xs):
        for e in beside:
            tokens_to(e, j).start()
    for copy in to_sib:
        copy.start()
    for d in range(1, tp_n):
        weights_to(d).start()

    for p in range(xs):
        tk_ref[tp, p] = tok_ref[:, core, p]
    wc_ref[tp, y] = w_ref[
        pl.ds(pl.multiple_of(y * wrows, wrows), wrows), pl.ds(pl.multiple_of(x * 2 * cols, 2 * cols), 2 * cols)
    ]
    null = slots
    vt_ref[:, width:, :] = jnp.ones((slots + 1, ONES, BLOCK), jnp.bfloat16)
    kn_ref[null] = jnp.zeros((BLOCK, width), jnp.bfloat16)
    vt_ref[null] = jnp.zeros((width + ONES, BLOCK), jnp.bfloat16)
    bd_ref[...] = jnp.zeros_like(bd_ref)

    def features(p):
        return jnp.concatenate([tk_ref[t, p].reshape(mine, feat) for t in range(tp_n)], axis=1)

    def hand_tokens(j):
        if j:
            for e in beside:
                tokens_to(e, j).wait_recv()
        if j != 1:
            tokens_on((j - 1) % xs, 0).start()
        if j < xs - 1:
            tokens_on(j + 1, 1).start()

    for d in range(1, kv_n):

        @pl.when(asks(d))
        def _(d=d):
            ask(d).wait_send()

        @pl.when(serves(d))
        def _(d=d):
            ask(d).wait_recv()

    to_smem = pltpu.make_async_copy(chs_ref, chs_s, lc.at[1])
    to_smem.start()
    for e in range(1, tp_n):
        tokens_to(e, 0).wait_recv()
    hand_tokens(0)
    lat = jnp.dot(features(x), wl_ref[...], preferred_element_type=jnp.float32).astype(jnp.bfloat16)
    lat_ref[...] = lat.reshape(blocks, piece, width)
    kvp_ref[tp, 0:blocks] = lat.reshape(blocks, piece, width)

    pltpu.make_async_copy(map_ref, map_s, lc.at[0]).wait()
    to_smem.wait()

    def slots_of(d):
        return pl.ds(blocks + (d - 1) * PER_OWNER, PER_OWNER)

    def give(d):
        return send(
            out_ref.at[d - 1], kvp_ref.at[tp, slots_of(d)], (b_s.at[d - 1], b_r.at[d - 1]), at_kv(lax.rem(kv + d, kv_n))
        )

    at_lane = lax.rem(kv, per_row) * blocks + blocks - 1
    for d in range(1, kv_n):

        @pl.when(serves(d))
        def _(d=d):
            code = chs_s[d - 1, 0, at_lane]
            for k in range(PER_OWNER):
                out_ref[d - 1, k] = lat_ref[(code >> (3 * k)) & (blocks - 1)]
            give(d).start()

    remote = owner_groups(kv_n)
    groups = [(0, blocks)] + [
        (blocks + (a - 1) * PER_OWNER, (b - a) * PER_OWNER) for a, b in remote
    ]

    def halves_of(g):
        first, size = groups[g]
        cut = (size + 1) // 2
        return [pl.ds(first, cut), pl.ds(first + cut, size - cut)]

    def spread(g, i):
        part = kvp_ref.at[tp, pl.ds(*groups[g])]
        where = sib if i == 2 else same_core(1 - 2 * i)
        return send(part, part, (k_s.at[g, i], k_r.at[g, i]), at_tp(where))

    def pass_on(g, way):
        step = 1 - 2 * way
        part = kvp_ref.at[same_core(-step), halves_of(g)[way]]
        return send(part, part, (kf_s.at[g, way], kf_r.at[g, way]), at_tp(same_core(step)))

    def relay(g, i):
        if i < 2:
            part = kvp_ref.at[same_core(2 * i - 1), pl.ds(*groups[g])]
        else:
            part = kvp_ref.at[same_core(2), halves_of(g)[i - 2]]
        return send(part, part, (kr_s.at[g, i], kr_r.at[g, i]), at_tp(sib))

    def when_group(g, body):
        if g == 0:
            body()
        else:
            pl.when(kv >= remote[g - 1][0])(body)

    def spread_group(g):
        def body():
            if g:
                for d in range(*remote[g - 1]):

                    @pl.when(asks(d))
                    def _(d=d):
                        give(d).wait_recv()

            for i in range(3):
                spread(g, i).start()

        when_group(g, body)

    def pass_group(g):
        def body():
            for i in range(2):
                spread(g, i).wait_recv()
                pass_on(g, i).start()
                relay(g, i).start()

        when_group(g, body)

    def relay_group(g):
        def body():
            for i in range(2):
                pass_on(g, i).wait_recv()
                relay(g, i + 2).start()

        when_group(g, body)

    gain_k = kgain_ref[...]

    def norm_group(g):
        def body():
            spread(g, 2).wait_recv()
            for i in range(4):
                relay(g, i).wait_recv()

            first, size = groups[g]
            each = next(n for n in (4, 2, 1) if size % n == 0)

            @pl.loop(0, size // each)
            def _(i):
                for u in range(each):
                    slot = first + i * each + u
                    rows = jnp.concatenate(
                        [kvp_ref[p * 2 + c, slot] for c in range(2) for p in range(xs)], axis=0
                    )
                    kn_ref[slot] = rms_scale(rows, gain_k)
                    vt_ref[slot, 0:width, :] = rows.T

        when_group(g, body)

    gain_q = qgain_ref[...] * (width**-0.5 * 1.4426950408889634)

    def project(j):
        if j:
            for way in range(2):
                tokens_on(j, way).wait_recv()
        p = lax.rem(x + j, xs)
        rows = features(p)
        for w, at in ((wq_ref, core), (wqs_ref, 1 - core)):
            qs = jnp.dot(rows, w[...], preferred_element_type=jnp.float32).astype(jnp.bfloat16)
            for h in range(heads):
                part = rms_scale(qs[:, h * width : (h + 1) * width], gain_q)
                q_ref[at * heads + h, p] = part.reshape(blocks, piece, width)

    spread_group(0)
    for copy in to_sib:
        copy.wait()
    for v, at in ((vu_ref, core), (vus_ref, 1 - core)):
        for h in range(heads):
            bd_ref[at, h * vdim : (h + 1) * vdim, h * width : (h + 1) * width] = v[h]
    count = len(groups)
    project(0)
    for j in range(1, xs):
        hand_tokens(j)
    for step in range(1, count + 3):
        if step < count:
            spread_group(step)
        if step <= count:
            pass_group(step - 1)
        if 2 <= step <= count + 1:
            relay_group(step - 2)
        if 2 <= step <= xs:
            project(step - 1)
        if step >= 3:
            norm_group(step - 3)
        if step == 3:
            for d in range(1, tp_n):
                weights_to(d).wait_recv()
            for e in range(1, RING):
                weights_on(e).start()

    def listed(b, c):
        block = chosen_s[b, c]
        known = jnp.maximum(block, 0)
        return jnp.where(block < 0, null, map_s[known >> 7, 0, known & (LANES - 1)])

    def attend_block(b):
        q = jnp.concatenate([q_ref[h, p, b] for h in range(2 * heads) for p in range(xs)], axis=0)
        qt = q.T
        acc = jnp.zeros((width + ONES, 2 * heads * half), jnp.float32)
        for i in range(0, picks, STEP):
            at = [listed(b, i + k) for k in range(STEP)]
            keys = jnp.concatenate([kn_ref[s] for s in at], axis=0)
            s = jnp.dot(keys, qt, preferred_element_type=jnp.float32)
            if i == 0:
                key_row = lax.broadcasted_iota(jnp.int32, s.shape, 0)
                query_row = lax.broadcasted_iota(jnp.int32, s.shape, 1) % half + core * half
                s = jnp.where((key_row <= query_row) | (key_row >= BLOCK), s, masked_score)
            p = jnp.exp2(s).astype(jnp.bfloat16)
            values = jnp.concatenate([vt_ref[s] for s in at], axis=1)
            acc = acc + jnp.dot(values, p, preferred_element_type=jnp.float32)
        att = (acc[:width] / acc[width : width + 1]).astype(jnp.bfloat16).T
        out = []
        for h in range(0, 2 * heads, 2):
            two = jnp.concatenate([att[h * half : (h + 1) * half], att[(h + 1) * half : (h + 2) * half]], axis=1)
            out.append(
                lax.dot_general(two, bd_ref[h // 2], (((1,), (1,)), ((), ())), preferred_element_type=jnp.float32)
            )
        return jnp.concatenate(out, axis=1).astype(jnp.bfloat16)

    pairs = blocks // 2

    def heads_to(b, i):
        part = ho_ref.at[x, b]
        return send(part, part, (h_s.at[b, i], h_r.at[b, i]), at_tp(same_core((2, 1, -1)[i])))

    def finish(g):
        for u in range(2):
            for i in range(3):
                heads_to(2 * g + u, i).wait_recv()
        total = jnp.zeros((BLOCK, 2 * cols), jnp.float32)
        for p in range(xs):
            rows = ho_ref[p, pl.ds(2 * g, 2)].reshape(BLOCK, 2 * cols)
            w = jnp.concatenate([wc_ref[2 * p + c].reshape(RING * wrows, 2 * cols) for c in range(2)], axis=0)
            total = total + jnp.dot(rows, w, preferred_element_type=jnp.float32)
        left, right = total[:, :cols], total[:, cols:]
        px_ref[g] = jnp.where(core == 0, right, left)
        proj_ref[g, core] = jnp.where(core == 0, left, right)
        squares = jnp.sum(total * total, axis=1, keepdims=True)
        ss_ref[tp, pl.ds(g, 1), :] = jnp.broadcast_to(squares, (BLOCK, BLOCK)).T[0:1]
        swap(g).start()

    def swap(g):
        return send(px_ref.at[g], proj_ref.at[g, core], (p_s.at[g], p_r.at[g]), at_tp(sib))

    @pl.loop(0, blocks)
    def _(b):
        ho_ref[x, b] = attend_block(b)
        for i in range(3):
            heads_to(b, i).start()

        @pl.when(b == 4)
        def _():
            for e in range(1, RING):
                weights_on(e).wait_recv()

        @pl.when((b >= 5) & (lax.rem(b, 2) == 1))
        def _():
            finish((b - 5) // 2)

    for g in range(max(pairs - 2, 0), pairs):
        finish(g)

    def sums(d):
        return send(ss_ref.at[tp], ss_ref.at[tp], (s_s.at[d - 1], s_r.at[d - 1]), at_tp(other_tp(d)))

    for d in range(1, tp_n):
        sums(d).start()

    for j in range(xs):
        for e in range(1, tp_n) if j == 0 else beside:
            tokens_to(e, j).wait_send()
        if j:
            for way in range(2):
                tokens_on(j, way).wait_send()
    for d in range(1, tp_n):
        weights_to(d).wait_send()
    for e in range(1, RING):
        weights_on(e).wait_send()
    for d in range(1, kv_n):

        @pl.when(serves(d))
        def _(d=d):
            give(d).wait_send()

    for g in range(count):

        def drain(g=g):
            for i in range(3):
                spread(g, i).wait_send()
            for i in range(2):
                pass_on(g, i).wait_send()
            for i in range(4):
                relay(g, i).wait_send()

        when_group(g, drain)

    @pl.loop(0, blocks)
    def _(b):
        for i in range(3):
            heads_to(b, i).wait_send()

    for g in range(pairs):
        swap(g).wait()
    for d in range(1, tp_n):
        sums(d).wait()
    gains = ogain_ref[:, pl.ds(pl.multiple_of(tp * cols, cols), cols)]
    inverse = []
    for c in range(2):
        total = ss_ref[c]
        for p in range(1, xs):
            total = total + ss_ref[2 * p + c]
        inverse.append(lax.rsqrt(total / (cols * tp_n) + epsilon))

    def store(g):
        part = pl.ds(2 * g * BLOCK, 2 * BLOCK)
        return pltpu.make_async_copy(o_ref.at[part], out_hbm.at[part], oc.at[g])

    for g in range(pairs):
        for c in range(2):
            scale = jnp.broadcast_to(inverse[c][g : g + 1], (BLOCK, BLOCK)).T
            scale = jnp.concatenate([scale] * (cols // BLOCK), axis=1)
            rows = (proj_ref[g, c] * scale * gains).astype(jnp.bfloat16)
            for u in range(2):
                o_ref[pl.ds((2 * g + u) * BLOCK + c * half, half), :] = rows[u * half : (u + 1) * half]
        store(g).start()
    for g in range(pairs):
        store(g).wait()


def on_device(
    tokens,
    query_weight,
    latent_weight,
    query_gain,
    key_gain,
    value_up,
    out_weight,
    out_gain,
    chosen,
):
    toks, feat = tokens.shape
    width = latent_weight.shape[1]
    heads = query_weight.shape[1] // width
    blocks = toks // BLOCK
    kv_n, tp_n = lax.axis_size("kv"), lax.axis_size("tp")
    cols = out_weight.shape[1] // tp_n
    hv = out_weight.shape[0]
    xs = tp_n // 2
    piece = BLOCK // tp_n
    slots = blocks + (kv_n - 1) * PER_OWNER
    halves = max(1, kv_n * blocks // LANES)
    count = 1 + len(owner_groups(kv_n))
    bf, f32, i32 = jnp.bfloat16, jnp.float32, jnp.int32
    dma = pltpu.SemaphoreType.DMA
    vmem = pl.BlockSpec(memory_space=pltpu.VMEM)
    sems = [
        (xs, tp_n - 1), (xs, 2), (2,), (kv_n - 1,), (kv_n - 1,), (count, 3), (count, 2), (count, 4),
        (tp_n - 1,), (RING - 1,), (blocks, 3), (blocks // 2,), (tp_n - 1,),
    ]
    return pl.pallas_call(
        functools.partial(kernel, kv_n, tp_n),
        out_shape=jax.ShapeDtypeStruct((toks, cols), bf),
        in_specs=[vmem] * 9 + [pl.BlockSpec(memory_space=pltpu.SMEM)],
        out_specs=pl.BlockSpec(memory_space=pl.ANY),
        scratch_shapes=[
            pltpu.VMEM((toks, cols), bf),
            pltpu.VMEM((tp_n, xs, blocks, piece, feat), bf),
            pltpu.VMEM(query_weight.shape, bf),
            pltpu.VMEM((value_up.shape[0], value_up.shape[2], value_up.shape[1]), bf),
            pltpu.VMEM((2 * heads, xs, blocks, piece, width), bf),
            pltpu.VMEM((blocks, piece, width), bf),
            pltpu.VMEM((kv_n - 1, PER_OWNER, piece, width), bf),
            pltpu.VMEM((tp_n, slots, piece, width), bf),
            pltpu.VMEM((slots + 1, BLOCK, width), bf),
            pltpu.VMEM((slots + 1, width + ONES, BLOCK), bf),
            pltpu.VMEM((2, hv, 2 * width), bf),
            pltpu.VMEM((halves, 1, LANES), i32),
            pltpu.VMEM((halves, 1, LANES), i32),
            pltpu.VMEM((kv_n - 1, 1, LANES), i32),
            pltpu.SMEM((halves, 1, LANES), i32),
            pltpu.SMEM((kv_n - 1, 1, LANES), i32),
            pltpu.VMEM((xs, blocks, BLOCK // 2, 2 * hv), bf),
            pltpu.VMEM((tp_n, RING, hv // RING, 2 * cols), bf),
            pltpu.VMEM((blocks // 2, 2, BLOCK, cols), f32),
            pltpu.VMEM((blocks // 2, BLOCK, cols), f32),
            pltpu.VMEM((tp_n, blocks // 2, BLOCK), f32),
            dma((2,)), dma((blocks // 2,)), *[dma(shape) for shape in sems for _ in range(2)],
        ],
        compiler_params=pltpu.CompilerParams(
            collective_id=0, has_side_effects=True, vmem_limit_bytes=60 << 20
        ),
    )(
        tokens.reshape(blocks, 2, xs, piece, feat), query_weight, latent_weight, query_gain[None, :],
        key_gain[None, :], jnp.swapaxes(value_up, 1, 2), out_weight, out_gain[None, :], chosen, chosen,
    )


def solution(mesh):
    in_specs = (
        P("kv", "tp"),
        P(None, "tp"),
        P(),
        P(),
        P(),
        P("tp", None, None),
        P("tp", None),
        P(),
        P("kv", None),
    )
    out_specs = P("kv", "tp")
    return jax.shard_map(
        on_device, mesh=mesh, in_specs=in_specs, out_specs=out_specs, check_vma=False
    )
```

```python
import functools

import jax
import jax.numpy as jnp
from jax import lax
from jax.experimental import pallas as pl
from jax.experimental.pallas import tpu as pltpu
from jax.sharding import PartitionSpec as P

BLOCK = 128
PER_OWNER = 2
RING = 4
OWNERS = 8
STEP = 8
LANES = 128
ONES = 16
MESH = pl.DeviceIdType.MESH

epsilon = 1e-06
masked_score = -1e30


def rms_scale(values, gain_row):
    widened = values.astype(jnp.float32)
    mean_sq = jnp.mean(widened * widened, axis=-1, keepdims=True)
    return (widened * lax.rsqrt(mean_sq + epsilon) * gain_row).astype(jnp.bfloat16)


def prefix_in_owner(values, lane, blocks, inclusive):
    total = values if inclusive else jnp.zeros_like(values)
    for s in range(1, blocks):
        total = total + jnp.where(lane % blocks >= s, pltpu.roll(values, s, 1), 0)
    return total


def send(src, dst, sems, where):
    return pltpu.make_async_remote_copy(
        src_ref=src, dst_ref=dst, send_sem=sems[0], recv_sem=sems[1], device_id=where, device_id_type=MESH
    )


def arrived(part, sem):
    pltpu.make_async_copy(part, part, sem).wait()


def owner_groups(kv_n):
    return [(d, min(d + OWNERS, kv_n)) for d in range(1, kv_n, OWNERS)]


def kernel(
    kv_n, tp_n,
    tok_ref, wq_ref, wl_ref, qgain_ref, kgain_ref, vu_ref, w_ref, ogain_ref, chosen_ref, chosen_s,
    out_hbm,
    o_ref, tk_ref, wqs_ref, vus_ref, q_ref, lat_ref, out_ref, kvp_ref, kn_ref, vt_ref, bd_ref,
    map_ref, req_ref, chs_ref, map_s, chs_s,
    ho_ref, wc_ref, proj_ref, px_ref, ss_ref,
    lc, oc, t_s, tf_s, t_r, tf_r, c_s, c_r, ch_s, ch_r, b_s, b_r, k_s, k_r, kf_r, kr_r,
    w_s, w_r, y_s, y_r, h_s, h_r, p_s, p_r, s_s, s_r,
):
    kv, tp = lax.axis_index("kv"), lax.axis_index("tp")
    core, x = lax.rem(tp, 2), tp // 2
    sib = tp + 1 - 2 * core
    blocks, _, xs, piece, feat = tok_ref.shape
    width = wl_ref.shape[1]
    heads = wq_ref.shape[1] // width
    vdim = vu_ref.shape[1]
    slots = kvp_ref.shape[1]
    picks = chosen_ref.shape[1]
    cols = o_ref.shape[1]
    half = BLOCK // 2
    mine = blocks * piece
    per_row = LANES // blocks
    wrows = w_ref.shape[0] // RING
    y = lax.rem(kv, RING)

    def at_kv(other):
        return {"kv": other, "tp": tp}

    def at_tp(other):
        return {"kv": kv, "tp": other}

    def other_tp(d):
        return lax.rem(tp + d + tp_n, tp_n)

    barrier = pltpu.get_barrier_semaphore()
    for d in range(1, kv_n):
        pl.semaphore_signal(barrier, inc=1, device_id=at_kv(lax.rem(kv + d, kv_n)), device_id_type=MESH)
    for d in range(1, tp_n):
        pl.semaphore_signal(barrier, inc=1, device_id=at_tp(other_tp(d)), device_id_type=MESH)

    lane = lax.broadcasted_iota(jnp.int32, (blocks, LANES), 1)
    halves = map_ref.shape[0]
    table = chosen_ref[...]
    for g in range(halves):
        hit = jnp.zeros((blocks, LANES), jnp.int32)
        for c in range(picks):
            hit = jnp.where(table[:, c : c + 1] == lane + g * LANES, 1, hit)
        need = jnp.broadcast_to(jnp.max(hit, axis=0, keepdims=True), (blocks, LANES))
        rank = prefix_in_owner(need, lane, blocks, False)
        local = lane % blocks
        dist = kv - (lane // blocks + g * per_row)
        slot = jnp.where(dist == 0, local, blocks + (dist - 1) * PER_OWNER + rank)
        map_ref[g] = jnp.clip(slot, 0, slots - 1)[0:1]
        code = jnp.zeros((blocks, LANES), jnp.int32)
        for k in range(PER_OWNER):
            code = code + jnp.where((need > 0) & (rank == k), local * blocks**k, 0)
        req_ref[g] = prefix_in_owner(code, lane, blocks, True)[0:1]

    pltpu.make_async_copy(map_ref, map_s, lc.at[0]).start()
    pl.semaphore_wait(barrier, kv_n - 1 + tp_n - 1)

    def chip(i):
        return lax.rem(x + i + xs, xs)

    def same_core(i):
        return 2 * chip(i) + core

    def tokens_to(e, j):
        c = lax.rem(core + e % 2, 2)
        part = chip(e // 2 + j)
        return send(
            tok_ref.at[:, c, part], tk_ref.at[tp, part], (t_s.at[j], t_r.at[j]), at_tp(2 * chip(e // 2) + c)
        )

    beside = [e for e in range(1, tp_n) if e // 2 != 2]

    def tokens_on(j, way):
        step = 1 - 2 * way
        part = tk_ref.at[2 * chip(-step) + way, chip(step + j)]
        return send(part, part, (tf_s.at[0], tf_r.at[j]), at_tp(same_core(step)))

    def ask(d):
        owner = lax.rem(kv - d + kv_n, kv_n)
        return send(
            req_ref.at[owner // per_row], chs_ref.at[d - 1],
            (ch_s.at[0], ch_r.at[0]), at_kv(owner),
        )

    def serves(d):
        return kv + d < kv_n

    def weights_to(d):
        other = other_tp(d)
        part = w_ref.at[
            pl.ds(pl.multiple_of(y * wrows, wrows), wrows),
            pl.ds(pl.multiple_of(other // 2 * 2 * cols, 2 * cols), 2 * cols),
        ]
        return send(part, wc_ref.at[tp, y], (w_s.at[0], w_r.at[0]), at_tp(other))

    def weights_on(e):
        part = wc_ref.at[:, y]
        other = kv - y + lax.rem(y + e, RING)
        return send(part, part, (y_s.at[0], y_r.at[0]), at_kv(other))

    to_sib = [
        send(wq_ref, wqs_ref, (c_s.at[0], c_r.at[0]), at_tp(sib)),
        send(vu_ref, vus_ref, (c_s.at[1], c_r.at[1]), at_tp(sib)),
    ]

    for e in range(1, tp_n):
        tokens_to(e, 0).start()
    for d in range(1, kv_n):
        ask(d).start()

    for j in range(1, xs):
        for e in beside:
            tokens_to(e, j).start()
    for copy in to_sib:
        copy.start()
    for d in range(1, tp_n):
        weights_to(d).start()

    for p in range(xs):
        tk_ref[tp, p] = tok_ref[:, core, p]
    wc_ref[tp, y] = w_ref[
        pl.ds(pl.multiple_of(y * wrows, wrows), wrows), pl.ds(pl.multiple_of(x * 2 * cols, 2 * cols), 2 * cols)
    ]
    null = slots
    vt_ref[:, width:, :] = jnp.ones((slots + 1, ONES, BLOCK), jnp.bfloat16)
    kn_ref[null] = jnp.zeros((BLOCK, width), jnp.bfloat16)
    vt_ref[null] = jnp.zeros((width + ONES, BLOCK), jnp.bfloat16)
    bd_ref[...] = jnp.zeros_like(bd_ref)

    def features(p):
        return jnp.concatenate([tk_ref[t, p].reshape(mine, feat) for t in range(tp_n)], axis=1)

    def hand_tokens(j):
        if j:
            arrived(tk_ref.at[pl.ds(0, len(beside)), 0], t_r.at[j])
        if j != 1:
            tokens_on((j - 1) % xs, 0).start()
        if j < xs - 1:
            tokens_on(j + 1, 1).start()

    arrived(chs_ref, ch_r.at[0])
    to_smem = pltpu.make_async_copy(chs_ref, chs_s, lc.at[1])
    to_smem.start()
    arrived(tk_ref.at[pl.ds(0, tp_n - 1), 0], t_r.at[0])
    hand_tokens(0)
    lat = jnp.dot(features(x), wl_ref[...], preferred_element_type=jnp.float32).astype(jnp.bfloat16)
    lat_ref[...] = lat.reshape(blocks, piece, width)
    kvp_ref[tp, 0:blocks] = lat.reshape(blocks, piece, width)

    pltpu.make_async_copy(map_ref, map_s, lc.at[0]).wait()
    to_smem.wait()

    def slots_of(d):
        return pl.ds(blocks + (d - 1) * PER_OWNER, PER_OWNER)

    def give(d):
        return send(
            out_ref.at[d - 1], kvp_ref.at[tp, slots_of(d)], (b_s.at[0], b_r.at[(d - 1) // OWNERS]), at_kv(lax.rem(kv + d, kv_n))
        )

    at_lane = lax.rem(kv, per_row) * blocks + blocks - 1
    for d in range(1, kv_n):

        @pl.when(serves(d))
        def _(d=d):
            code = chs_s[d - 1, 0, at_lane]
            for k in range(PER_OWNER):
                out_ref[d - 1, k] = lat_ref[(code >> (3 * k)) & (blocks - 1)]
            give(d).start()

    remote = owner_groups(kv_n)
    groups = [(0, blocks)] + [
        (blocks + (a - 1) * PER_OWNER, (b - a) * PER_OWNER) for a, b in remote
    ]

    def halves_of(g):
        first, size = groups[g]
        cut = (size + 1) // 2
        return [pl.ds(first, cut), pl.ds(first + cut, size - cut)]

    def spread(g, i):
        part = kvp_ref.at[tp, pl.ds(*groups[g])]
        where = sib if i == 2 else same_core(1 - 2 * i)
        return send(part, part, (k_s.at[g], (kr_r if i == 2 else k_r).at[g]), at_tp(where))

    def pass_on(g, way):
        step = 1 - 2 * way
        part = kvp_ref.at[same_core(-step), halves_of(g)[way]]
        return send(part, part, (k_s.at[g], kf_r.at[g]), at_tp(same_core(step)))

    def relay(g, i):
        if i < 2:
            part = kvp_ref.at[same_core(2 * i - 1), pl.ds(*groups[g])]
        else:
            part = kvp_ref.at[same_core(2), halves_of(g)[i - 2]]
        return send(part, part, (k_s.at[g], kr_r.at[g]), at_tp(sib))

    def when_group(g, body):
        if g == 0:
            body()
        else:
            pl.when(kv >= remote[g - 1][0])(body)

    def spread_group(g):
        def body():
            if g:
                a, b = remote[g - 1]
                for n in range(1, b - a + 1):

                    @pl.when((kv >= b - 1) if n == b - a else (kv == a + n - 1))
                    def _(n=n):
                        arrived(kvp_ref.at[tp, pl.ds(groups[g][0], n * PER_OWNER)], b_r.at[g - 1])

            for i in range(3):
                spread(g, i).start()

        when_group(g, body)

    def pass_group(g):
        def body():
            arrived(kvp_ref.at[pl.ds(0, 2), pl.ds(*groups[g])], k_r.at[g])
            for i in range(2):
                pass_on(g, i).start()
                relay(g, i).start()

        when_group(g, body)

    def relay_group(g):
        def body():
            arrived(kvp_ref.at[0, pl.ds(*groups[g])], kf_r.at[g])
            for i in range(2):
                relay(g, i + 2).start()

        when_group(g, body)

    gain_k = kgain_ref[...]

    def norm_group(g):
        def body():
            arrived(kvp_ref.at[pl.ds(0, 4), pl.ds(*groups[g])], kr_r.at[g])

            first, size = groups[g]
            each = next(n for n in (4, 2, 1) if size % n == 0)

            @pl.loop(0, size // each)
            def _(i):
                for u in range(each):
                    slot = first + i * each + u
                    rows = jnp.concatenate(
                        [kvp_ref[p * 2 + c, slot] for c in range(2) for p in range(xs)], axis=0
                    )
                    kn_ref[slot] = rms_scale(rows, gain_k)
                    vt_ref[slot, 0:width, :] = rows.T

        when_group(g, body)

    gain_q = qgain_ref[...] * (width**-0.5 * 1.4426950408889634)

    def project(j):
        if j:
            arrived(tk_ref.at[pl.ds(0, 2), 0], tf_r.at[j])
        p = lax.rem(x + j, xs)
        rows = features(p)
        for w, at in ((wq_ref, core), (wqs_ref, 1 - core)):
            qs = jnp.dot(rows, w[...], preferred_element_type=jnp.float32).astype(jnp.bfloat16)
            for h in range(heads):
                part = rms_scale(qs[:, h * width : (h + 1) * width], gain_q)
                q_ref[at * heads + h, p] = part.reshape(blocks, piece, width)

    spread_group(0)
    for copy in to_sib:
        copy.wait()
    for v, at in ((vu_ref, core), (vus_ref, 1 - core)):
        for h in range(heads):
            bd_ref[at, h * vdim : (h + 1) * vdim, h * width : (h + 1) * width] = v[h]
    count = len(groups)
    project(0)
    for j in range(1, xs):
        hand_tokens(j)
    for step in range(1, count + 3):
        if step < count:
            spread_group(step)
        if step <= count:
            pass_group(step - 1)
        if 2 <= step <= count + 1:
            relay_group(step - 2)
        if 2 <= step <= xs:
            project(step - 1)
        if step >= 3:
            norm_group(step - 3)
        if step == 3:
            arrived(wc_ref.at[pl.ds(0, tp_n - 1), 0], w_r.at[0])
            for e in range(1, RING):
                weights_on(e).start()

    def listed(b, c):
        block = chosen_s[b, c]
        known = jnp.maximum(block, 0)
        return jnp.where(block < 0, null, map_s[known >> 7, 0, known & (LANES - 1)])

    def attend_block(b):
        q = jnp.concatenate([q_ref[h, p, b] for h in range(2 * heads) for p in range(xs)], axis=0)
        qt = q.T
        acc = jnp.zeros((width + ONES, 2 * heads * half), jnp.float32)
        for i in range(0, picks, STEP):
            at = [listed(b, i + k) for k in range(STEP)]
            keys = jnp.concatenate([kn_ref[s] for s in at], axis=0)
            s = jnp.dot(keys, qt, preferred_element_type=jnp.float32)
            if i == 0:
                key_row = lax.broadcasted_iota(jnp.int32, s.shape, 0)
                query_row = lax.broadcasted_iota(jnp.int32, s.shape, 1) % half + core * half
                s = jnp.where((key_row <= query_row) | (key_row >= BLOCK), s, masked_score)
            p = jnp.exp2(s).astype(jnp.bfloat16)
            values = jnp.concatenate([vt_ref[s] for s in at], axis=1)
            acc = acc + jnp.dot(values, p, preferred_element_type=jnp.float32)
        att = (acc[:width] / acc[width : width + 1]).astype(jnp.bfloat16).T
        out = []
        for h in range(0, 2 * heads, 2):
            two = jnp.concatenate([att[h * half : (h + 1) * half], att[(h + 1) * half : (h + 2) * half]], axis=1)
            out.append(
                lax.dot_general(two, bd_ref[h // 2], (((1,), (1,)), ((), ())), preferred_element_type=jnp.float32)
            )
        return jnp.concatenate(out, axis=1).astype(jnp.bfloat16)

    pairs = blocks // 2

    def heads_to(b, i):
        part = ho_ref.at[x, b]
        return send(part, part, (h_s.at[0], h_r.at[b // 2]), at_tp(same_core((2, 1, -1)[i])))

    def finish(g):
        arrived(ho_ref.at[pl.ds(0, xs - 1), pl.ds(0, 2)], h_r.at[g])
        total = jnp.zeros((BLOCK, 2 * cols), jnp.float32)
        for p in range(xs):
            rows = ho_ref[p, pl.ds(2 * g, 2)].reshape(BLOCK, 2 * cols)
            w = jnp.concatenate([wc_ref[2 * p + c].reshape(RING * wrows, 2 * cols) for c in range(2)], axis=0)
            total = total + jnp.dot(rows, w, preferred_element_type=jnp.float32)
        left, right = total[:, :cols], total[:, cols:]
        px_ref[g] = jnp.where(core == 0, right, left)
        proj_ref[g, core] = jnp.where(core == 0, left, right)
        squares = jnp.sum(total * total, axis=1, keepdims=True)
        ss_ref[tp, pl.ds(g, 1), :] = jnp.broadcast_to(squares, (BLOCK, BLOCK)).T[0:1]
        swap(g).start()

    def swap(g):
        return send(px_ref.at[g], proj_ref.at[g, core], (p_s.at[0], p_r.at[0]), at_tp(sib))

    @pl.loop(0, blocks)
    def _(b):
        ho_ref[x, b] = attend_block(b)
        for i in range(3):
            heads_to(b, i).start()

        @pl.when(b == 4)
        def _():
            arrived(wc_ref.at[:, pl.ds(0, RING - 1)], y_r.at[0])

        @pl.when((b >= 5) & (lax.rem(b, 2) == 1))
        def _():
            finish((b - 5) // 2)

    for g in range(max(pairs - 2, 0), pairs):
        finish(g)

    def sums(d):
        return send(ss_ref.at[tp], ss_ref.at[tp], (s_s.at[0], s_r.at[0]), at_tp(other_tp(d)))

    for d in range(1, tp_n):
        sums(d).start()

    for j in range(xs):
        arrived(tk_ref.at[pl.ds(0, len(beside) if j else tp_n - 1), 0], t_s.at[j])
    arrived(tk_ref.at[pl.ds(0, 2), pl.ds(0, xs - 1)], tf_s.at[0])
    arrived(chs_ref, ch_s.at[0])
    arrived(wc_ref.at[pl.ds(0, tp_n - 1), 0], w_s.at[0])
    arrived(wc_ref.at[:, pl.ds(0, RING - 1)], y_s.at[0])
    for n in range(1, kv_n):

        @pl.when(kv == kv_n - 1 - n)
        def _(n=n):
            arrived(out_ref.at[pl.ds(0, n)], b_s.at[0])

    for g in range(count):

        def drain(g=g):
            arrived(kvp_ref.at[pl.ds(0, 7), pl.ds(*groups[g])], k_s.at[g])

        when_group(g, drain)

    arrived(ho_ref.at[pl.ds(0, xs - 1)], h_s.at[0])
    arrived(px_ref, p_s.at[0])
    arrived(ss_ref.at[pl.ds(0, tp_n - 1)], s_s.at[0])
    arrived(px_ref, p_r.at[0])
    arrived(ss_ref.at[pl.ds(0, tp_n - 1)], s_r.at[0])
    gains = ogain_ref[:, pl.ds(pl.multiple_of(tp * cols, cols), cols)]
    inverse = []
    for c in range(2):
        total = ss_ref[c]
        for p in range(1, xs):
            total = total + ss_ref[2 * p + c]
        inverse.append(lax.rsqrt(total / (cols * tp_n) + epsilon))

    def store(g):
        part = pl.ds(2 * g * BLOCK, 2 * BLOCK)
        return pltpu.make_async_copy(o_ref.at[part], out_hbm.at[part], oc.at[0])

    for g in range(pairs):
        for c in range(2):
            scale = jnp.broadcast_to(inverse[c][g : g + 1], (BLOCK, BLOCK)).T
            scale = jnp.concatenate([scale] * (cols // BLOCK), axis=1)
            rows = (proj_ref[g, c] * scale * gains).astype(jnp.bfloat16)
            for u in range(2):
                o_ref[pl.ds((2 * g + u) * BLOCK + c * half, half), :] = rows[u * half : (u + 1) * half]
        store(g).start()
    arrived(o_ref, oc.at[0])


def on_device(
    tokens,
    query_weight,
    latent_weight,
    query_gain,
    key_gain,
    value_up,
    out_weight,
    out_gain,
    chosen,
):
    toks, feat = tokens.shape
    width = latent_weight.shape[1]
    heads = query_weight.shape[1] // width
    blocks = toks // BLOCK
    kv_n, tp_n = lax.axis_size("kv"), lax.axis_size("tp")
    cols = out_weight.shape[1] // tp_n
    hv = out_weight.shape[0]
    xs = tp_n // 2
    piece = BLOCK // tp_n
    slots = blocks + (kv_n - 1) * PER_OWNER
    halves = max(1, kv_n * blocks // LANES)
    count = 1 + len(owner_groups(kv_n))
    bf, f32, i32 = jnp.bfloat16, jnp.float32, jnp.int32
    dma = pltpu.SemaphoreType.DMA
    vmem = pl.BlockSpec(memory_space=pltpu.VMEM)
    near = len(owner_groups(kv_n))
    sems = [
        1, xs, 1, xs, xs, 2, 2, 1, 1, 1, near, count, count, count, count,
        1, 1, 1, 1, 1, blocks // 2, 1, 1, 1, 1,
    ]
    return pl.pallas_call(
        functools.partial(kernel, kv_n, tp_n),
        out_shape=jax.ShapeDtypeStruct((toks, cols), bf),
        in_specs=[vmem] * 9 + [pl.BlockSpec(memory_space=pltpu.SMEM)],
        out_specs=pl.BlockSpec(memory_space=pl.ANY),
        scratch_shapes=[
            pltpu.VMEM((toks, cols), bf),
            pltpu.VMEM((tp_n, xs, blocks, piece, feat), bf),
            pltpu.VMEM(query_weight.shape, bf),
            pltpu.VMEM((value_up.shape[0], value_up.shape[2], value_up.shape[1]), bf),
            pltpu.VMEM((2 * heads, xs, blocks, piece, width), bf),
            pltpu.VMEM((blocks, piece, width), bf),
            pltpu.VMEM((kv_n - 1, PER_OWNER, piece, width), bf),
            pltpu.VMEM((tp_n, slots, piece, width), bf),
            pltpu.VMEM((slots + 1, BLOCK, width), bf),
            pltpu.VMEM((slots + 1, width + ONES, BLOCK), bf),
            pltpu.VMEM((2, hv, 2 * width), bf),
            pltpu.VMEM((halves, 1, LANES), i32),
            pltpu.VMEM((halves, 1, LANES), i32),
            pltpu.VMEM((kv_n - 1, 1, LANES), i32),
            pltpu.SMEM((halves, 1, LANES), i32),
            pltpu.SMEM((kv_n - 1, 1, LANES), i32),
            pltpu.VMEM((xs, blocks, BLOCK // 2, 2 * hv), bf),
            pltpu.VMEM((tp_n, RING, hv // RING, 2 * cols), bf),
            pltpu.VMEM((blocks // 2, 2, BLOCK, cols), f32),
            pltpu.VMEM((blocks // 2, BLOCK, cols), f32),
            pltpu.VMEM((tp_n, blocks // 2, BLOCK), f32),
            dma((2,)), *[dma((n,)) for n in sems],
        ],
        compiler_params=pltpu.CompilerParams(
            collective_id=0, has_side_effects=True, vmem_limit_bytes=60 << 20
        ),
    )(
        tokens.reshape(blocks, 2, xs, piece, feat), query_weight, latent_weight, query_gain[None, :],
        key_gain[None, :], jnp.swapaxes(value_up, 1, 2), out_weight, out_gain[None, :], chosen, chosen,
    )


def solution(mesh):
    in_specs = (
        P("kv", "tp"),
        P(None, "tp"),
        P(),
        P(),
        P(),
        P("tp", None, None),
        P("tp", None),
        P(),
        P("kv", None),
    )
    out_specs = P("kv", "tp")
    return jax.shard_map(
        on_device, mesh=mesh, in_specs=in_specs, out_specs=out_specs, check_vma=False
    )
```

```python
import functools

import jax
import jax.numpy as jnp
from jax import lax
from jax.experimental import pallas as pl
from jax.experimental.pallas import tpu as pltpu
from jax.sharding import PartitionSpec as P

BLOCK = 128
PER_OWNER = 2
RING = 4
OWNERS = 8
STEP = 8
LANES = 128
ONES = 16
MESH = pl.DeviceIdType.MESH

epsilon = 1e-06
masked_score = -1e30


def rms_scale(values, gain_row):
    widened = values.astype(jnp.float32)
    mean_sq = jnp.mean(widened * widened, axis=-1, keepdims=True)
    return (widened * lax.rsqrt(mean_sq + epsilon) * gain_row).astype(jnp.bfloat16)


def prefix_in_owner(values, lane, blocks, inclusive):
    total = values if inclusive else jnp.zeros_like(values)
    for s in range(1, blocks):
        total = total + jnp.where(lane % blocks >= s, pltpu.roll(values, s, 1), 0)
    return total


def send(src, dst, sems, where):
    return pltpu.make_async_remote_copy(
        src_ref=src, dst_ref=dst, send_sem=sems[0], recv_sem=sems[1], device_id=where, device_id_type=MESH
    )


def arrived(part, sem):
    pltpu.make_async_copy(part, part, sem).wait()


def owner_groups(kv_n):
    return [(d, min(d + OWNERS, kv_n)) for d in range(1, kv_n, OWNERS)]


def kernel(
    kv_n, tp_n,
    tok_in, wq_in, wl_in, qgain_in, kgain_in, vu_in, w_in, ogain_in, chosen_in,
    o_ref,
    chosen_ref, chosen_s, tok_ref, wl_ref, wq_ref, vu_ref, w_ref, qgain_ref, kgain_ref, ogain_ref,
    tk_ref, wqs_ref, vus_ref, q_ref, lat_ref, out_ref, kvp_ref, kn_ref, vt_ref, bd_ref,
    map_ref, req_ref, chs_ref, map_s, chs_s,
    ho_ref, wc_ref, proj_ref, px_ref, ss_ref,
    in_s, lc, t_s, tf_s, t_r, tf_r, c_s, c_r, ch_s, ch_r, b_s, b_r, k_s, k_r, kf_r, kr_r,
    w_s, w_r, y_s, y_r, h_s, h_r, p_s, p_r, s_s, s_r,
):
    kv, tp = lax.axis_index("kv"), lax.axis_index("tp")
    core, x = lax.rem(tp, 2), tp // 2
    sib = tp + 1 - 2 * core
    blocks, _, xs, piece, feat = tok_ref.shape
    width = wl_ref.shape[1]
    heads = wq_ref.shape[1] // width
    vdim = vu_ref.shape[1]
    slots = kvp_ref.shape[1]
    picks = chosen_ref.shape[1]
    cols = o_ref.shape[1]
    half = BLOCK // 2
    mine = blocks * piece
    per_row = LANES // blocks
    wrows = w_ref.shape[0] // RING
    y = lax.rem(kv, RING)

    def at_kv(other):
        return {"kv": other, "tp": tp}

    def at_tp(other):
        return {"kv": kv, "tp": other}

    def other_tp(d):
        return lax.rem(tp + d + tp_n, tp_n)

    barrier = pltpu.get_barrier_semaphore()
    for d in range(1, kv_n):
        pl.semaphore_signal(barrier, inc=1, device_id=at_kv(lax.rem(kv + d, kv_n)), device_id_type=MESH)
    for d in range(1, tp_n):
        pl.semaphore_signal(barrier, inc=1, device_id=at_tp(other_tp(d)), device_id_type=MESH)

    loads = [
        pltpu.make_async_copy(a, b, in_s.at[i])
        for i, (a, b) in enumerate([
            (chosen_in, chosen_ref), (chosen_in, chosen_s), (tok_in, tok_ref), (wl_in, wl_ref), (wq_in, wq_ref),
            (vu_in, vu_ref), (w_in, w_ref), (qgain_in, qgain_ref), (kgain_in, kgain_ref), (ogain_in, ogain_ref),
        ])
    ]
    for load in loads:
        load.start()
    loads[0].wait()
    lane = lax.broadcasted_iota(jnp.int32, (blocks, LANES), 1)
    halves = map_ref.shape[0]
    table = chosen_ref[...]
    for g in range(halves):
        hit = jnp.zeros((blocks, LANES), jnp.int32)
        for c in range(picks):
            hit = jnp.where(table[:, c : c + 1] == lane + g * LANES, 1, hit)
        need = jnp.broadcast_to(jnp.max(hit, axis=0, keepdims=True), (blocks, LANES))
        rank = prefix_in_owner(need, lane, blocks, False)
        local = lane % blocks
        dist = kv - (lane // blocks + g * per_row)
        slot = jnp.where(dist == 0, local, blocks + (dist - 1) * PER_OWNER + rank)
        map_ref[g] = jnp.clip(slot, 0, slots - 1)[0:1]
        code = jnp.zeros((blocks, LANES), jnp.int32)
        for k in range(PER_OWNER):
            code = code + jnp.where((need > 0) & (rank == k), local * blocks**k, 0)
        req_ref[g] = prefix_in_owner(code, lane, blocks, True)[0:1]

    pltpu.make_async_copy(map_ref, map_s, lc.at[0]).start()
    for load in loads[1:]:
        load.wait()
    pl.semaphore_wait(barrier, kv_n - 1 + tp_n - 1)

    def chip(i):
        return lax.rem(x + i + xs, xs)

    def same_core(i):
        return 2 * chip(i) + core

    def tokens_to(e, j):
        c = lax.rem(core + e % 2, 2)
        part = chip(e // 2 + j)
        return send(
            tok_ref.at[:, c, part], tk_ref.at[tp, part], (t_s.at[j], t_r.at[j]), at_tp(2 * chip(e // 2) + c)
        )

    beside = [e for e in range(1, tp_n) if e // 2 != 2]

    def tokens_on(j, way):
        step = 1 - 2 * way
        part = tk_ref.at[2 * chip(-step) + way, chip(step + j)]
        return send(part, part, (tf_s.at[0], tf_r.at[j]), at_tp(same_core(step)))

    def ask(d):
        owner = lax.rem(kv - d + kv_n, kv_n)
        return send(
            req_ref.at[owner // per_row], chs_ref.at[d - 1],
            (ch_s.at[0], ch_r.at[0]), at_kv(owner),
        )

    def serves(d):
        return kv + d < kv_n

    def weights_to(d):
        other = other_tp(d)
        part = w_ref.at[
            pl.ds(pl.multiple_of(y * wrows, wrows), wrows),
            pl.ds(pl.multiple_of(other // 2 * 2 * cols, 2 * cols), 2 * cols),
        ]
        return send(part, wc_ref.at[tp, y], (w_s.at[0], w_r.at[0]), at_tp(other))

    def weights_on(e):
        part = wc_ref.at[:, y]
        other = kv - y + lax.rem(y + e, RING)
        return send(part, part, (y_s.at[0], y_r.at[0]), at_kv(other))

    to_sib = [
        send(wq_ref, wqs_ref, (c_s.at[0], c_r.at[0]), at_tp(sib)),
        send(vu_ref, vus_ref, (c_s.at[1], c_r.at[1]), at_tp(sib)),
    ]

    for e in range(1, tp_n):
        tokens_to(e, 0).start()
    for d in range(1, kv_n):

        @pl.when(kv - d >= 0)
        def _(d=d):
            ask(d).start()

    for j in range(1, xs):
        for e in beside:
            tokens_to(e, j).start()
    for copy in to_sib:
        copy.start()
    for d in range(1, tp_n):
        weights_to(d).start()

    for p in range(xs):
        tk_ref[tp, p] = tok_ref[:, core, p]
    wc_ref[tp, y] = w_ref[
        pl.ds(pl.multiple_of(y * wrows, wrows), wrows), pl.ds(pl.multiple_of(x * 2 * cols, 2 * cols), 2 * cols)
    ]
    null = slots
    vt_ref[:, width:, :] = jnp.ones((slots + 1, ONES, BLOCK), jnp.bfloat16)
    kn_ref[null] = jnp.zeros((BLOCK, width), jnp.bfloat16)
    vt_ref[null] = jnp.zeros((width + ONES, BLOCK), jnp.bfloat16)
    bd_ref[...] = jnp.zeros_like(bd_ref)

    def features(p):
        return jnp.concatenate([tk_ref[t, p].reshape(mine, feat) for t in range(tp_n)], axis=1)

    def hand_tokens(j):
        if j:
            arrived(tk_ref.at[pl.ds(0, len(beside)), 0], t_r.at[j])
        if j != 1:
            tokens_on((j - 1) % xs, 0).start()
        if j < xs - 1:
            tokens_on(j + 1, 1).start()

    for n in range(1, kv_n):

        @pl.when(kv == kv_n - 1 - n)
        def _(n=n):
            arrived(chs_ref.at[pl.ds(0, n)], ch_r.at[0])

    to_smem = pltpu.make_async_copy(chs_ref, chs_s, lc.at[1])
    to_smem.start()
    arrived(tk_ref.at[pl.ds(0, tp_n - 1), 0], t_r.at[0])
    hand_tokens(0)
    lat = jnp.dot(features(x), wl_ref[...], preferred_element_type=jnp.float32).astype(jnp.bfloat16)
    lat_ref[...] = lat.reshape(blocks, piece, width)
    kvp_ref[tp, 0:blocks] = lat.reshape(blocks, piece, width)

    pltpu.make_async_copy(map_ref, map_s, lc.at[0]).wait()
    to_smem.wait()

    def slots_of(d):
        return pl.ds(blocks + (d - 1) * PER_OWNER, PER_OWNER)

    def give(d):
        return send(
            out_ref.at[d - 1], kvp_ref.at[tp, slots_of(d)], (b_s.at[0], b_r.at[(d - 1) // OWNERS]), at_kv(lax.rem(kv + d, kv_n))
        )

    at_lane = lax.rem(kv, per_row) * blocks + blocks - 1
    for d in range(1, kv_n):

        @pl.when(serves(d))
        def _(d=d):
            code = chs_s[d - 1, 0, at_lane]
            for k in range(PER_OWNER):
                out_ref[d - 1, k] = lat_ref[(code >> (3 * k)) & (blocks - 1)]
            give(d).start()

    remote = owner_groups(kv_n)
    groups = [(0, blocks)] + [
        (blocks + (a - 1) * PER_OWNER, (b - a) * PER_OWNER) for a, b in remote
    ]

    def direct(g):
        return g == len(groups) - 1

    def halves_of(g):
        first, size = groups[g]
        cut = (size + 1) // 2
        return [pl.ds(first, cut), pl.ds(first + cut, size - cut)]

    def spread(g, i):
        part = kvp_ref.at[tp, pl.ds(*groups[g])]
        where = sib if i == 2 else same_core((1, -1, 0, 2)[i])
        return send(part, part, (k_s.at[g], (kr_r if i == 2 else k_r).at[g]), at_tp(where))

    def pass_on(g, way):
        step = 1 - 2 * way
        part = kvp_ref.at[same_core(-step), halves_of(g)[way]]
        return send(part, part, (k_s.at[g], kf_r.at[g]), at_tp(same_core(step)))

    def relay(g, i):
        if i < 2 or direct(g):
            part = kvp_ref.at[same_core((-1, 1, 2)[i]), pl.ds(*groups[g])]
        else:
            part = kvp_ref.at[same_core(2), halves_of(g)[i - 2]]
        return send(part, part, (k_s.at[g], kr_r.at[g]), at_tp(sib))

    def when_group(g, body):
        if g == 0:
            body()
        else:
            pl.when(kv >= remote[g - 1][0])(body)

    def spread_group(g):
        def body():
            if g:
                a, b = remote[g - 1]
                for n in range(1, b - a + 1):

                    @pl.when((kv >= b - 1) if n == b - a else (kv == a + n - 1))
                    def _(n=n):
                        arrived(kvp_ref.at[tp, pl.ds(groups[g][0], n * PER_OWNER)], b_r.at[g - 1])

            for i in range(3 + direct(g)):
                spread(g, i).start()

        when_group(g, body)

    def pass_group(g):
        def body():
            arrived(kvp_ref.at[pl.ds(0, 2 + direct(g)), pl.ds(*groups[g])], k_r.at[g])
            for i in range(2 + direct(g)):
                if not direct(g):
                    pass_on(g, i).start()
                relay(g, i).start()

        when_group(g, body)

    def relay_group(g):
        def body():
            arrived(kvp_ref.at[0, pl.ds(*groups[g])], kf_r.at[g])
            for i in range(2):
                relay(g, i + 2).start()

        when_group(g, body)

    gain_k = kgain_ref[...]

    def norm_group(g):
        def body():
            arrived(kvp_ref.at[pl.ds(0, 4), pl.ds(*groups[g])], kr_r.at[g])

            first, size = groups[g]
            each = next(n for n in (4, 2, 1) if size % n == 0)

            @pl.loop(0, size // each)
            def _(i):
                for u in range(each):
                    slot = first + i * each + u
                    rows = jnp.concatenate(
                        [kvp_ref[p * 2 + c, slot] for c in range(2) for p in range(xs)], axis=0
                    )
                    kn_ref[slot] = rms_scale(rows, gain_k)
                    vt_ref[slot, 0:width, :] = rows.T

        when_group(g, body)

    gain_q = qgain_ref[...] * (width**-0.5 * 1.4426950408889634)

    def project(j):
        if j:
            arrived(tk_ref.at[pl.ds(0, 2), 0], tf_r.at[j])
        p = lax.rem(x + j, xs)
        rows = features(p)
        for w, at in ((wq_ref, core), (wqs_ref, 1 - core)):
            qs = jnp.dot(rows, w[...], preferred_element_type=jnp.float32).astype(jnp.bfloat16)
            for h in range(heads):
                part = rms_scale(qs[:, h * width : (h + 1) * width], gain_q)
                q_ref[at * heads + h, p] = part.reshape(blocks, piece, width)

    spread_group(0)
    for copy in to_sib:
        copy.wait()
    for v, at in ((vu_ref, core), (vus_ref, 1 - core)):
        for h in range(heads):
            bd_ref[at, h * vdim : (h + 1) * vdim, h * width : (h + 1) * width] = v[h]
    count = len(groups)
    project(0)
    for j in range(1, xs):
        hand_tokens(j)
    def weights_step():
        arrived(wc_ref.at[pl.ds(0, tp_n - 1), 0], w_r.at[0])
        for e in range(1, RING):
            weights_on(e).start()

    normed = 0
    projected = 1
    for step in range(1, count + 1):
        if step < count:
            spread_group(step)
        if step < count or count == 1:
            pass_group(step - 1)
        if 2 <= step:
            relay_group(step - 2)
        if step >= 2 and projected < xs and step < count:
            project(projected)
            projected += 1
        if step == 3:
            weights_step()
        if step >= 4:
            norm_group(normed)
            normed += 1
    for j in range(projected, xs):
        project(j)
    if count < 4:
        weights_step()
    for g in range(normed, max(count - 2, 0)):
        norm_group(g)
    if count > 1:
        pass_group(count - 1)
    for g in range(max(normed, count - 2), count):
        norm_group(g)

    def listed(b, c):
        block = chosen_s[b, c]
        known = jnp.maximum(block, 0)
        return jnp.where(block < 0, null, map_s[known >> 7, 0, known & (LANES - 1)])

    def attend_block(b):
        q = jnp.concatenate([q_ref[h, p, b] for h in range(2 * heads) for p in range(xs)], axis=0)
        qt = q.T
        acc = jnp.zeros((width + ONES, 2 * heads * half), jnp.float32)
        for i in range(0, picks, STEP):
            at = [listed(b, i + k) for k in range(STEP)]
            keys = jnp.concatenate([kn_ref[s] for s in at], axis=0)
            s = jnp.dot(keys, qt, preferred_element_type=jnp.float32)
            if i == 0:
                key_row = lax.broadcasted_iota(jnp.int32, s.shape, 0)
                query_row = lax.broadcasted_iota(jnp.int32, s.shape, 1) % half + core * half
                s = jnp.where((key_row <= query_row) | (key_row >= BLOCK), s, masked_score)
            p = jnp.exp2(s).astype(jnp.bfloat16)
            values = jnp.concatenate([vt_ref[s] for s in at], axis=1)
            acc = acc + jnp.dot(values, p, preferred_element_type=jnp.float32)
        att = (acc[:width] / acc[width : width + 1]).astype(jnp.bfloat16).T
        out = []
        for h in range(0, 2 * heads, 2):
            two = jnp.concatenate([att[h * half : (h + 1) * half], att[(h + 1) * half : (h + 2) * half]], axis=1)
            out.append(
                lax.dot_general(two, bd_ref[h // 2], (((1,), (1,)), ((), ())), preferred_element_type=jnp.float32)
            )
        return jnp.concatenate(out, axis=1).astype(jnp.bfloat16)

    pairs = blocks // 2

    def heads_to(b, i):
        part = ho_ref.at[x, b]
        return send(part, part, (h_s.at[0], h_r.at[b // 2]), at_tp(same_core((2, 1, -1)[i])))

    def finish(g):
        arrived(ho_ref.at[pl.ds(0, xs - 1), pl.ds(0, 2)], h_r.at[g])
        total = jnp.zeros((BLOCK, 2 * cols), jnp.float32)
        for p in range(xs):
            rows = ho_ref[p, pl.ds(2 * g, 2)].reshape(BLOCK, 2 * cols)
            w = jnp.concatenate([wc_ref[2 * p + c].reshape(RING * wrows, 2 * cols) for c in range(2)], axis=0)
            total = total + jnp.dot(rows, w, preferred_element_type=jnp.float32)
        left, right = total[:, :cols], total[:, cols:]
        px_ref[g] = jnp.where(core == 0, right, left)
        proj_ref[g, core] = jnp.where(core == 0, left, right)
        squares = jnp.sum(total * total, axis=1, keepdims=True)
        ss_ref[tp, pl.ds(g, 1), :] = jnp.broadcast_to(squares, (BLOCK, BLOCK)).T[0:1]
        swap(g).start()

    def swap(g):
        return send(px_ref.at[g], proj_ref.at[g, core], (p_s.at[0], p_r.at[0]), at_tp(sib))

    @pl.loop(0, blocks)
    def _(b):
        ho_ref[x, b] = attend_block(b)
        for i in range(3):
            heads_to(b, i).start()

        @pl.when(b == 4)
        def _():
            arrived(wc_ref.at[:, pl.ds(0, RING - 1)], y_r.at[0])

        @pl.when((b >= 5) & (lax.rem(b, 2) == 1))
        def _():
            finish((b - 5) // 2)

    for g in range(max(pairs - 2, 0), pairs):
        finish(g)

    def sums(d):
        return send(ss_ref.at[tp], ss_ref.at[tp], (s_s.at[0], s_r.at[0]), at_tp(other_tp(d)))

    for d in range(1, tp_n):
        sums(d).start()

    for j in range(xs):
        arrived(tk_ref.at[pl.ds(0, len(beside) if j else tp_n - 1), 0], t_s.at[j])
    arrived(tk_ref.at[pl.ds(0, 2), pl.ds(0, xs - 1)], tf_s.at[0])
    for n in range(1, kv_n):

        @pl.when(kv == n)
        def _(n=n):
            arrived(chs_ref.at[pl.ds(0, n)], ch_s.at[0])

    arrived(wc_ref.at[pl.ds(0, tp_n - 1), 0], w_s.at[0])
    arrived(wc_ref.at[:, pl.ds(0, RING - 1)], y_s.at[0])
    for n in range(1, kv_n):

        @pl.when(kv == kv_n - 1 - n)
        def _(n=n):
            arrived(out_ref.at[pl.ds(0, n)], b_s.at[0])

    for g in range(count):

        def drain(g=g):
            arrived(kvp_ref.at[pl.ds(0, 7), pl.ds(*groups[g])], k_s.at[g])

        when_group(g, drain)

    arrived(ho_ref.at[pl.ds(0, xs - 1)], h_s.at[0])
    arrived(px_ref, p_s.at[0])
    arrived(ss_ref.at[pl.ds(0, tp_n - 1)], s_s.at[0])
    arrived(px_ref, p_r.at[0])
    arrived(ss_ref.at[pl.ds(0, tp_n - 1)], s_r.at[0])
    gains = ogain_ref[:, pl.ds(pl.multiple_of(tp * cols, cols), cols)]
    inverse = []
    for c in range(2):
        total = ss_ref[c]
        for p in range(1, xs):
            total = total + ss_ref[2 * p + c]
        inverse.append(lax.rsqrt(total / (cols * tp_n) + epsilon))

    for g in range(pairs):
        for c in range(2):
            scale = jnp.broadcast_to(inverse[c][g : g + 1], (BLOCK, BLOCK)).T
            scale = jnp.concatenate([scale] * (cols // BLOCK), axis=1)
            rows = (proj_ref[g, c] * scale * gains).astype(jnp.bfloat16)
            for u in range(2):
                o_ref[pl.ds((2 * g + u) * BLOCK + c * half, half), :] = rows[u * half : (u + 1) * half]


def on_device(
    tokens,
    query_weight,
    latent_weight,
    query_gain,
    key_gain,
    value_up,
    out_weight,
    out_gain,
    chosen,
):
    toks, feat = tokens.shape
    width = latent_weight.shape[1]
    heads = query_weight.shape[1] // width
    blocks = toks // BLOCK
    kv_n, tp_n = lax.axis_size("kv"), lax.axis_size("tp")
    cols = out_weight.shape[1] // tp_n
    hv = out_weight.shape[0]
    xs = tp_n // 2
    piece = BLOCK // tp_n
    slots = blocks + (kv_n - 1) * PER_OWNER
    halves = max(1, kv_n * blocks // LANES)
    count = 1 + len(owner_groups(kv_n))
    bf, f32, i32 = jnp.bfloat16, jnp.float32, jnp.int32
    dma = pltpu.SemaphoreType.DMA
    vmem = pl.BlockSpec(memory_space=pltpu.VMEM)
    near = len(owner_groups(kv_n))
    sems = [
        xs, 1, xs, xs, 2, 2, 1, 1, 1, near, count, count, count, count,
        1, 1, 1, 1, 1, blocks // 2, 1, 1, 1, 1,
    ]
    return pl.pallas_call(
        functools.partial(kernel, kv_n, tp_n),
        out_shape=jax.ShapeDtypeStruct((toks, cols), bf),
        in_specs=[pl.BlockSpec(memory_space=pltpu.HBM)] * 9,
        out_specs=vmem,
        scratch_shapes=[
            pltpu.VMEM(chosen.shape, i32),
            pltpu.SMEM(chosen.shape, i32),
            pltpu.VMEM((blocks, 2, xs, piece, feat), bf),
            pltpu.VMEM(latent_weight.shape, bf),
            pltpu.VMEM(query_weight.shape, bf),
            pltpu.VMEM((value_up.shape[0], value_up.shape[2], value_up.shape[1]), bf),
            pltpu.VMEM(out_weight.shape, bf),
            pltpu.VMEM((1, width), f32),
            pltpu.VMEM((1, width), f32),
            pltpu.VMEM((1, cols * tp_n), f32),
            pltpu.VMEM((tp_n, xs, blocks, piece, feat), bf),
            pltpu.VMEM(query_weight.shape, bf),
            pltpu.VMEM((value_up.shape[0], value_up.shape[2], value_up.shape[1]), bf),
            pltpu.VMEM((2 * heads, xs, blocks, piece, width), bf),
            pltpu.VMEM((blocks, piece, width), bf),
            pltpu.VMEM((kv_n - 1, PER_OWNER, piece, width), bf),
            pltpu.VMEM((tp_n, slots, piece, width), bf),
            pltpu.VMEM((slots + 1, BLOCK, width), bf),
            pltpu.VMEM((slots + 1, width + ONES, BLOCK), bf),
            pltpu.VMEM((2, hv, 2 * width), bf),
            pltpu.VMEM((halves, 1, LANES), i32),
            pltpu.VMEM((halves, 1, LANES), i32),
            pltpu.VMEM((kv_n - 1, 1, LANES), i32),
            pltpu.SMEM((halves, 1, LANES), i32),
            pltpu.SMEM((kv_n - 1, 1, LANES), i32),
            pltpu.VMEM((xs, blocks, BLOCK // 2, 2 * hv), bf),
            pltpu.VMEM((tp_n, RING, hv // RING, 2 * cols), bf),
            pltpu.VMEM((blocks // 2, 2, BLOCK, cols), f32),
            pltpu.VMEM((blocks // 2, BLOCK, cols), f32),
            pltpu.VMEM((tp_n, blocks // 2, BLOCK), f32),
            dma((10,)), dma((2,)), *[dma((n,)) for n in sems],
        ],
        compiler_params=pltpu.CompilerParams(
            collective_id=0, has_side_effects=True, vmem_limit_bytes=24 << 20
        ),
    )(*[
        pltpu.with_memory_space_constraint(a, pltpu.HBM)
        for a in (
            tokens.reshape(blocks, 2, xs, piece, feat), query_weight, latent_weight, query_gain[None, :],
            key_gain[None, :], jnp.swapaxes(value_up, 1, 2), out_weight, out_gain[None, :], chosen,
        )
    ])


def solution(mesh):
    in_specs = (
        P("kv", "tp"),
        P(None, "tp"),
        P(),
        P(),
        P(),
        P("tp", None, None),
        P("tp", None),
        P(),
        P("kv", None),
    )
    out_specs = P("kv", "tp")
    return jax.shard_map(
        on_device, mesh=mesh, in_specs=in_specs, out_specs=out_specs, check_vma=False
    )
```

```python
import functools

import jax
import jax.numpy as jnp
from jax import lax
from jax.experimental import pallas as pl
from jax.experimental.pallas import tpu as pltpu
from jax.sharding import PartitionSpec as P

BLOCK = 128
PER_OWNER = 2
RING = 4
OWNERS = 8
STEP = 8
LANES = 128
ONES = 16
MESH = pl.DeviceIdType.MESH

epsilon = 1e-06
masked_score = -1e30


def rms_scale(values, gain_row):
    widened = values.astype(jnp.float32)
    mean_sq = jnp.mean(widened * widened, axis=-1, keepdims=True)
    return (widened * lax.rsqrt(mean_sq + epsilon) * gain_row).astype(jnp.bfloat16)


def prefix_in_owner(values, lane, blocks, inclusive):
    total = values if inclusive else jnp.zeros_like(values)
    for s in range(1, blocks):
        total = total + jnp.where(lane % blocks >= s, pltpu.roll(values, s, 1), 0)
    return total


def send(src, dst, sems, where):
    return pltpu.make_async_remote_copy(
        src_ref=src, dst_ref=dst, send_sem=sems[0], recv_sem=sems[1], device_id=where, device_id_type=MESH
    )


def arrived(part, sem):
    pltpu.make_async_copy(part, part, sem).wait()


def owner_groups(kv_n):
    spans = [(d, min(d + OWNERS, kv_n)) for d in range(1, kv_n, OWNERS)]
    return spans[:1] + spans[:1:-1] + spans[1:2]


def kernel(
    kv_n, tp_n,
    tok_in, wq_in, wl_in, qgain_in, kgain_in, vu_in, w_in, ogain_in, chosen_in,
    o_ref,
    chosen_ref, chosen_s, tok_ref, wl_ref, wq_ref, vu_ref, w_ref, qgain_ref, kgain_ref, ogain_ref,
    tk_ref, wqs_ref, vus_ref, q_ref, lat_ref, out_ref, kvp_ref, kn_ref, vt_ref, bd_ref,
    map_ref, req_ref, chs_ref, map_s, chs_s,
    ho_ref, wc_ref, proj_ref, px_ref, ss_ref,
    in_s, lc, t_s, tf_s, t_r, tf_r, c_s, c_r, ch_s, ch_r, b_s, b_r, k_s, k_r, kf_r, kr_r,
    w_s, w_r, y_s, y_r, h_s, h_r, p_s, p_r, s_s, s_r,
):
    kv, tp = lax.axis_index("kv"), lax.axis_index("tp")
    core, x = lax.rem(tp, 2), tp // 2
    sib = tp + 1 - 2 * core
    blocks, _, xs, piece, feat = tok_ref.shape
    width = wl_ref.shape[1]
    heads = wq_ref.shape[1] // width
    vdim = vu_ref.shape[1]
    slots = kvp_ref.shape[1]
    picks = chosen_ref.shape[1]
    cols = o_ref.shape[1]
    half = BLOCK // 2
    mine = blocks * piece
    per_row = LANES // blocks
    wrows = w_ref.shape[0] // RING
    y = lax.rem(kv, RING)

    def at_kv(other):
        return {"kv": other, "tp": tp}

    def at_tp(other):
        return {"kv": kv, "tp": other}

    def other_tp(d):
        return lax.rem(tp + d + tp_n, tp_n)

    barrier = pltpu.get_barrier_semaphore()
    for d in range(1, kv_n):
        pl.semaphore_signal(barrier, inc=1, device_id=at_kv(lax.rem(kv + d, kv_n)), device_id_type=MESH)
    for d in range(1, tp_n):
        pl.semaphore_signal(barrier, inc=1, device_id=at_tp(other_tp(d)), device_id_type=MESH)

    loads = [
        pltpu.make_async_copy(a, b, in_s.at[i])
        for i, (a, b) in enumerate([
            (chosen_in, chosen_ref), (chosen_in, chosen_s), (tok_in, tok_ref), (wl_in, wl_ref), (wq_in, wq_ref),
            (vu_in, vu_ref), (w_in, w_ref), (qgain_in, qgain_ref), (kgain_in, kgain_ref), (ogain_in, ogain_ref),
        ])
    ]
    for load in loads:
        load.start()
    loads[0].wait()
    lane = lax.broadcasted_iota(jnp.int32, (blocks, LANES), 1)
    halves = map_ref.shape[0]
    table = chosen_ref[...]
    for g in range(halves):
        hit = jnp.zeros((blocks, LANES), jnp.int32)
        for c in range(picks):
            hit = jnp.where(table[:, c : c + 1] == lane + g * LANES, 1, hit)
        need = jnp.broadcast_to(jnp.max(hit, axis=0, keepdims=True), (blocks, LANES))
        rank = prefix_in_owner(need, lane, blocks, False)
        local = lane % blocks
        dist = kv - (lane // blocks + g * per_row)
        slot = jnp.where(dist == 0, local, blocks + (dist - 1) * PER_OWNER + rank)
        map_ref[g] = jnp.clip(slot, 0, slots - 1)[0:1]
        code = jnp.zeros((blocks, LANES), jnp.int32)
        for k in range(PER_OWNER):
            code = code + jnp.where((need > 0) & (rank == k), local * blocks**k, 0)
        req_ref[g] = prefix_in_owner(code, lane, blocks, True)[0:1]

    pltpu.make_async_copy(map_ref, map_s, lc.at[0]).start()
    for load in loads[1:]:
        load.wait()
    pl.semaphore_wait(barrier, kv_n - 1 + tp_n - 1)

    def chip(i):
        return lax.rem(x + i + xs, xs)

    def same_core(i):
        return 2 * chip(i) + core

    def tokens_to(e, j):
        c = lax.rem(core + e % 2, 2)
        part = chip(e // 2 + j)
        return send(
            tok_ref.at[:, c, part], tk_ref.at[tp, part], (t_s.at[j], t_r.at[j]), at_tp(2 * chip(e // 2) + c)
        )

    beside = [e for e in range(1, tp_n) if e // 2 != 2]

    def tokens_on(j, way):
        step = 1 - 2 * way
        part = tk_ref.at[2 * chip(-step) + way, chip(step + j)]
        return send(part, part, (tf_s.at[0], tf_r.at[j]), at_tp(same_core(step)))

    def ask(d):
        owner = lax.rem(kv - d + kv_n, kv_n)
        return send(
            req_ref.at[owner // per_row], chs_ref.at[d - 1],
            (ch_s.at[0], ch_r.at[0]), at_kv(owner),
        )

    def serves(d):
        return kv + d < kv_n

    def weights_to(d):
        other = other_tp(d)
        part = w_ref.at[
            pl.ds(pl.multiple_of(y * wrows, wrows), wrows),
            pl.ds(pl.multiple_of(other // 2 * 2 * cols, 2 * cols), 2 * cols),
        ]
        return send(part, wc_ref.at[tp, y], (w_s.at[0], w_r.at[0]), at_tp(other))

    def weights_on(e):
        part = wc_ref.at[:, y]
        other = kv - y + lax.rem(y + e, RING)
        return send(part, part, (y_s.at[0], y_r.at[0]), at_kv(other))

    to_sib = [
        send(wq_ref, wqs_ref, (c_s.at[0], c_r.at[0]), at_tp(sib)),
        send(vu_ref, vus_ref, (c_s.at[1], c_r.at[1]), at_tp(sib)),
    ]

    for e in (4, 5, 2, 3, 6, 7, 1):
        tokens_to(e, 0).start()
    for d in range(1, kv_n):

        @pl.when(kv - d >= 0)
        def _(d=d):
            ask(d).start()

    for j in range(1, xs):
        for e in beside:
            tokens_to(e, j).start()
    for copy in to_sib:
        copy.start()
    for p in range(xs):
        tk_ref[tp, p] = tok_ref[:, core, p]
    wc_ref[tp, y] = w_ref[
        pl.ds(pl.multiple_of(y * wrows, wrows), wrows), pl.ds(pl.multiple_of(x * 2 * cols, 2 * cols), 2 * cols)
    ]
    null = slots
    vt_ref[:, width:, :] = jnp.ones((slots + 1, ONES, BLOCK), jnp.bfloat16)
    kn_ref[null] = jnp.zeros((BLOCK, width), jnp.bfloat16)
    vt_ref[null] = jnp.zeros((width + ONES, BLOCK), jnp.bfloat16)
    bd_ref[...] = jnp.zeros_like(bd_ref)

    def features(p):
        return jnp.concatenate([tk_ref[t, p].reshape(mine, feat) for t in range(tp_n)], axis=1)

    def hand_tokens(j):
        if j:
            arrived(tk_ref.at[pl.ds(0, len(beside)), 0], t_r.at[j])
        if j != 1:
            tokens_on((j - 1) % xs, 0).start()
        if j < xs - 1:
            tokens_on(j + 1, 1).start()

    for n in range(1, kv_n):

        @pl.when(kv == kv_n - 1 - n)
        def _(n=n):
            arrived(chs_ref.at[pl.ds(0, n)], ch_r.at[0])

    to_smem = pltpu.make_async_copy(chs_ref, chs_s, lc.at[1])
    to_smem.start()
    arrived(tk_ref.at[pl.ds(0, tp_n - 1), 0], t_r.at[0])
    hand_tokens(0)
    lat = jnp.dot(features(x), wl_ref[...], preferred_element_type=jnp.float32).astype(jnp.bfloat16)
    lat_ref[...] = lat.reshape(blocks, piece, width)
    kvp_ref[tp, 0:blocks] = lat.reshape(blocks, piece, width)

    pltpu.make_async_copy(map_ref, map_s, lc.at[0]).wait()
    to_smem.wait()

    def slots_of(d):
        return pl.ds(blocks + (d - 1) * PER_OWNER, PER_OWNER)

    remote = owner_groups(kv_n)

    def span_of(d):
        return next(i for i, (a, b) in enumerate(remote) if a <= d < b)

    def give(d):
        return send(
            out_ref.at[d - 1], kvp_ref.at[tp, slots_of(d)], (b_s.at[0], b_r.at[span_of(d)]), at_kv(lax.rem(kv + d, kv_n))
        )

    at_lane = lax.rem(kv, per_row) * blocks + blocks - 1
    for d in range(1, kv_n):

        @pl.when(serves(d))
        def _(d=d):
            code = chs_s[d - 1, 0, at_lane]
            for k in range(PER_OWNER):
                out_ref[d - 1, k] = lat_ref[(code >> (3 * k)) & (blocks - 1)]
            give(d).start()

    groups = [(0, blocks)] + [
        (blocks + (a - 1) * PER_OWNER, (b - a) * PER_OWNER) for a, b in remote
    ]

    def direct(g):
        return g == len(groups) - 1

    def halves_of(g):
        first, size = groups[g]
        cut = (size + 1) // 2
        return [pl.ds(first, cut), pl.ds(first + cut, size - cut)]

    def spread(g, i):
        part = kvp_ref.at[tp, pl.ds(*groups[g])]
        where = sib if i == 2 else same_core((1, -1, 0, 2)[i])
        return send(part, part, (k_s.at[g], (kr_r if i == 2 else k_r).at[g]), at_tp(where))

    def pass_on(g, way):
        step = 1 - 2 * way
        part = kvp_ref.at[same_core(-step), halves_of(g)[way]]
        return send(part, part, (k_s.at[g], kf_r.at[g]), at_tp(same_core(step)))

    def relay(g, i):
        if i < 2 or direct(g):
            part = kvp_ref.at[same_core((-1, 1, 2)[i]), pl.ds(*groups[g])]
        else:
            part = kvp_ref.at[same_core(2), halves_of(g)[i - 2]]
        return send(part, part, (k_s.at[g], kr_r.at[g]), at_tp(sib))

    def when_group(g, body):
        if g == 0:
            body()
        else:
            pl.when(kv >= remote[g - 1][0])(body)

    def spread_group(g):
        def body():
            if g:
                a, b = remote[g - 1]
                for n in range(1, b - a + 1):

                    @pl.when((kv >= b - 1) if n == b - a else (kv == a + n - 1))
                    def _(n=n):
                        arrived(kvp_ref.at[tp, pl.ds(groups[g][0], n * PER_OWNER)], b_r.at[g - 1])

            for i in range(3 + direct(g)):
                spread(g, i).start()

        when_group(g, body)

    def pass_group(g):
        def body():
            arrived(kvp_ref.at[pl.ds(0, 2 + direct(g)), pl.ds(*groups[g])], k_r.at[g])
            for i in range(2 + direct(g)):
                if not direct(g):
                    pass_on(g, i).start()
                relay(g, i).start()

        when_group(g, body)

    def relay_group(g):
        def body():
            arrived(kvp_ref.at[0, pl.ds(*groups[g])], kf_r.at[g])
            for i in range(2):
                relay(g, i + 2).start()

        when_group(g, body)

    gain_k = kgain_ref[...]

    def norm_group(g):
        def body():
            arrived(kvp_ref.at[pl.ds(0, 4), pl.ds(*groups[g])], kr_r.at[g])

            first, size = groups[g]
            each = next(n for n in (4, 2, 1) if size % n == 0)

            @pl.loop(0, size // each)
            def _(i):
                for u in range(each):
                    slot = first + i * each + u
                    rows = jnp.concatenate(
                        [kvp_ref[p * 2 + c, slot] for c in range(2) for p in range(xs)], axis=0
                    )
                    kn_ref[slot] = rms_scale(rows, gain_k)
                    vt_ref[slot, 0:width, :] = rows.T

        when_group(g, body)

    gain_q = qgain_ref[...] * (width**-0.5 * 1.4426950408889634)

    def project(j):
        if j:
            arrived(tk_ref.at[pl.ds(0, 2), 0], tf_r.at[j])
        p = lax.rem(x + j, xs)
        rows = features(p)
        for w, at in ((wq_ref, core), (wqs_ref, 1 - core)):
            qs = jnp.dot(rows, w[...], preferred_element_type=jnp.float32).astype(jnp.bfloat16)
            for h in range(heads):
                part = rms_scale(qs[:, h * width : (h + 1) * width], gain_q)
                q_ref[at * heads + h, p] = part.reshape(blocks, piece, width)

    spread_group(0)
    for copy in to_sib:
        copy.wait()
    for v, at in ((vu_ref, core), (vus_ref, 1 - core)):
        for h in range(heads):
            bd_ref[at, h * vdim : (h + 1) * vdim, h * width : (h + 1) * width] = v[h]
    count = len(groups)
    project(0)
    for j in range(1, xs):
        hand_tokens(j)
    def weights_step():
        arrived(wc_ref.at[pl.ds(0, tp_n - 1), 0], w_r.at[0])
        for e in range(1, RING):
            weights_on(e).start()

    normed = 0
    projected = 1
    for step in range(1, count + 1):
        if step < count:
            spread_group(step)
        if step < count or count == 1:
            pass_group(step - 1)
        if 2 <= step:
            relay_group(step - 2)
        if step == min(2, count):
            for d in range(1, tp_n):
                weights_to(d).start()
        if step >= 2 and projected < xs and step < count:
            project(projected)
            projected += 1
        if step >= 4:
            norm_group(normed)
            normed += 1
    for j in range(projected, xs):
        project(j)
    for g in range(normed, max(count - 2, 0)):
        norm_group(g)
    weights_step()
    if count > 1:
        pass_group(count - 1)
    for g in range(max(normed, count - 2), count):
        norm_group(g)

    def listed(b, c):
        block = chosen_s[b, c]
        known = jnp.maximum(block, 0)
        return jnp.where(block < 0, null, map_s[known >> 7, 0, known & (LANES - 1)])

    def attend_block(b):
        q = jnp.concatenate([q_ref[h, p, b] for h in range(2 * heads) for p in range(xs)], axis=0)
        qt = q.T
        acc = jnp.zeros((width + ONES, 2 * heads * half), jnp.float32)
        for i in range(0, picks, STEP):
            at = [listed(b, i + k) for k in range(STEP)]
            keys = jnp.concatenate([kn_ref[s] for s in at], axis=0)
            s = jnp.dot(keys, qt, preferred_element_type=jnp.float32)
            if i == 0:
                key_row = lax.broadcasted_iota(jnp.int32, s.shape, 0)
                query_row = lax.broadcasted_iota(jnp.int32, s.shape, 1) % half + core * half
                s = jnp.where((key_row <= query_row) | (key_row >= BLOCK), s, masked_score)
            p = jnp.exp2(s).astype(jnp.bfloat16)
            values = jnp.concatenate([vt_ref[s] for s in at], axis=1)
            acc = acc + jnp.dot(values, p, preferred_element_type=jnp.float32)
        att = (acc[:width] / acc[width : width + 1]).astype(jnp.bfloat16).T
        out = []
        for h in range(0, 2 * heads, 2):
            two = jnp.concatenate([att[h * half : (h + 1) * half], att[(h + 1) * half : (h + 2) * half]], axis=1)
            out.append(
                lax.dot_general(two, bd_ref[h // 2], (((1,), (1,)), ((), ())), preferred_element_type=jnp.float32)
            )
        return jnp.concatenate(out, axis=1).astype(jnp.bfloat16)

    pairs = blocks // 2

    def heads_to(b, i):
        part = ho_ref.at[x, b]
        return send(part, part, (h_s.at[0], h_r.at[b // 2]), at_tp(same_core((2, 1, -1)[i])))

    def finish(g):
        arrived(ho_ref.at[pl.ds(0, xs - 1), pl.ds(0, 2)], h_r.at[g])
        total = jnp.zeros((BLOCK, 2 * cols), jnp.float32)
        for p in range(xs):
            rows = ho_ref[p, pl.ds(2 * g, 2)].reshape(BLOCK, 2 * cols)
            w = jnp.concatenate([wc_ref[2 * p + c].reshape(RING * wrows, 2 * cols) for c in range(2)], axis=0)
            total = total + jnp.dot(rows, w, preferred_element_type=jnp.float32)
        left, right = total[:, :cols], total[:, cols:]
        px_ref[g] = jnp.where(core == 0, right, left)
        proj_ref[g, core] = jnp.where(core == 0, left, right)
        squares = jnp.sum(total * total, axis=1, keepdims=True)
        ss_ref[tp, pl.ds(g, 1), :] = jnp.broadcast_to(squares, (BLOCK, BLOCK)).T[0:1]
        swap(g).start()

    def swap(g):
        return send(px_ref.at[g], proj_ref.at[g, core], (p_s.at[0], p_r.at[0]), at_tp(sib))

    @pl.loop(0, blocks)
    def _(b):
        ho_ref[x, b] = attend_block(b)
        for i in range(3):
            heads_to(b, i).start()

    arrived(wc_ref.at[:, pl.ds(0, RING - 1)], y_r.at[0])
    for g in range(pairs):
        finish(g)

    def sums(d):
        return send(ss_ref.at[tp], ss_ref.at[tp], (s_s.at[0], s_r.at[0]), at_tp(other_tp(d)))

    for d in range(1, tp_n):
        sums(d).start()

    for j in range(xs):
        arrived(tk_ref.at[pl.ds(0, len(beside) if j else tp_n - 1), 0], t_s.at[j])
    arrived(tk_ref.at[pl.ds(0, 2), pl.ds(0, xs - 1)], tf_s.at[0])
    for n in range(1, kv_n):

        @pl.when(kv == n)
        def _(n=n):
            arrived(chs_ref.at[pl.ds(0, n)], ch_s.at[0])

    arrived(wc_ref.at[pl.ds(0, tp_n - 1), 0], w_s.at[0])
    arrived(wc_ref.at[:, pl.ds(0, RING - 1)], y_s.at[0])
    for n in range(1, kv_n):

        @pl.when(kv == kv_n - 1 - n)
        def _(n=n):
            arrived(out_ref.at[pl.ds(0, n)], b_s.at[0])

    for g in range(count):

        def drain(g=g):
            arrived(kvp_ref.at[pl.ds(0, 7), pl.ds(*groups[g])], k_s.at[g])

        when_group(g, drain)

    arrived(ho_ref.at[pl.ds(0, xs - 1)], h_s.at[0])
    arrived(px_ref, p_s.at[0])
    arrived(ss_ref.at[pl.ds(0, tp_n - 1)], s_s.at[0])
    arrived(px_ref, p_r.at[0])
    arrived(ss_ref.at[pl.ds(0, tp_n - 1)], s_r.at[0])
    gains = ogain_ref[:, pl.ds(pl.multiple_of(tp * cols, cols), cols)]
    inverse = []
    for c in range(2):
        total = ss_ref[c]
        for p in range(1, xs):
            total = total + ss_ref[2 * p + c]
        inverse.append(lax.rsqrt(total / (cols * tp_n) + epsilon))

    for g in range(pairs):
        for c in range(2):
            scale = jnp.broadcast_to(inverse[c][g : g + 1], (BLOCK, BLOCK)).T
            scale = jnp.concatenate([scale] * (cols // BLOCK), axis=1)
            rows = (proj_ref[g, c] * scale * gains).astype(jnp.bfloat16)
            for u in range(2):
                o_ref[pl.ds((2 * g + u) * BLOCK + c * half, half), :] = rows[u * half : (u + 1) * half]


def on_device(
    tokens,
    query_weight,
    latent_weight,
    query_gain,
    key_gain,
    value_up,
    out_weight,
    out_gain,
    chosen,
):
    toks, feat = tokens.shape
    width = latent_weight.shape[1]
    heads = query_weight.shape[1] // width
    blocks = toks // BLOCK
    kv_n, tp_n = lax.axis_size("kv"), lax.axis_size("tp")
    cols = out_weight.shape[1] // tp_n
    hv = out_weight.shape[0]
    xs = tp_n // 2
    piece = BLOCK // tp_n
    slots = blocks + (kv_n - 1) * PER_OWNER
    halves = max(1, kv_n * blocks // LANES)
    count = 1 + len(owner_groups(kv_n))
    bf, f32, i32 = jnp.bfloat16, jnp.float32, jnp.int32
    dma = pltpu.SemaphoreType.DMA
    vmem = pl.BlockSpec(memory_space=pltpu.VMEM)
    near = len(owner_groups(kv_n))
    sems = [
        xs, 1, xs, xs, 2, 2, 1, 1, 1, near, count, count, count, count,
        1, 1, 1, 1, 1, blocks // 2, 1, 1, 1, 1,
    ]
    return pl.pallas_call(
        functools.partial(kernel, kv_n, tp_n),
        out_shape=jax.ShapeDtypeStruct((toks, cols), bf),
        in_specs=[pl.BlockSpec(memory_space=pltpu.HBM)] * 9,
        out_specs=vmem,
        scratch_shapes=[
            pltpu.VMEM(chosen.shape, i32),
            pltpu.SMEM(chosen.shape, i32),
            pltpu.VMEM((blocks, 2, xs, piece, feat), bf),
            pltpu.VMEM(latent_weight.shape, bf),
            pltpu.VMEM(query_weight.shape, bf),
            pltpu.VMEM((value_up.shape[0], value_up.shape[2], value_up.shape[1]), bf),
            pltpu.VMEM(out_weight.shape, bf),
            pltpu.VMEM((1, width), f32),
            pltpu.VMEM((1, width), f32),
            pltpu.VMEM((1, cols * tp_n), f32),
            pltpu.VMEM((tp_n, xs, blocks, piece, feat), bf),
            pltpu.VMEM(query_weight.shape, bf),
            pltpu.VMEM((value_up.shape[0], value_up.shape[2], value_up.shape[1]), bf),
            pltpu.VMEM((2 * heads, xs, blocks, piece, width), bf),
            pltpu.VMEM((blocks, piece, width), bf),
            pltpu.VMEM((kv_n - 1, PER_OWNER, piece, width), bf),
            pltpu.VMEM((tp_n, slots, piece, width), bf),
            pltpu.VMEM((slots + 1, BLOCK, width), bf),
            pltpu.VMEM((slots + 1, width + ONES, BLOCK), bf),
            pltpu.VMEM((2, hv, 2 * width), bf),
            pltpu.VMEM((halves, 1, LANES), i32),
            pltpu.VMEM((halves, 1, LANES), i32),
            pltpu.VMEM((kv_n - 1, 1, LANES), i32),
            pltpu.SMEM((halves, 1, LANES), i32),
            pltpu.SMEM((kv_n - 1, 1, LANES), i32),
            pltpu.VMEM((xs, blocks, BLOCK // 2, 2 * hv), bf),
            pltpu.VMEM((tp_n, RING, hv // RING, 2 * cols), bf),
            pltpu.VMEM((blocks // 2, 2, BLOCK, cols), f32),
            pltpu.VMEM((blocks // 2, BLOCK, cols), f32),
            pltpu.VMEM((tp_n, blocks // 2, BLOCK), f32),
            dma((10,)), dma((2,)), *[dma((n,)) for n in sems],
        ],
        compiler_params=pltpu.CompilerParams(
            collective_id=0, has_side_effects=True, vmem_limit_bytes=24 << 20
        ),
    )(*[
        pltpu.with_memory_space_constraint(a, pltpu.HBM)
        for a in (
            tokens.reshape(blocks, 2, xs, piece, feat), query_weight, latent_weight, query_gain[None, :],
            key_gain[None, :], jnp.swapaxes(value_up, 1, 2), out_weight, out_gain[None, :], chosen,
        )
    ])


def solution(mesh):
    in_specs = (
        P("kv", "tp"),
        P(None, "tp"),
        P(),
        P(),
        P(),
        P("tp", None, None),
        P("tp", None),
        P(),
        P("kv", None),
    )
    out_specs = P("kv", "tp")
    return jax.shard_map(
        on_device, mesh=mesh, in_specs=in_specs, out_specs=out_specs, check_vma=False
    )
```

```python
import functools

import jax
import jax.numpy as jnp
from jax import lax
from jax.experimental import pallas as pl
from jax.experimental.pallas import tpu as pltpu
from jax.sharding import PartitionSpec as P

BLOCK = 128
PER_OWNER = 2
RING = 4
OWNERS = 8
STEP = 8
LANES = 128
ONES = 16
MESH = pl.DeviceIdType.MESH

epsilon = 1e-06
masked_score = -1e30


def rms_scale(values, gain_row):
    widened = values.astype(jnp.float32)
    mean_sq = jnp.mean(widened * widened, axis=-1, keepdims=True)
    return (widened * lax.rsqrt(mean_sq + epsilon) * gain_row).astype(jnp.bfloat16)


def prefix_in_owner(values, lane, blocks, inclusive):
    total = values if inclusive else jnp.zeros_like(values)
    for s in range(1, blocks):
        total = total + jnp.where(lane % blocks >= s, pltpu.roll(values, s, 1), 0)
    return total


def send(src, dst, sems, where):
    return pltpu.make_async_remote_copy(
        src_ref=src, dst_ref=dst, send_sem=sems[0], recv_sem=sems[1], device_id=where, device_id_type=MESH
    )


def arrived(part, sem):
    pltpu.make_async_copy(part, part, sem).wait()


def owner_groups(kv_n):
    spans = [(d, min(d + OWNERS, kv_n)) for d in range(1, kv_n, OWNERS)]
    return spans[:1] + spans[:1:-1] + spans[1:2]


def kernel(
    kv_n, tp_n,
    tok_in, wq_in, wl_in, qgain_in, kgain_in, vu_in, w_in, ogain_in, chosen_in,
    o_ref,
    chosen_ref, chosen_s, tok_ref, wl_ref, wq_ref, vu_ref, w_ref, qgain_ref, kgain_ref, ogain_ref,
    tk_ref, wqs_ref, vus_ref, q_ref, lat_ref, out_ref, kvp_ref, kn_ref, vt_ref, bd_ref,
    map_ref, req_ref, chs_ref, map_s, chs_s,
    ho_ref, wc_ref, proj_ref, px_ref, ss_ref,
    in_s, lc, t_s, tf_s, t_r, tf_r, c_s, c_r, ch_s, ch_r, b_s, b_r, k_s, k_r, kf_r, kr_r,
    w_s, w_r, y_s, y_r, h_s, h_r, p_s, p_r, s_s, s_r,
):
    kv, tp = lax.axis_index("kv"), lax.axis_index("tp")
    core, x = lax.rem(tp, 2), tp // 2
    sib = tp + 1 - 2 * core
    blocks, _, xs, piece, feat = tok_ref.shape
    width = wl_ref.shape[1]
    heads = wq_ref.shape[1] // width
    vdim = vu_ref.shape[1]
    slots = kvp_ref.shape[1]
    picks = chosen_ref.shape[1]
    cols = o_ref.shape[1]
    half = BLOCK // 2
    mine = blocks * piece
    per_row = LANES // blocks
    wrows = w_ref.shape[0] // RING
    y = lax.rem(kv, RING)

    def at_kv(other):
        return {"kv": other, "tp": tp}

    def at_tp(other):
        return {"kv": kv, "tp": other}

    def other_tp(d):
        return lax.rem(tp + d + tp_n, tp_n)

    barrier = pltpu.get_barrier_semaphore()
    for d in range(1, kv_n):
        pl.semaphore_signal(barrier, inc=1, device_id=at_kv(lax.rem(kv + d, kv_n)), device_id_type=MESH)
    for d in range(1, tp_n):
        pl.semaphore_signal(barrier, inc=1, device_id=at_tp(other_tp(d)), device_id_type=MESH)

    loads = [
        pltpu.make_async_copy(a, b, in_s.at[i])
        for i, (a, b) in enumerate([
            (chosen_in, chosen_ref), (chosen_in, chosen_s), (tok_in, tok_ref), (wl_in, wl_ref), (wq_in, wq_ref),
            (vu_in, vu_ref), (w_in, w_ref), (qgain_in, qgain_ref), (kgain_in, kgain_ref), (ogain_in, ogain_ref),
        ])
    ]
    for load in loads:
        load.start()
    loads[0].wait()
    lane = lax.broadcasted_iota(jnp.int32, (blocks, LANES), 1)
    halves = map_ref.shape[0]
    table = chosen_ref[...]
    for g in range(halves):
        hit = jnp.zeros((blocks, LANES), jnp.int32)
        for c in range(picks):
            hit = jnp.where(table[:, c : c + 1] == lane + g * LANES, 1, hit)
        need = jnp.broadcast_to(jnp.max(hit, axis=0, keepdims=True), (blocks, LANES))
        rank = prefix_in_owner(need, lane, blocks, False)
        local = lane % blocks
        dist = kv - (lane // blocks + g * per_row)
        slot = jnp.where(dist == 0, local, blocks + (dist - 1) * PER_OWNER + rank)
        map_ref[g] = jnp.clip(slot, 0, slots - 1)[0:1]
        code = jnp.zeros((blocks, LANES), jnp.int32)
        for k in range(PER_OWNER):
            code = code + jnp.where((need > 0) & (rank == k), local * blocks**k, 0)
        req_ref[g] = prefix_in_owner(code, lane, blocks, True)[0:1]

    pltpu.make_async_copy(map_ref, map_s, lc.at[0]).start()
    for load in loads[1:]:
        load.wait()
    pl.semaphore_wait(barrier, kv_n - 1 + tp_n - 1)

    def chip(i):
        return lax.rem(x + i + xs, xs)

    def same_core(i):
        return 2 * chip(i) + core

    def tokens_to(e, j):
        c = lax.rem(core + e % 2, 2)
        part = chip(e // 2 + j)
        return send(
            tok_ref.at[:, c, part], tk_ref.at[tp, part], (t_s.at[j], t_r.at[j]), at_tp(2 * chip(e // 2) + c)
        )

    beside = [e for e in range(1, tp_n) if e // 2 != 2]

    def tokens_on(j, way):
        step = 1 - 2 * way
        part = tk_ref.at[2 * chip(-step) + way, chip(step + j)]
        return send(part, part, (tf_s.at[0], tf_r.at[j]), at_tp(same_core(step)))

    def ask(d):
        owner = lax.rem(kv - d + kv_n, kv_n)
        return send(
            req_ref.at[owner // per_row], chs_ref.at[d - 1],
            (ch_s.at[0], ch_r.at[0]), at_kv(owner),
        )

    def serves(d):
        return kv + d < kv_n

    def weights_to(d):
        other = other_tp(d)
        part = w_ref.at[
            pl.ds(pl.multiple_of(y * wrows, wrows), wrows),
            pl.ds(pl.multiple_of(other // 2 * 2 * cols, 2 * cols), 2 * cols),
        ]
        return send(part, wc_ref.at[tp, y], (w_s.at[0], w_r.at[0]), at_tp(other))

    def weights_on(e):
        part = wc_ref.at[:, y]
        other = kv - y + lax.rem(y + e, RING)
        return send(part, part, (y_s.at[0], y_r.at[0]), at_kv(other))

    to_sib = [
        send(wq_ref, wqs_ref, (c_s.at[0], c_r.at[0]), at_tp(sib)),
        send(vu_ref, vus_ref, (c_s.at[1], c_r.at[1]), at_tp(sib)),
    ]

    for e in (4, 5, 2, 3, 6, 7, 1):
        tokens_to(e, 0).start()
    for d in range(1, kv_n):

        @pl.when(kv - d >= 0)
        def _(d=d):
            ask(d).start()

    for j in range(1, xs):
        for e in beside:
            tokens_to(e, j).start()
    for copy in to_sib:
        copy.start()
    for p in range(xs):
        tk_ref[tp, p] = tok_ref[:, core, p]
    wc_ref[tp, y] = w_ref[
        pl.ds(pl.multiple_of(y * wrows, wrows), wrows), pl.ds(pl.multiple_of(x * 2 * cols, 2 * cols), 2 * cols)
    ]
    null = slots
    vt_ref[:, width:, :] = jnp.ones((slots + 1, ONES, BLOCK), jnp.bfloat16)
    kn_ref[null] = jnp.zeros((BLOCK, width), jnp.bfloat16)
    vt_ref[null] = jnp.zeros((width + ONES, BLOCK), jnp.bfloat16)
    bd_ref[...] = jnp.zeros_like(bd_ref)

    def features(p):
        return jnp.concatenate([tk_ref[t, p].reshape(mine, feat) for t in range(tp_n)], axis=1)

    def hand_tokens(j):
        if j:
            arrived(tk_ref.at[pl.ds(0, len(beside)), 0], t_r.at[j])
        if j != 1:
            tokens_on((j - 1) % xs, 0).start()
        if j < xs - 1:
            tokens_on(j + 1, 1).start()

    for n in range(1, kv_n):

        @pl.when(kv == kv_n - 1 - n)
        def _(n=n):
            arrived(chs_ref.at[pl.ds(0, n)], ch_r.at[0])

    to_smem = pltpu.make_async_copy(chs_ref, chs_s, lc.at[1])
    to_smem.start()
    arrived(tk_ref.at[pl.ds(0, tp_n - 1), 0], t_r.at[0])
    hand_tokens(0)
    lat = jnp.dot(features(x), wl_ref[...], preferred_element_type=jnp.float32).astype(jnp.bfloat16)
    lat_ref[...] = lat.reshape(blocks, piece, width)
    kvp_ref[tp, 0:blocks] = lat.reshape(blocks, piece, width)

    pltpu.make_async_copy(map_ref, map_s, lc.at[0]).wait()
    to_smem.wait()

    def slots_of(d):
        return pl.ds(blocks + (d - 1) * PER_OWNER, PER_OWNER)

    remote = owner_groups(kv_n)

    def span_of(d):
        return next(i for i, (a, b) in enumerate(remote) if a <= d < b)

    def give(d):
        return send(
            out_ref.at[d - 1], kvp_ref.at[tp, slots_of(d)], (b_s.at[0], b_r.at[span_of(d)]), at_kv(lax.rem(kv + d, kv_n))
        )

    at_lane = lax.rem(kv, per_row) * blocks + blocks - 1
    for d in range(1, kv_n):

        @pl.when(serves(d))
        def _(d=d):
            code = chs_s[d - 1, 0, at_lane]
            for k in range(PER_OWNER):
                out_ref[d - 1, k] = lat_ref[(code >> (3 * k)) & (blocks - 1)]
            give(d).start()

    groups = [(0, blocks)] + [
        (blocks + (a - 1) * PER_OWNER, (b - a) * PER_OWNER) for a, b in remote
    ]

    def direct(g):
        return g >= min(1, len(groups) - 1)

    def halves_of(g):
        first, size = groups[g]
        cut = (size + 1) // 2
        return [pl.ds(first, cut), pl.ds(first + cut, size - cut)]

    def spread(g, i):
        part = kvp_ref.at[tp, pl.ds(*groups[g])]
        where = sib if i == 2 else same_core((1, -1, 0, 2)[i])
        return send(part, part, (k_s.at[g], (kr_r if i == 2 else k_r).at[g]), at_tp(where))

    def pass_on(g, way):
        step = 1 - 2 * way
        part = kvp_ref.at[same_core(-step), halves_of(g)[way]]
        return send(part, part, (k_s.at[g], kf_r.at[g]), at_tp(same_core(step)))

    def relay(g, i):
        if i < 2 or direct(g):
            part = kvp_ref.at[same_core((-1, 1, 2)[i]), pl.ds(*groups[g])]
        else:
            part = kvp_ref.at[same_core(2), halves_of(g)[i - 2]]
        return send(part, part, (k_s.at[g], kr_r.at[g]), at_tp(sib))

    def when_group(g, body):
        if g == 0:
            body()
        else:
            pl.when(kv >= remote[g - 1][0])(body)

    def spread_group(g):
        def body():
            if g:
                a, b = remote[g - 1]
                for n in range(1, b - a + 1):

                    @pl.when((kv >= b - 1) if n == b - a else (kv == a + n - 1))
                    def _(n=n):
                        arrived(kvp_ref.at[tp, pl.ds(groups[g][0], n * PER_OWNER)], b_r.at[g - 1])

            for i in range(3 + direct(g)):
                spread(g, i).start()

        when_group(g, body)

    def pass_group(g):
        def body():
            arrived(kvp_ref.at[pl.ds(0, 2 + direct(g)), pl.ds(*groups[g])], k_r.at[g])
            for i in range(2 + direct(g)):
                if not direct(g):
                    pass_on(g, i).start()
                relay(g, i).start()

        when_group(g, body)

    def relay_group(g):
        def body():
            if not direct(g):
                arrived(kvp_ref.at[0, pl.ds(*groups[g])], kf_r.at[g])
                for i in range(2):
                    relay(g, i + 2).start()

        when_group(g, body)

    gain_k = kgain_ref[...]

    def norm_group(g):
        def body():
            arrived(kvp_ref.at[pl.ds(0, 4), pl.ds(*groups[g])], kr_r.at[g])

            first, size = groups[g]
            each = next(n for n in (4, 2, 1) if size % n == 0)

            @pl.loop(0, size // each)
            def _(i):
                for u in range(each):
                    slot = first + i * each + u
                    rows = jnp.concatenate(
                        [kvp_ref[p * 2 + c, slot] for c in range(2) for p in range(xs)], axis=0
                    )
                    kn_ref[slot] = rms_scale(rows, gain_k)
                    vt_ref[slot, 0:width, :] = rows.T

        when_group(g, body)

    gain_q = qgain_ref[...] * (width**-0.5 * 1.4426950408889634)

    def project(j):
        if j:
            arrived(tk_ref.at[pl.ds(0, 2), 0], tf_r.at[j])
        p = lax.rem(x + j, xs)
        rows = features(p)
        for w, at in ((wq_ref, core), (wqs_ref, 1 - core)):
            qs = jnp.dot(rows, w[...], preferred_element_type=jnp.float32).astype(jnp.bfloat16)
            for h in range(heads):
                part = rms_scale(qs[:, h * width : (h + 1) * width], gain_q)
                q_ref[at * heads + h, p] = part.reshape(blocks, piece, width)

    spread_group(0)
    for copy in to_sib:
        copy.wait()
    for v, at in ((vu_ref, core), (vus_ref, 1 - core)):
        for h in range(heads):
            bd_ref[at, h * vdim : (h + 1) * vdim, h * width : (h + 1) * width] = v[h]
    count = len(groups)
    project(0)
    for j in range(1, xs):
        hand_tokens(j)
    def weights_step():
        arrived(wc_ref.at[pl.ds(0, tp_n - 1), 0], w_r.at[0])
        for e in range(1, RING):
            weights_on(e).start()

    for g in range(1, count):
        spread_group(g)
        if g <= 2:
            pass_group(g - 1)
    if count < 3:
        pass_group(count - 1)
    for d in range(1, tp_n):
        weights_to(d).start()
    if not direct(0):
        relay_group(0)
    passed, normed = min(count, 2), 0
    for j in range(1, xs):
        project(j)
    norm_group(normed)
    normed += 1
    for g in range(passed, count):
        pass_group(g)
        if normed < g:
            norm_group(normed)
            normed += 1
    weights_step()
    for g in range(normed, count):
        norm_group(g)

    def listed(b, c):
        block = chosen_s[b, c]
        known = jnp.maximum(block, 0)
        return jnp.where(block < 0, null, map_s[known >> 7, 0, known & (LANES - 1)])

    def attend_block(b):
        q = jnp.concatenate([q_ref[h, p, b] for h in range(2 * heads) for p in range(xs)], axis=0)
        qt = q.T
        acc = jnp.zeros((width + ONES, 2 * heads * half), jnp.float32)
        for i in range(0, picks, STEP):
            at = [listed(b, i + k) for k in range(STEP)]
            keys = jnp.concatenate([kn_ref[s] for s in at], axis=0)
            s = jnp.dot(keys, qt, preferred_element_type=jnp.float32)
            if i == 0:
                key_row = lax.broadcasted_iota(jnp.int32, s.shape, 0)
                query_row = lax.broadcasted_iota(jnp.int32, s.shape, 1) % half + core * half
                s = jnp.where((key_row <= query_row) | (key_row >= BLOCK), s, masked_score)
            p = jnp.exp2(s).astype(jnp.bfloat16)
            values = jnp.concatenate([vt_ref[s] for s in at], axis=1)
            acc = acc + jnp.dot(values, p, preferred_element_type=jnp.float32)
        att = (acc[:width] / acc[width : width + 1]).astype(jnp.bfloat16).T
        out = []
        for h in range(0, 2 * heads, 2):
            two = jnp.concatenate([att[h * half : (h + 1) * half], att[(h + 1) * half : (h + 2) * half]], axis=1)
            out.append(
                lax.dot_general(two, bd_ref[h // 2], (((1,), (1,)), ((), ())), preferred_element_type=jnp.float32)
            )
        return jnp.concatenate(out, axis=1).astype(jnp.bfloat16)

    pairs = blocks // 2

    def heads_to(b, i):
        part = ho_ref.at[x, b]
        return send(part, part, (h_s.at[0], h_r.at[b // 2]), at_tp(same_core((2, 1, -1)[i])))

    def finish(g):
        arrived(ho_ref.at[pl.ds(0, xs - 1), pl.ds(0, 2)], h_r.at[g])
        total = jnp.zeros((BLOCK, 2 * cols), jnp.float32)
        for p in range(xs):
            rows = ho_ref[p, pl.ds(2 * g, 2)].reshape(BLOCK, 2 * cols)
            w = jnp.concatenate([wc_ref[2 * p + c].reshape(RING * wrows, 2 * cols) for c in range(2)], axis=0)
            total = total + jnp.dot(rows, w, preferred_element_type=jnp.float32)
        left, right = total[:, :cols], total[:, cols:]
        px_ref[g] = jnp.where(core == 0, right, left)
        proj_ref[g, core] = jnp.where(core == 0, left, right)
        squares = jnp.sum(total * total, axis=1, keepdims=True)
        ss_ref[tp, pl.ds(g, 1), :] = jnp.broadcast_to(squares, (BLOCK, BLOCK)).T[0:1]
        swap(g).start()

    def swap(g):
        return send(px_ref.at[g], proj_ref.at[g, core], (p_s.at[0], p_r.at[0]), at_tp(sib))

    @pl.loop(0, blocks)
    def _(b):
        ho_ref[x, b] = attend_block(b)
        for i in range(3):
            heads_to(b, i).start()

    arrived(wc_ref.at[:, pl.ds(0, RING - 1)], y_r.at[0])
    for g in range(pairs):
        finish(g)

    def sums(d):
        return send(ss_ref.at[tp], ss_ref.at[tp], (s_s.at[0], s_r.at[0]), at_tp(other_tp(d)))

    for d in range(1, tp_n):
        sums(d).start()

    for j in range(xs):
        arrived(tk_ref.at[pl.ds(0, len(beside) if j else tp_n - 1), 0], t_s.at[j])
    arrived(tk_ref.at[pl.ds(0, 2), pl.ds(0, xs - 1)], tf_s.at[0])
    for n in range(1, kv_n):

        @pl.when(kv == n)
        def _(n=n):
            arrived(chs_ref.at[pl.ds(0, n)], ch_s.at[0])

    arrived(wc_ref.at[pl.ds(0, tp_n - 1), 0], w_s.at[0])
    arrived(wc_ref.at[:, pl.ds(0, RING - 1)], y_s.at[0])
    for n in range(1, kv_n):

        @pl.when(kv == kv_n - 1 - n)
        def _(n=n):
            arrived(out_ref.at[pl.ds(0, n)], b_s.at[0])

    for g in range(count):

        def drain(g=g):
            arrived(kvp_ref.at[pl.ds(0, 7), pl.ds(*groups[g])], k_s.at[g])

        when_group(g, drain)

    arrived(ho_ref.at[pl.ds(0, xs - 1)], h_s.at[0])
    arrived(px_ref, p_s.at[0])
    arrived(ss_ref.at[pl.ds(0, tp_n - 1)], s_s.at[0])
    arrived(px_ref, p_r.at[0])
    arrived(ss_ref.at[pl.ds(0, tp_n - 1)], s_r.at[0])
    gains = ogain_ref[:, pl.ds(pl.multiple_of(tp * cols, cols), cols)]
    inverse = []
    for c in range(2):
        total = ss_ref[c]
        for p in range(1, xs):
            total = total + ss_ref[2 * p + c]
        inverse.append(lax.rsqrt(total / (cols * tp_n) + epsilon))

    for g in range(pairs):
        for c in range(2):
            scale = jnp.broadcast_to(inverse[c][g : g + 1], (BLOCK, BLOCK)).T
            scale = jnp.concatenate([scale] * (cols // BLOCK), axis=1)
            rows = (proj_ref[g, c] * scale * gains).astype(jnp.bfloat16)
            for u in range(2):
                o_ref[pl.ds((2 * g + u) * BLOCK + c * half, half), :] = rows[u * half : (u + 1) * half]


def on_device(
    tokens,
    query_weight,
    latent_weight,
    query_gain,
    key_gain,
    value_up,
    out_weight,
    out_gain,
    chosen,
):
    toks, feat = tokens.shape
    width = latent_weight.shape[1]
    heads = query_weight.shape[1] // width
    blocks = toks // BLOCK
    kv_n, tp_n = lax.axis_size("kv"), lax.axis_size("tp")
    cols = out_weight.shape[1] // tp_n
    hv = out_weight.shape[0]
    xs = tp_n // 2
    piece = BLOCK // tp_n
    slots = blocks + (kv_n - 1) * PER_OWNER
    halves = max(1, kv_n * blocks // LANES)
    count = 1 + len(owner_groups(kv_n))
    bf, f32, i32 = jnp.bfloat16, jnp.float32, jnp.int32
    dma = pltpu.SemaphoreType.DMA
    vmem = pl.BlockSpec(memory_space=pltpu.VMEM)
    near = len(owner_groups(kv_n))
    sems = [
        xs, 1, xs, xs, 2, 2, 1, 1, 1, near, count, count, count, count,
        1, 1, 1, 1, 1, blocks // 2, 1, 1, 1, 1,
    ]
    return pl.pallas_call(
        functools.partial(kernel, kv_n, tp_n),
        out_shape=jax.ShapeDtypeStruct((toks, cols), bf),
        in_specs=[pl.BlockSpec(memory_space=pltpu.HBM)] * 9,
        out_specs=vmem,
        scratch_shapes=[
            pltpu.VMEM(chosen.shape, i32),
            pltpu.SMEM(chosen.shape, i32),
            pltpu.VMEM((blocks, 2, xs, piece, feat), bf),
            pltpu.VMEM(latent_weight.shape, bf),
            pltpu.VMEM(query_weight.shape, bf),
            pltpu.VMEM((value_up.shape[0], value_up.shape[2], value_up.shape[1]), bf),
            pltpu.VMEM(out_weight.shape, bf),
            pltpu.VMEM((1, width), f32),
            pltpu.VMEM((1, width), f32),
            pltpu.VMEM((1, cols * tp_n), f32),
            pltpu.VMEM((tp_n, xs, blocks, piece, feat), bf),
            pltpu.VMEM(query_weight.shape, bf),
            pltpu.VMEM((value_up.shape[0], value_up.shape[2], value_up.shape[1]), bf),
            pltpu.VMEM((2 * heads, xs, blocks, piece, width), bf),
            pltpu.VMEM((blocks, piece, width), bf),
            pltpu.VMEM((kv_n - 1, PER_OWNER, piece, width), bf),
            pltpu.VMEM((tp_n, slots, piece, width), bf),
            pltpu.VMEM((slots + 1, BLOCK, width), bf),
            pltpu.VMEM((slots + 1, width + ONES, BLOCK), bf),
            pltpu.VMEM((2, hv, 2 * width), bf),
            pltpu.VMEM((halves, 1, LANES), i32),
            pltpu.VMEM((halves, 1, LANES), i32),
            pltpu.VMEM((kv_n - 1, 1, LANES), i32),
            pltpu.SMEM((halves, 1, LANES), i32),
            pltpu.SMEM((kv_n - 1, 1, LANES), i32),
            pltpu.VMEM((xs, blocks, BLOCK // 2, 2 * hv), bf),
            pltpu.VMEM((tp_n, RING, hv // RING, 2 * cols), bf),
            pltpu.VMEM((blocks // 2, 2, BLOCK, cols), f32),
            pltpu.VMEM((blocks // 2, BLOCK, cols), f32),
            pltpu.VMEM((tp_n, blocks // 2, BLOCK), f32),
            dma((10,)), dma((2,)), *[dma((n,)) for n in sems],
        ],
        compiler_params=pltpu.CompilerParams(
            collective_id=0, has_side_effects=True, vmem_limit_bytes=24 << 20
        ),
    )(*[
        pltpu.with_memory_space_constraint(a, pltpu.HBM)
        for a in (
            tokens.reshape(blocks, 2, xs, piece, feat), query_weight, latent_weight, query_gain[None, :],
            key_gain[None, :], jnp.swapaxes(value_up, 1, 2), out_weight, out_gain[None, :], chosen,
        )
    ])


def solution(mesh):
    in_specs = (
        P("kv", "tp"),
        P(None, "tp"),
        P(),
        P(),
        P(),
        P("tp", None, None),
        P("tp", None),
        P(),
        P("kv", None),
    )
    out_specs = P("kv", "tp")
    return jax.shard_map(
        on_device, mesh=mesh, in_specs=in_specs, out_specs=out_specs, check_vma=False
    )
```

```python
import functools

import jax
import jax.numpy as jnp
from jax import lax
from jax.experimental import pallas as pl
from jax.experimental.pallas import tpu as pltpu
from jax.sharding import PartitionSpec as P

BLOCK = 128
PER_OWNER = 2
RING = 4
OWNERS = 8
STEP = 8
LANES = 128
ONES = 16
MESH = pl.DeviceIdType.MESH

epsilon = 1e-06
masked_score = -1e30


def rms_scale(values, gain_row):
    widened = values.astype(jnp.float32)
    mean_sq = jnp.mean(widened * widened, axis=-1, keepdims=True)
    return (widened * lax.rsqrt(mean_sq + epsilon) * gain_row).astype(jnp.bfloat16)


def prefix_in_owner(values, lane, blocks, inclusive):
    total = values if inclusive else jnp.zeros_like(values)
    for s in range(1, blocks):
        total = total + jnp.where(lane % blocks >= s, pltpu.roll(values, s, 1), 0)
    return total


def send(src, dst, sems, where):
    return pltpu.make_async_remote_copy(
        src_ref=src, dst_ref=dst, send_sem=sems[0], recv_sem=sems[1], device_id=where, device_id_type=MESH
    )


def arrived(part, sem):
    pltpu.make_async_copy(part, part, sem).wait()


def owner_groups(kv_n):
    rising = [(d, min(d + OWNERS, kv_n)) for d in range(1, kv_n, OWNERS)]
    top = kv_n - RING
    if top <= 3 * OWNERS:
        return rising, rising
    return rising, [(1, 1 + OWNERS), (top - OWNERS, top), (1 + OWNERS, top - OWNERS)]


def kernel(
    kv_n, tp_n,
    tok_in, wq_in, wl_in, qgain_in, kgain_in, vu_in, w_in, ogain_in, chosen_in,
    o_ref,
    chosen_ref, chosen_s, tok_ref, wl_ref, wq_ref, vu_ref, w_ref, qgain_ref, kgain_ref, ogain_ref,
    tk_ref, wqs_ref, vus_ref, q_ref, lat_ref, out_ref, kvp_ref, kn_ref, vt_ref, bd_ref,
    map_ref, req_ref, chs_ref, map_s, chs_s,
    ho_ref, wc_ref, proj_ref, px_ref, ss_ref,
    in_s, lc, t_s, tf_s, t_r, tf_r, c_s, c_r, ch_s, ch_r, b_s, b_r, k_s, k_r, kf_r, kr_r,
    w_s, w_r, y_s, y_r, h_s, h_r, p_s, p_r, s_s, s_r,
):
    kv, tp = lax.axis_index("kv"), lax.axis_index("tp")
    core, x = lax.rem(tp, 2), tp // 2
    sib = tp + 1 - 2 * core
    blocks, _, xs, piece, feat = tok_ref.shape
    width = wl_ref.shape[1]
    heads = wq_ref.shape[1] // width
    vdim = vu_ref.shape[1]
    slots = kvp_ref.shape[1]
    picks = chosen_ref.shape[1]
    cols = o_ref.shape[1]
    half = BLOCK // 2
    mine = blocks * piece
    per_row = LANES // blocks
    wrows = w_ref.shape[0] // RING
    y = lax.rem(kv, RING)

    def at_kv(other):
        return {"kv": other, "tp": tp}

    def at_tp(other):
        return {"kv": kv, "tp": other}

    def other_tp(d):
        return lax.rem(tp + d + tp_n, tp_n)

    barrier = pltpu.get_barrier_semaphore()
    for d in range(1, kv_n):
        pl.semaphore_signal(barrier, inc=1, device_id=at_kv(lax.rem(kv + d, kv_n)), device_id_type=MESH)
    for d in range(1, tp_n):
        pl.semaphore_signal(barrier, inc=1, device_id=at_tp(other_tp(d)), device_id_type=MESH)

    loads = [
        pltpu.make_async_copy(a, b, in_s.at[i])
        for i, (a, b) in enumerate([
            (chosen_in, chosen_ref), (chosen_in, chosen_s), (tok_in, tok_ref), (wl_in, wl_ref), (wq_in, wq_ref),
            (vu_in, vu_ref), (w_in, w_ref), (qgain_in, qgain_ref), (kgain_in, kgain_ref), (ogain_in, ogain_ref),
        ])
    ]
    for load in loads:
        load.start()
    loads[0].wait()
    lane = lax.broadcasted_iota(jnp.int32, (blocks, LANES), 1)
    halves = map_ref.shape[0]
    table = chosen_ref[...]
    for g in range(halves):
        hit = jnp.zeros((blocks, LANES), jnp.int32)
        for c in range(picks):
            hit = jnp.where(table[:, c : c + 1] == lane + g * LANES, 1, hit)
        need = jnp.broadcast_to(jnp.max(hit, axis=0, keepdims=True), (blocks, LANES))
        rank = prefix_in_owner(need, lane, blocks, False)
        local = lane % blocks
        dist = kv - (lane // blocks + g * per_row)
        slot = jnp.where(dist == 0, local, blocks + (dist - 1) * PER_OWNER + rank)
        map_ref[g] = jnp.clip(slot, 0, slots - 1)[0:1]
        code = jnp.zeros((blocks, LANES), jnp.int32)
        for k in range(PER_OWNER):
            code = code + jnp.where((need > 0) & (rank == k), local * blocks**k, 0)
        req_ref[g] = prefix_in_owner(code, lane, blocks, True)[0:1]

    pltpu.make_async_copy(map_ref, map_s, lc.at[0]).start()
    for load in loads[1:]:
        load.wait()
    pl.semaphore_wait(barrier, kv_n - 1 + tp_n - 1)

    def chip(i):
        return lax.rem(x + i + xs, xs)

    def same_core(i):
        return 2 * chip(i) + core

    def tokens_to(e, j):
        c = lax.rem(core + e % 2, 2)
        part = chip(e // 2 + j)
        return send(
            tok_ref.at[:, c, part], tk_ref.at[tp, part], (t_s.at[j], t_r.at[j]), at_tp(2 * chip(e // 2) + c)
        )

    beside = [e for e in range(1, tp_n) if e // 2 != 2]

    def tokens_on(j, way):
        step = 1 - 2 * way
        part = tk_ref.at[2 * chip(-step) + way, chip(step + j)]
        return send(part, part, (tf_s.at[0], tf_r.at[j]), at_tp(same_core(step)))

    def ask(d):
        owner = lax.rem(kv - d + kv_n, kv_n)
        return send(
            req_ref.at[owner // per_row], chs_ref.at[d - 1],
            (ch_s.at[0], ch_r.at[0]), at_kv(owner),
        )

    def serves(d):
        return kv + d < kv_n

    def weights_to(d):
        other = other_tp(d)
        part = w_ref.at[
            pl.ds(pl.multiple_of(y * wrows, wrows), wrows),
            pl.ds(pl.multiple_of(other // 2 * 2 * cols, 2 * cols), 2 * cols),
        ]
        return send(part, wc_ref.at[tp, y], (w_s.at[0], w_r.at[0]), at_tp(other))

    def weights_on(e):
        part = wc_ref.at[:, y]
        other = kv - y + lax.rem(y + e, RING)
        return send(part, part, (y_s.at[0], y_r.at[0]), at_kv(other))

    to_sib = [
        send(wq_ref, wqs_ref, (c_s.at[0], c_r.at[0]), at_tp(sib)),
        send(vu_ref, vus_ref, (c_s.at[1], c_r.at[1]), at_tp(sib)),
    ]

    for e in (4, 5, 2, 3, 6, 7, 1):
        tokens_to(e, 0).start()
    for d in range(1, kv_n):

        @pl.when(kv - d >= 0)
        def _(d=d):
            ask(d).start()

    for j in range(1, xs):
        for e in beside:
            tokens_to(e, j).start()
    for copy in to_sib:
        copy.start()
    for p in range(xs):
        tk_ref[tp, p] = tok_ref[:, core, p]
    wc_ref[tp, y] = w_ref[
        pl.ds(pl.multiple_of(y * wrows, wrows), wrows), pl.ds(pl.multiple_of(x * 2 * cols, 2 * cols), 2 * cols)
    ]
    null = slots
    vt_ref[:, width:, :] = jnp.ones((slots + 1, ONES, BLOCK), jnp.bfloat16)
    kn_ref[null] = jnp.zeros((BLOCK, width), jnp.bfloat16)
    vt_ref[null] = jnp.zeros((width + ONES, BLOCK), jnp.bfloat16)
    bd_ref[...] = jnp.zeros_like(bd_ref)

    def features(p):
        return jnp.concatenate([tk_ref[t, p].reshape(mine, feat) for t in range(tp_n)], axis=1)

    def hand_tokens(j):
        if j:
            arrived(tk_ref.at[pl.ds(0, len(beside)), 0], t_r.at[j])
        if j != 1:
            tokens_on((j - 1) % xs, 0).start()
        if j < xs - 1:
            tokens_on(j + 1, 1).start()

    for n in range(1, kv_n):

        @pl.when(kv == kv_n - 1 - n)
        def _(n=n):
            arrived(chs_ref.at[pl.ds(0, n)], ch_r.at[0])

    to_smem = pltpu.make_async_copy(chs_ref, chs_s, lc.at[1])
    to_smem.start()
    arrived(tk_ref.at[pl.ds(0, tp_n - 1), 0], t_r.at[0])
    hand_tokens(0)
    lat = jnp.dot(features(x), wl_ref[...], preferred_element_type=jnp.float32).astype(jnp.bfloat16)
    lat_ref[...] = lat.reshape(blocks, piece, width)
    kvp_ref[tp, 0:blocks] = lat.reshape(blocks, piece, width)

    pltpu.make_async_copy(map_ref, map_s, lc.at[0]).wait()
    to_smem.wait()

    def slots_of(d):
        return pl.ds(blocks + (d - 1) * PER_OWNER, PER_OWNER)

    rising, split = owner_groups(kv_n)

    def span_of(d):
        index = [next((i for i, (a, b) in enumerate(spans) if a <= d < b), 0) for spans in (rising, split)]
        return jnp.where(kv + d >= kv_n - RING, index[0], index[1])

    def give(d):
        return send(
            out_ref.at[d - 1], kvp_ref.at[tp, slots_of(d)], (b_s.at[0], b_r.at[span_of(d)]), at_kv(lax.rem(kv + d, kv_n))
        )

    at_lane = lax.rem(kv, per_row) * blocks + blocks - 1
    for d in range(1, kv_n):

        @pl.when(serves(d))
        def _(d=d):
            code = chs_s[d - 1, 0, at_lane]
            for k in range(PER_OWNER):
                out_ref[d - 1, k] = lat_ref[(code >> (3 * k)) & (blocks - 1)]
            give(d).start()

    gain_k = kgain_ref[...]
    gain_q = qgain_ref[...] * (width**-0.5 * 1.4426950408889634)

    def project(j):
        if j:
            arrived(tk_ref.at[pl.ds(0, 2), 0], tf_r.at[j])
        p = lax.rem(x + j, xs)
        rows = features(p)
        for w, at in ((wq_ref, core), (wqs_ref, 1 - core)):
            qs = jnp.dot(rows, w[...], preferred_element_type=jnp.float32).astype(jnp.bfloat16)
            for h in range(heads):
                part = rms_scale(qs[:, h * width : (h + 1) * width], gain_q)
                q_ref[at * heads + h, p] = part.reshape(blocks, piece, width)

    def exchange(remote):
        groups = [(0, blocks)] + [
            (blocks + (a - 1) * PER_OWNER, (b - a) * PER_OWNER) for a, b in remote
        ]

        def direct(g):
            return g >= min(1, len(groups) - 1)

        def halves_of(g):
            first, size = groups[g]
            cut = (size + 1) // 2
            return [pl.ds(first, cut), pl.ds(first + cut, size - cut)]

        def spread(g, i):
            part = kvp_ref.at[tp, pl.ds(*groups[g])]
            where = sib if i == 2 else same_core((1, -1, 0, 2)[i])
            return send(part, part, (k_s.at[g], (kr_r if i == 2 else k_r).at[g]), at_tp(where))

        def pass_on(g, way):
            step = 1 - 2 * way
            part = kvp_ref.at[same_core(-step), halves_of(g)[way]]
            return send(part, part, (k_s.at[g], kf_r.at[g]), at_tp(same_core(step)))

        def relay(g, i):
            if i < 2 or direct(g):
                part = kvp_ref.at[same_core((-1, 1, 2)[i]), pl.ds(*groups[g])]
            else:
                part = kvp_ref.at[same_core(2), halves_of(g)[i - 2]]
            return send(part, part, (k_s.at[g], kr_r.at[g]), at_tp(sib))

        def when_group(g, body):
            if g == 0:
                body()
            else:
                pl.when(kv >= remote[g - 1][0])(body)

        def spread_group(g):
            def body():
                if g:
                    a, b = remote[g - 1]
                    for n in range(1, b - a + 1):

                        @pl.when((kv >= b - 1) if n == b - a else (kv == a + n - 1))
                        def _(n=n):
                            arrived(kvp_ref.at[tp, pl.ds(groups[g][0], n * PER_OWNER)], b_r.at[g - 1])

                for i in range(3 + direct(g)):
                    spread(g, i).start()

            when_group(g, body)

        def pass_group(g):
            def body():
                arrived(kvp_ref.at[pl.ds(0, 2 + direct(g)), pl.ds(*groups[g])], k_r.at[g])
                for i in range(2 + direct(g)):
                    if not direct(g):
                        pass_on(g, i).start()
                    relay(g, i).start()

            when_group(g, body)

        def relay_group(g):
            def body():
                if not direct(g):
                    arrived(kvp_ref.at[0, pl.ds(*groups[g])], kf_r.at[g])
                    for i in range(2):
                        relay(g, i + 2).start()

            when_group(g, body)

        def norm_group(g):
            def body():
                arrived(kvp_ref.at[pl.ds(0, 4), pl.ds(*groups[g])], kr_r.at[g])

                first, size = groups[g]
                each = next(n for n in (4, 2, 1) if size % n == 0)

                @pl.loop(0, size // each)
                def _(i):
                    for u in range(each):
                        slot = first + i * each + u
                        rows = jnp.concatenate(
                            [kvp_ref[p * 2 + c, slot] for c in range(2) for p in range(xs)], axis=0
                        )
                        kn_ref[slot] = rms_scale(rows, gain_k)
                        vt_ref[slot, 0:width, :] = rows.T

            when_group(g, body)

        spread_group(0)
        for copy in to_sib:
            copy.wait()
        for v, at in ((vu_ref, core), (vus_ref, 1 - core)):
            for h in range(heads):
                bd_ref[at, h * vdim : (h + 1) * vdim, h * width : (h + 1) * width] = v[h]
        count = len(groups)
        project(0)
        for j in range(1, xs):
            hand_tokens(j)
        def weights_step():
            arrived(wc_ref.at[pl.ds(0, tp_n - 1), 0], w_r.at[0])
            for e in range(1, RING):
                weights_on(e).start()

        for g in range(1, count):
            spread_group(g)
            if g <= 2:
                pass_group(g - 1)
        if count < 3:
            pass_group(count - 1)
        for d in range(1, tp_n):
            weights_to(d).start()
        if not direct(0):
            relay_group(0)
        passed, normed = min(count, 2), 0
        for j in range(1, xs):
            project(j)
        norm_group(normed)
        normed += 1
        for g in range(passed, count):
            pass_group(g)
            if normed < g:
                norm_group(normed)
                normed += 1
        weights_step()
        for g in range(normed, count):
            norm_group(g)


    @pl.when(kv >= kv_n - RING)
    def _():
        exchange(rising)

    @pl.when(kv < kv_n - RING)
    def _():
        exchange(split)

    def listed(b, c):
        block = chosen_s[b, c]
        known = jnp.maximum(block, 0)
        return jnp.where(block < 0, null, map_s[known >> 7, 0, known & (LANES - 1)])

    def attend_block(b):
        q = jnp.concatenate([q_ref[h, p, b] for h in range(2 * heads) for p in range(xs)], axis=0)
        qt = q.T
        acc = jnp.zeros((width + ONES, 2 * heads * half), jnp.float32)
        for i in range(0, picks, STEP):
            at = [listed(b, i + k) for k in range(STEP)]
            keys = jnp.concatenate([kn_ref[s] for s in at], axis=0)
            s = jnp.dot(keys, qt, preferred_element_type=jnp.float32)
            if i == 0:
                key_row = lax.broadcasted_iota(jnp.int32, s.shape, 0)
                query_row = lax.broadcasted_iota(jnp.int32, s.shape, 1) % half + core * half
                s = jnp.where((key_row <= query_row) | (key_row >= BLOCK), s, masked_score)
            p = jnp.exp2(s).astype(jnp.bfloat16)
            values = jnp.concatenate([vt_ref[s] for s in at], axis=1)
            acc = acc + jnp.dot(values, p, preferred_element_type=jnp.float32)
        att = (acc[:width] / acc[width : width + 1]).astype(jnp.bfloat16).T
        out = []
        for h in range(0, 2 * heads, 2):
            two = jnp.concatenate([att[h * half : (h + 1) * half], att[(h + 1) * half : (h + 2) * half]], axis=1)
            out.append(
                lax.dot_general(two, bd_ref[h // 2], (((1,), (1,)), ((), ())), preferred_element_type=jnp.float32)
            )
        return jnp.concatenate(out, axis=1).astype(jnp.bfloat16)

    pairs = blocks // 2

    def heads_to(b, i):
        part = ho_ref.at[x, b]
        return send(part, part, (h_s.at[0], h_r.at[b // 2]), at_tp(same_core((2, 1, -1)[i])))

    def finish(g):
        arrived(ho_ref.at[pl.ds(0, xs - 1), pl.ds(0, 2)], h_r.at[g])
        total = jnp.zeros((BLOCK, 2 * cols), jnp.float32)
        for p in range(xs):
            rows = ho_ref[p, pl.ds(2 * g, 2)].reshape(BLOCK, 2 * cols)
            w = jnp.concatenate([wc_ref[2 * p + c].reshape(RING * wrows, 2 * cols) for c in range(2)], axis=0)
            total = total + jnp.dot(rows, w, preferred_element_type=jnp.float32)
        left, right = total[:, :cols], total[:, cols:]
        px_ref[g] = jnp.where(core == 0, right, left)
        proj_ref[g, core] = jnp.where(core == 0, left, right)
        squares = jnp.sum(total * total, axis=1, keepdims=True)
        ss_ref[tp, pl.ds(g, 1), :] = jnp.broadcast_to(squares, (BLOCK, BLOCK)).T[0:1]
        swap(g).start()

    def swap(g):
        return send(px_ref.at[g], proj_ref.at[g, core], (p_s.at[0], p_r.at[0]), at_tp(sib))

    @pl.loop(0, blocks)
    def _(b):
        ho_ref[x, b] = attend_block(b)
        for i in range(3):
            heads_to(b, i).start()

    arrived(wc_ref.at[:, pl.ds(0, RING - 1)], y_r.at[0])
    for g in range(pairs):
        finish(g)

    def sums(d):
        return send(ss_ref.at[tp], ss_ref.at[tp], (s_s.at[0], s_r.at[0]), at_tp(other_tp(d)))

    for d in range(1, tp_n):
        sums(d).start()

    for j in range(xs):
        arrived(tk_ref.at[pl.ds(0, len(beside) if j else tp_n - 1), 0], t_s.at[j])
    arrived(tk_ref.at[pl.ds(0, 2), pl.ds(0, xs - 1)], tf_s.at[0])
    for n in range(1, kv_n):

        @pl.when(kv == n)
        def _(n=n):
            arrived(chs_ref.at[pl.ds(0, n)], ch_s.at[0])

    arrived(wc_ref.at[pl.ds(0, tp_n - 1), 0], w_s.at[0])
    arrived(wc_ref.at[:, pl.ds(0, RING - 1)], y_s.at[0])
    for n in range(1, kv_n):

        @pl.when(kv == kv_n - 1 - n)
        def _(n=n):
            arrived(out_ref.at[pl.ds(0, n)], b_s.at[0])

    def drain(remote):
        arrived(kvp_ref.at[pl.ds(0, 7), pl.ds(0, blocks)], k_s.at[0])
        for g, (a, b) in enumerate(remote):

            @pl.when(kv >= a)
            def _(g=g, a=a, b=b):
                part = pl.ds(blocks + (a - 1) * PER_OWNER, (b - a) * PER_OWNER)
                arrived(kvp_ref.at[pl.ds(0, 7), part], k_s.at[g + 1])

    @pl.when(kv >= kv_n - RING)
    def _():
        drain(rising)

    @pl.when(kv < kv_n - RING)
    def _():
        drain(split)

    arrived(ho_ref.at[pl.ds(0, xs - 1)], h_s.at[0])
    arrived(px_ref, p_s.at[0])
    arrived(ss_ref.at[pl.ds(0, tp_n - 1)], s_s.at[0])
    arrived(px_ref, p_r.at[0])
    arrived(ss_ref.at[pl.ds(0, tp_n - 1)], s_r.at[0])
    gains = ogain_ref[:, pl.ds(pl.multiple_of(tp * cols, cols), cols)]
    inverse = []
    for c in range(2):
        total = ss_ref[c]
        for p in range(1, xs):
            total = total + ss_ref[2 * p + c]
        inverse.append(lax.rsqrt(total / (cols * tp_n) + epsilon))

    for g in range(pairs):
        for c in range(2):
            scale = jnp.broadcast_to(inverse[c][g : g + 1], (BLOCK, BLOCK)).T
            scale = jnp.concatenate([scale] * (cols // BLOCK), axis=1)
            rows = (proj_ref[g, c] * scale * gains).astype(jnp.bfloat16)
            for u in range(2):
                o_ref[pl.ds((2 * g + u) * BLOCK + c * half, half), :] = rows[u * half : (u + 1) * half]


def on_device(
    tokens,
    query_weight,
    latent_weight,
    query_gain,
    key_gain,
    value_up,
    out_weight,
    out_gain,
    chosen,
):
    toks, feat = tokens.shape
    width = latent_weight.shape[1]
    heads = query_weight.shape[1] // width
    blocks = toks // BLOCK
    kv_n, tp_n = lax.axis_size("kv"), lax.axis_size("tp")
    cols = out_weight.shape[1] // tp_n
    hv = out_weight.shape[0]
    xs = tp_n // 2
    piece = BLOCK // tp_n
    slots = blocks + (kv_n - 1) * PER_OWNER
    halves = max(1, kv_n * blocks // LANES)
    count = 1 + len(owner_groups(kv_n)[0])
    bf, f32, i32 = jnp.bfloat16, jnp.float32, jnp.int32
    dma = pltpu.SemaphoreType.DMA
    vmem = pl.BlockSpec(memory_space=pltpu.VMEM)
    near = len(owner_groups(kv_n)[0])
    sems = [
        xs, 1, xs, xs, 2, 2, 1, 1, 1, near, count, count, count, count,
        1, 1, 1, 1, 1, blocks // 2, 1, 1, 1, 1,
    ]
    return pl.pallas_call(
        functools.partial(kernel, kv_n, tp_n),
        out_shape=jax.ShapeDtypeStruct((toks, cols), bf),
        in_specs=[pl.BlockSpec(memory_space=pltpu.HBM)] * 9,
        out_specs=vmem,
        scratch_shapes=[
            pltpu.VMEM(chosen.shape, i32),
            pltpu.SMEM(chosen.shape, i32),
            pltpu.VMEM((blocks, 2, xs, piece, feat), bf),
            pltpu.VMEM(latent_weight.shape, bf),
            pltpu.VMEM(query_weight.shape, bf),
            pltpu.VMEM((value_up.shape[0], value_up.shape[2], value_up.shape[1]), bf),
            pltpu.VMEM(out_weight.shape, bf),
            pltpu.VMEM((1, width), f32),
            pltpu.VMEM((1, width), f32),
            pltpu.VMEM((1, cols * tp_n), f32),
            pltpu.VMEM((tp_n, xs, blocks, piece, feat), bf),
            pltpu.VMEM(query_weight.shape, bf),
            pltpu.VMEM((value_up.shape[0], value_up.shape[2], value_up.shape[1]), bf),
            pltpu.VMEM((2 * heads, xs, blocks, piece, width), bf),
            pltpu.VMEM((blocks, piece, width), bf),
            pltpu.VMEM((kv_n - 1, PER_OWNER, piece, width), bf),
            pltpu.VMEM((tp_n, slots, piece, width), bf),
            pltpu.VMEM((slots + 1, BLOCK, width), bf),
            pltpu.VMEM((slots + 1, width + ONES, BLOCK), bf),
            pltpu.VMEM((2, hv, 2 * width), bf),
            pltpu.VMEM((halves, 1, LANES), i32),
            pltpu.VMEM((halves, 1, LANES), i32),
            pltpu.VMEM((kv_n - 1, 1, LANES), i32),
            pltpu.SMEM((halves, 1, LANES), i32),
            pltpu.SMEM((kv_n - 1, 1, LANES), i32),
            pltpu.VMEM((xs, blocks, BLOCK // 2, 2 * hv), bf),
            pltpu.VMEM((tp_n, RING, hv // RING, 2 * cols), bf),
            pltpu.VMEM((blocks // 2, 2, BLOCK, cols), f32),
            pltpu.VMEM((blocks // 2, BLOCK, cols), f32),
            pltpu.VMEM((tp_n, blocks // 2, BLOCK), f32),
            dma((10,)), dma((2,)), *[dma((n,)) for n in sems],
        ],
        compiler_params=pltpu.CompilerParams(
            collective_id=0, has_side_effects=True, vmem_limit_bytes=24 << 20
        ),
    )(*[
        pltpu.with_memory_space_constraint(a, pltpu.HBM)
        for a in (
            tokens.reshape(blocks, 2, xs, piece, feat), query_weight, latent_weight, query_gain[None, :],
            key_gain[None, :], jnp.swapaxes(value_up, 1, 2), out_weight, out_gain[None, :], chosen,
        )
    ])


def solution(mesh):
    in_specs = (
        P("kv", "tp"),
        P(None, "tp"),
        P(),
        P(),
        P(),
        P("tp", None, None),
        P("tp", None),
        P(),
        P("kv", None),
    )
    out_specs = P("kv", "tp")
    return jax.shard_map(
        on_device, mesh=mesh, in_specs=in_specs, out_specs=out_specs, check_vma=False
    )
```

```python
import functools

import jax
import jax.numpy as jnp
from jax import lax
from jax.experimental import pallas as pl
from jax.experimental.pallas import tpu as pltpu
from jax.sharding import PartitionSpec as P

BLOCK = 128
PER_OWNER = 2
RING = 4
OWNERS = 8
STEP = 8
LANES = 128
ONES = 16
MESH = pl.DeviceIdType.MESH

epsilon = 1e-06
masked_score = -1e30


def rms_scale(values, gain_row):
    widened = values.astype(jnp.float32)
    mean_sq = jnp.mean(widened * widened, axis=-1, keepdims=True)
    return (widened * lax.rsqrt(mean_sq + epsilon) * gain_row).astype(jnp.bfloat16)


def prefix_in_owner(values, lane, blocks, inclusive):
    total = values if inclusive else jnp.zeros_like(values)
    for s in range(1, blocks):
        total = total + jnp.where(lane % blocks >= s, pltpu.roll(values, s, 1), 0)
    return total


def send(src, dst, sems, where):
    return pltpu.make_async_remote_copy(
        src_ref=src, dst_ref=dst, send_sem=sems[0], recv_sem=sems[1], device_id=where, device_id_type=MESH
    )


def arrived(part, sem):
    pltpu.make_async_copy(part, part, sem).wait()


def owner_groups(kv_n):
    if kv_n != 8 * RING:
        return [(0, kv_n, [(d, min(d + OWNERS, kv_n)) for d in range(1, kv_n, OWNERS)])]
    return [
        (0, 8, [(1, 8)]),
        (8, 16, [(1, 7), (7, 12), (12, 16)]),
        (16, 20, [(1, 9), (9, 15), (15, 20)]),
        (20, 24, [(1, 9), (17, 24), (9, 13), (13, 17)]),
        (24, 28, [(1, 9), (20, 28), (9, 15), (15, 20)]),
        (28, 32, [(1, 9), (9, 17), (17, 25), (25, 32)]),
    ]


def kernel(
    kv_n, tp_n,
    tok_in, wq_in, wl_in, qgain_in, kgain_in, vu_in, w_in, ogain_in, chosen_in,
    o_ref,
    chosen_ref, chosen_s, tok_ref, wl_ref, wq_ref, vu_ref, w_ref, qgain_ref, kgain_ref, ogain_ref,
    tk_ref, wqs_ref, vus_ref, q_ref, lat_ref, out_ref, kvp_ref, kn_ref, vt_ref, bd_ref,
    map_ref, req_ref, chs_ref, map_s, chs_s,
    ho_ref, wc_ref, proj_ref, px_ref, ss_ref,
    in_s, lc, t_s, tf_s, t_r, tf_r, c_s, c_r, ch_s, ch_r, b_s, b_r, k_s, k_r, kf_r, kr_r,
    w_s, w_r, y_s, y_r, h_s, h_r, p_s, p_r, s_s, s_r,
):
    kv, tp = lax.axis_index("kv"), lax.axis_index("tp")
    core, x = lax.rem(tp, 2), tp // 2
    sib = tp + 1 - 2 * core
    blocks, _, xs, piece, feat = tok_ref.shape
    width = wl_ref.shape[1]
    heads = wq_ref.shape[1] // width
    vdim = vu_ref.shape[1]
    slots = kvp_ref.shape[1]
    picks = chosen_ref.shape[1]
    cols = o_ref.shape[1]
    half = BLOCK // 2
    mine = blocks * piece
    per_row = LANES // blocks
    wrows = w_ref.shape[0] // RING
    y = lax.rem(kv, RING)

    def at_kv(other):
        return {"kv": other, "tp": tp}

    def at_tp(other):
        return {"kv": kv, "tp": other}

    def other_tp(d):
        return lax.rem(tp + d + tp_n, tp_n)

    barrier = pltpu.get_barrier_semaphore()
    for d in range(1, kv_n):
        pl.semaphore_signal(barrier, inc=1, device_id=at_kv(lax.rem(kv + d, kv_n)), device_id_type=MESH)
    for d in range(1, tp_n):
        pl.semaphore_signal(barrier, inc=1, device_id=at_tp(other_tp(d)), device_id_type=MESH)

    loads = [
        pltpu.make_async_copy(a, b, in_s.at[i])
        for i, (a, b) in enumerate([
            (chosen_in, chosen_ref), (chosen_in, chosen_s), (tok_in, tok_ref), (wl_in, wl_ref), (wq_in, wq_ref),
            (vu_in, vu_ref), (w_in, w_ref), (qgain_in, qgain_ref), (kgain_in, kgain_ref), (ogain_in, ogain_ref),
        ])
    ]
    for load in loads:
        load.start()
    loads[0].wait()
    lane = lax.broadcasted_iota(jnp.int32, (blocks, LANES), 1)
    halves = map_ref.shape[0]
    table = chosen_ref[...]
    for g in range(halves):
        hit = jnp.zeros((blocks, LANES), jnp.int32)
        for c in range(picks):
            hit = jnp.where(table[:, c : c + 1] == lane + g * LANES, 1, hit)
        need = jnp.broadcast_to(jnp.max(hit, axis=0, keepdims=True), (blocks, LANES))
        rank = prefix_in_owner(need, lane, blocks, False)
        local = lane % blocks
        dist = kv - (lane // blocks + g * per_row)
        slot = jnp.where(dist == 0, local, blocks + (dist - 1) * PER_OWNER + rank)
        map_ref[g] = jnp.clip(slot, 0, slots - 1)[0:1]
        code = jnp.zeros((blocks, LANES), jnp.int32)
        for k in range(PER_OWNER):
            code = code + jnp.where((need > 0) & (rank == k), local * blocks**k, 0)
        req_ref[g] = prefix_in_owner(code, lane, blocks, True)[0:1]

    pltpu.make_async_copy(map_ref, map_s, lc.at[0]).start()
    for load in loads[1:]:
        load.wait()
    pl.semaphore_wait(barrier, kv_n - 1 + tp_n - 1)

    def chip(i):
        return lax.rem(x + i + xs, xs)

    def same_core(i):
        return 2 * chip(i) + core

    def tokens_to(e, j):
        c = lax.rem(core + e % 2, 2)
        part = chip(e // 2 + j)
        return send(
            tok_ref.at[:, c, part], tk_ref.at[tp, part], (t_s.at[j], t_r.at[j]), at_tp(2 * chip(e // 2) + c)
        )

    beside = [e for e in range(1, tp_n) if e // 2 != 2]

    def tokens_on(j, way):
        step = 1 - 2 * way
        part = tk_ref.at[2 * chip(-step) + way, chip(step + j)]
        return send(part, part, (tf_s.at[0], tf_r.at[j]), at_tp(same_core(step)))

    def ask(d):
        owner = lax.rem(kv - d + kv_n, kv_n)
        return send(
            req_ref.at[owner // per_row], chs_ref.at[d - 1],
            (ch_s.at[0], ch_r.at[0]), at_kv(owner),
        )

    def serves(d):
        return kv + d < kv_n

    def weights_to(d):
        other = other_tp(d)
        part = w_ref.at[
            pl.ds(pl.multiple_of(y * wrows, wrows), wrows),
            pl.ds(pl.multiple_of(other // 2 * 2 * cols, 2 * cols), 2 * cols),
        ]
        return send(part, wc_ref.at[tp, y], (w_s.at[0], w_r.at[0]), at_tp(other))

    def weights_on(e):
        part = wc_ref.at[:, y]
        other = kv - y + lax.rem(y + e, RING)
        return send(part, part, (y_s.at[0], y_r.at[0]), at_kv(other))

    to_sib = [
        send(wq_ref, wqs_ref, (c_s.at[0], c_r.at[0]), at_tp(sib)),
        send(vu_ref, vus_ref, (c_s.at[1], c_r.at[1]), at_tp(sib)),
    ]

    for e in (4, 5, 2, 3, 6, 7, 1):
        tokens_to(e, 0).start()
    for d in range(1, kv_n):

        @pl.when(kv - d >= 0)
        def _(d=d):
            ask(d).start()

    for j in range(1, xs):
        for e in beside:
            tokens_to(e, j).start()
    for copy in to_sib:
        copy.start()
    for p in range(xs):
        tk_ref[tp, p] = tok_ref[:, core, p]
    wc_ref[tp, y] = w_ref[
        pl.ds(pl.multiple_of(y * wrows, wrows), wrows), pl.ds(pl.multiple_of(x * 2 * cols, 2 * cols), 2 * cols)
    ]
    null = slots
    vt_ref[:, width:, :] = jnp.ones((slots + 1, ONES, BLOCK), jnp.bfloat16)
    kn_ref[null] = jnp.zeros((BLOCK, width), jnp.bfloat16)
    vt_ref[null] = jnp.zeros((width + ONES, BLOCK), jnp.bfloat16)
    bd_ref[...] = jnp.zeros_like(bd_ref)

    def features(p):
        return jnp.concatenate([tk_ref[t, p].reshape(mine, feat) for t in range(tp_n)], axis=1)

    def hand_tokens(j):
        if j:
            arrived(tk_ref.at[pl.ds(0, len(beside)), 0], t_r.at[j])
        if j != 1:
            tokens_on((j - 1) % xs, 0).start()
        if j < xs - 1:
            tokens_on(j + 1, 1).start()

    for n in range(1, kv_n):

        @pl.when(kv == kv_n - 1 - n)
        def _(n=n):
            arrived(chs_ref.at[pl.ds(0, n)], ch_r.at[0])

    to_smem = pltpu.make_async_copy(chs_ref, chs_s, lc.at[1])
    to_smem.start()
    arrived(tk_ref.at[pl.ds(0, tp_n - 1), 0], t_r.at[0])
    hand_tokens(0)
    lat = jnp.dot(features(x), wl_ref[...], preferred_element_type=jnp.float32).astype(jnp.bfloat16)
    lat_ref[...] = lat.reshape(blocks, piece, width)
    kvp_ref[tp, 0:blocks] = lat.reshape(blocks, piece, width)

    pltpu.make_async_copy(map_ref, map_s, lc.at[0]).wait()
    to_smem.wait()

    def slots_of(d):
        return pl.ds(blocks + (d - 1) * PER_OWNER, PER_OWNER)

    plans = owner_groups(kv_n)

    def span_of(d):
        index = 0
        for low, _, spans in plans:
            here = next((i for i, (a, b) in enumerate(spans) if a <= d < b), 0)
            index = jnp.where(kv + d >= low, here, index)
        return index

    def give(d):
        return send(
            out_ref.at[d - 1], kvp_ref.at[tp, slots_of(d)], (b_s.at[0], b_r.at[span_of(d)]), at_kv(lax.rem(kv + d, kv_n))
        )

    at_lane = lax.rem(kv, per_row) * blocks + blocks - 1
    for d in range(1, kv_n):

        @pl.when(serves(d))
        def _(d=d):
            code = chs_s[d - 1, 0, at_lane]
            for k in range(PER_OWNER):
                out_ref[d - 1, k] = lat_ref[(code >> (3 * k)) & (blocks - 1)]
            give(d).start()

    gain_k = kgain_ref[...]
    gain_q = qgain_ref[...] * (width**-0.5 * 1.4426950408889634)

    def project(j):
        if j:
            arrived(tk_ref.at[pl.ds(0, 2), 0], tf_r.at[j])
        p = lax.rem(x + j, xs)
        rows = features(p)
        for w, at in ((wq_ref, core), (wqs_ref, 1 - core)):
            qs = jnp.dot(rows, w[...], preferred_element_type=jnp.float32).astype(jnp.bfloat16)
            for h in range(heads):
                part = rms_scale(qs[:, h * width : (h + 1) * width], gain_q)
                q_ref[at * heads + h, p] = part.reshape(blocks, piece, width)

    def exchange(remote):
        groups = [(0, blocks)] + [
            (blocks + (a - 1) * PER_OWNER, (b - a) * PER_OWNER) for a, b in remote
        ]

        def direct(g):
            return g >= min(1, len(groups) - 1)

        def halves_of(g):
            first, size = groups[g]
            cut = (size + 1) // 2
            return [pl.ds(first, cut), pl.ds(first + cut, size - cut)]

        def spread(g, i):
            part = kvp_ref.at[tp, pl.ds(*groups[g])]
            where = sib if i == 2 else same_core((1, -1, 0, 2)[i])
            return send(part, part, (k_s.at[g], (kr_r if i == 2 else k_r).at[g]), at_tp(where))

        def pass_on(g, way):
            step = 1 - 2 * way
            part = kvp_ref.at[same_core(-step), halves_of(g)[way]]
            return send(part, part, (k_s.at[g], kf_r.at[g]), at_tp(same_core(step)))

        def relay(g, i):
            if i < 2 or direct(g):
                part = kvp_ref.at[same_core((-1, 1, 2)[i]), pl.ds(*groups[g])]
            else:
                part = kvp_ref.at[same_core(2), halves_of(g)[i - 2]]
            return send(part, part, (k_s.at[g], kr_r.at[g]), at_tp(sib))

        def when_group(g, body):
            if g == 0:
                body()
            else:
                pl.when(kv >= remote[g - 1][0])(body)

        def spread_group(g):
            def body():
                if g:
                    a, b = remote[g - 1]
                    for n in range(1, b - a + 1):

                        @pl.when((kv >= b - 1) if n == b - a else (kv == a + n - 1))
                        def _(n=n):
                            arrived(kvp_ref.at[tp, pl.ds(groups[g][0], n * PER_OWNER)], b_r.at[g - 1])

                for i in range(3 + direct(g)):
                    spread(g, i).start()

            when_group(g, body)

        def pass_group(g):
            def body():
                arrived(kvp_ref.at[pl.ds(0, 2 + direct(g)), pl.ds(*groups[g])], k_r.at[g])
                for i in range(2 + direct(g)):
                    if not direct(g):
                        pass_on(g, i).start()
                    relay(g, i).start()

            when_group(g, body)

        def relay_group(g):
            def body():
                if not direct(g):
                    arrived(kvp_ref.at[0, pl.ds(*groups[g])], kf_r.at[g])
                    for i in range(2):
                        relay(g, i + 2).start()

            when_group(g, body)

        def norm_group(g):
            def body():
                arrived(kvp_ref.at[pl.ds(0, 4), pl.ds(*groups[g])], kr_r.at[g])

                first, size = groups[g]
                each = next(n for n in (4, 2, 1) if size % n == 0)

                @pl.loop(0, size // each)
                def _(i):
                    for u in range(each):
                        slot = first + i * each + u
                        rows = jnp.concatenate(
                            [kvp_ref[p * 2 + c, slot] for c in range(2) for p in range(xs)], axis=0
                        )
                        kn_ref[slot] = rms_scale(rows, gain_k)
                        vt_ref[slot, 0:width, :] = rows.T

            when_group(g, body)

        spread_group(0)
        for copy in to_sib:
            copy.wait()
        for v, at in ((vu_ref, core), (vus_ref, 1 - core)):
            for h in range(heads):
                bd_ref[at, h * vdim : (h + 1) * vdim, h * width : (h + 1) * width] = v[h]
        count = len(groups)
        project(0)
        for j in range(1, xs):
            hand_tokens(j)
        def weights_step():
            arrived(wc_ref.at[pl.ds(0, tp_n - 1), 0], w_r.at[0])
            for e in range(1, RING):
                weights_on(e).start()

        for g in range(1, count):
            spread_group(g)
            if g <= 2:
                pass_group(g - 1)
        if count < 3:
            pass_group(count - 1)
        for d in range(1, tp_n):
            weights_to(d).start()
        if not direct(0):
            relay_group(0)
        passed, normed = min(count, 2), 0
        for j in range(1, xs):
            project(j)
        norm_group(normed)
        normed += 1
        for g in range(passed, count):
            pass_group(g)
            if normed < g:
                norm_group(normed)
                normed += 1
        weights_step()
        for g in range(normed, count):
            norm_group(g)


    for low, high, spans in plans:

        @pl.when((kv >= low) & (kv < high))
        def _(spans=spans):
            exchange(spans)

    def listed(b, c):
        block = chosen_s[b, c]
        known = jnp.maximum(block, 0)
        return jnp.where(block < 0, null, map_s[known >> 7, 0, known & (LANES - 1)])

    def attend_block(b):
        q = jnp.concatenate([q_ref[h, p, b] for h in range(2 * heads) for p in range(xs)], axis=0)
        qt = q.T
        acc = jnp.zeros((width + ONES, 2 * heads * half), jnp.float32)
        for i in range(0, picks, STEP):
            at = [listed(b, i + k) for k in range(STEP)]
            keys = jnp.concatenate([kn_ref[s] for s in at], axis=0)
            s = jnp.dot(keys, qt, preferred_element_type=jnp.float32)
            if i == 0:
                key_row = lax.broadcasted_iota(jnp.int32, s.shape, 0)
                query_row = lax.broadcasted_iota(jnp.int32, s.shape, 1) % half + core * half
                s = jnp.where((key_row <= query_row) | (key_row >= BLOCK), s, masked_score)
            p = jnp.exp2(s).astype(jnp.bfloat16)
            values = jnp.concatenate([vt_ref[s] for s in at], axis=1)
            acc = acc + jnp.dot(values, p, preferred_element_type=jnp.float32)
        att = (acc[:width] / acc[width : width + 1]).astype(jnp.bfloat16).T
        out = []
        for h in range(0, 2 * heads, 2):
            two = jnp.concatenate([att[h * half : (h + 1) * half], att[(h + 1) * half : (h + 2) * half]], axis=1)
            out.append(
                lax.dot_general(two, bd_ref[h // 2], (((1,), (1,)), ((), ())), preferred_element_type=jnp.float32)
            )
        return jnp.concatenate(out, axis=1).astype(jnp.bfloat16)

    pairs = blocks // 2

    def heads_to(b, i):
        part = ho_ref.at[x, b]
        return send(part, part, (h_s.at[0], h_r.at[b // 2]), at_tp(same_core((2, 1, -1)[i])))

    def finish(g):
        arrived(ho_ref.at[pl.ds(0, xs - 1), pl.ds(0, 2)], h_r.at[g])
        total = jnp.zeros((BLOCK, 2 * cols), jnp.float32)
        for p in range(xs):
            rows = ho_ref[p, pl.ds(2 * g, 2)].reshape(BLOCK, 2 * cols)
            w = jnp.concatenate([wc_ref[2 * p + c].reshape(RING * wrows, 2 * cols) for c in range(2)], axis=0)
            total = total + jnp.dot(rows, w, preferred_element_type=jnp.float32)
        left, right = total[:, :cols], total[:, cols:]
        px_ref[g] = jnp.where(core == 0, right, left)
        proj_ref[g, core] = jnp.where(core == 0, left, right)
        squares = jnp.sum(total * total, axis=1, keepdims=True)
        ss_ref[tp, pl.ds(g, 1), :] = jnp.broadcast_to(squares, (BLOCK, BLOCK)).T[0:1]
        swap(g).start()

    def swap(g):
        return send(px_ref.at[g], proj_ref.at[g, core], (p_s.at[0], p_r.at[0]), at_tp(sib))

    @pl.loop(0, blocks)
    def _(b):
        ho_ref[x, b] = attend_block(b)
        for i in range(3):
            heads_to(b, i).start()

    arrived(wc_ref.at[:, pl.ds(0, RING - 1)], y_r.at[0])
    for g in range(pairs):
        finish(g)

    def sums(d):
        return send(ss_ref.at[tp], ss_ref.at[tp], (s_s.at[0], s_r.at[0]), at_tp(other_tp(d)))

    for d in range(1, tp_n):
        sums(d).start()

    for j in range(xs):
        arrived(tk_ref.at[pl.ds(0, len(beside) if j else tp_n - 1), 0], t_s.at[j])
    arrived(tk_ref.at[pl.ds(0, 2), pl.ds(0, xs - 1)], tf_s.at[0])
    for n in range(1, kv_n):

        @pl.when(kv == n)
        def _(n=n):
            arrived(chs_ref.at[pl.ds(0, n)], ch_s.at[0])

    arrived(wc_ref.at[pl.ds(0, tp_n - 1), 0], w_s.at[0])
    arrived(wc_ref.at[:, pl.ds(0, RING - 1)], y_s.at[0])
    for n in range(1, kv_n):

        @pl.when(kv == kv_n - 1 - n)
        def _(n=n):
            arrived(out_ref.at[pl.ds(0, n)], b_s.at[0])

    def drain(remote):
        arrived(kvp_ref.at[pl.ds(0, 7), pl.ds(0, blocks)], k_s.at[0])
        for g, (a, b) in enumerate(remote):

            @pl.when(kv >= a)
            def _(g=g, a=a, b=b):
                part = pl.ds(blocks + (a - 1) * PER_OWNER, (b - a) * PER_OWNER)
                arrived(kvp_ref.at[pl.ds(0, 7), part], k_s.at[g + 1])

    for low, high, spans in plans:

        @pl.when((kv >= low) & (kv < high))
        def _(spans=spans):
            drain(spans)

    arrived(ho_ref.at[pl.ds(0, xs - 1)], h_s.at[0])
    arrived(px_ref, p_s.at[0])
    arrived(ss_ref.at[pl.ds(0, tp_n - 1)], s_s.at[0])
    arrived(px_ref, p_r.at[0])
    arrived(ss_ref.at[pl.ds(0, tp_n - 1)], s_r.at[0])
    gains = ogain_ref[:, pl.ds(pl.multiple_of(tp * cols, cols), cols)]
    inverse = []
    for c in range(2):
        total = ss_ref[c]
        for p in range(1, xs):
            total = total + ss_ref[2 * p + c]
        inverse.append(lax.rsqrt(total / (cols * tp_n) + epsilon))

    for g in range(pairs):
        for c in range(2):
            scale = jnp.broadcast_to(inverse[c][g : g + 1], (BLOCK, BLOCK)).T
            scale = jnp.concatenate([scale] * (cols // BLOCK), axis=1)
            rows = (proj_ref[g, c] * scale * gains).astype(jnp.bfloat16)
            for u in range(2):
                o_ref[pl.ds((2 * g + u) * BLOCK + c * half, half), :] = rows[u * half : (u + 1) * half]


def on_device(
    tokens,
    query_weight,
    latent_weight,
    query_gain,
    key_gain,
    value_up,
    out_weight,
    out_gain,
    chosen,
):
    toks, feat = tokens.shape
    width = latent_weight.shape[1]
    heads = query_weight.shape[1] // width
    blocks = toks // BLOCK
    kv_n, tp_n = lax.axis_size("kv"), lax.axis_size("tp")
    cols = out_weight.shape[1] // tp_n
    hv = out_weight.shape[0]
    xs = tp_n // 2
    piece = BLOCK // tp_n
    slots = blocks + (kv_n - 1) * PER_OWNER
    halves = max(1, kv_n * blocks // LANES)
    near = max(len(spans) for _, _, spans in owner_groups(kv_n))
    count = near + 1
    bf, f32, i32 = jnp.bfloat16, jnp.float32, jnp.int32
    dma = pltpu.SemaphoreType.DMA
    vmem = pl.BlockSpec(memory_space=pltpu.VMEM)
    sems = [
        xs, 1, xs, xs, 2, 2, 1, 1, 1, near, count, count, count, count,
        1, 1, 1, 1, 1, blocks // 2, 1, 1, 1, 1,
    ]
    return pl.pallas_call(
        functools.partial(kernel, kv_n, tp_n),
        out_shape=jax.ShapeDtypeStruct((toks, cols), bf),
        in_specs=[pl.BlockSpec(memory_space=pltpu.HBM)] * 9,
        out_specs=vmem,
        scratch_shapes=[
            pltpu.VMEM(chosen.shape, i32),
            pltpu.SMEM(chosen.shape, i32),
            pltpu.VMEM((blocks, 2, xs, piece, feat), bf),
            pltpu.VMEM(latent_weight.shape, bf),
            pltpu.VMEM(query_weight.shape, bf),
            pltpu.VMEM((value_up.shape[0], value_up.shape[2], value_up.shape[1]), bf),
            pltpu.VMEM(out_weight.shape, bf),
            pltpu.VMEM((1, width), f32),
            pltpu.VMEM((1, width), f32),
            pltpu.VMEM((1, cols * tp_n), f32),
            pltpu.VMEM((tp_n, xs, blocks, piece, feat), bf),
            pltpu.VMEM(query_weight.shape, bf),
            pltpu.VMEM((value_up.shape[0], value_up.shape[2], value_up.shape[1]), bf),
            pltpu.VMEM((2 * heads, xs, blocks, piece, width), bf),
            pltpu.VMEM((blocks, piece, width), bf),
            pltpu.VMEM((kv_n - 1, PER_OWNER, piece, width), bf),
            pltpu.VMEM((tp_n, slots, piece, width), bf),
            pltpu.VMEM((slots + 1, BLOCK, width), bf),
            pltpu.VMEM((slots + 1, width + ONES, BLOCK), bf),
            pltpu.VMEM((2, hv, 2 * width), bf),
            pltpu.VMEM((halves, 1, LANES), i32),
            pltpu.VMEM((halves, 1, LANES), i32),
            pltpu.VMEM((kv_n - 1, 1, LANES), i32),
            pltpu.SMEM((halves, 1, LANES), i32),
            pltpu.SMEM((kv_n - 1, 1, LANES), i32),
            pltpu.VMEM((xs, blocks, BLOCK // 2, 2 * hv), bf),
            pltpu.VMEM((tp_n, RING, hv // RING, 2 * cols), bf),
            pltpu.VMEM((blocks // 2, 2, BLOCK, cols), f32),
            pltpu.VMEM((blocks // 2, BLOCK, cols), f32),
            pltpu.VMEM((tp_n, blocks // 2, BLOCK), f32),
            dma((10,)), dma((2,)), *[dma((n,)) for n in sems],
        ],
        compiler_params=pltpu.CompilerParams(
            collective_id=0, has_side_effects=True, vmem_limit_bytes=24 << 20
        ),
    )(*[
        pltpu.with_memory_space_constraint(a, pltpu.HBM)
        for a in (
            tokens.reshape(blocks, 2, xs, piece, feat), query_weight, latent_weight, query_gain[None, :],
            key_gain[None, :], jnp.swapaxes(value_up, 1, 2), out_weight, out_gain[None, :], chosen,
        )
    ])


def solution(mesh):
    in_specs = (
        P("kv", "tp"),
        P(None, "tp"),
        P(),
        P(),
        P(),
        P("tp", None, None),
        P("tp", None),
        P(),
        P("kv", None),
    )
    out_specs = P("kv", "tp")
    return jax.shard_map(
        on_device, mesh=mesh, in_specs=in_specs, out_specs=out_specs, check_vma=False
    )
```

```python
import functools

import jax
import jax.numpy as jnp
from jax import lax
from jax.experimental import pallas as pl
from jax.experimental.pallas import tpu as pltpu
from jax.sharding import PartitionSpec as P

BLOCK = 128
PER_OWNER = 2
RING = 4
OWNERS = 8
STEP = 8
LANES = 128
ONES = 16
MESH = pl.DeviceIdType.MESH

epsilon = 1e-06
masked_score = -1e30


def rms_scale(values, gain_row):
    widened = values.astype(jnp.float32)
    mean_sq = jnp.mean(widened * widened, axis=-1, keepdims=True)
    return (widened * lax.rsqrt(mean_sq + epsilon) * gain_row).astype(jnp.bfloat16)


def prefix_in_owner(values, lane, blocks, inclusive):
    total = values if inclusive else jnp.zeros_like(values)
    for s in range(1, blocks):
        total = total + jnp.where(lane % blocks >= s, pltpu.roll(values, s, 1), 0)
    return total


def send(src, dst, sems, where):
    return pltpu.make_async_remote_copy(
        src_ref=src, dst_ref=dst, send_sem=sems[0], recv_sem=sems[1], device_id=where, device_id_type=MESH
    )


def arrived(part, sem):
    pltpu.make_async_copy(part, part, sem).wait()


def owner_groups(kv_n):
    if kv_n != 8 * RING:
        return [(0, kv_n, [(d, min(d + OWNERS, kv_n)) for d in range(1, kv_n, OWNERS)])]
    return [
        (0, 8, [(1, 8)]),
        (8, 16, [(1, 7), (7, 12), (12, 16)]),
        (16, 20, [(1, 9), (9, 15), (15, 20)]),
        (20, 24, [(1, 9), (17, 24), (9, 13), (13, 17)]),
        (24, 28, [(1, 9), (20, 28), (9, 15), (15, 20)]),
        (28, 32, [(1, 7), (7, 13), (13, 19), (19, 24), (24, 29), (29, 32)]),
    ]


def kernel(
    kv_n, tp_n,
    tok_in, wq_in, wl_in, qgain_in, kgain_in, vu_in, w_in, ogain_in, chosen_in,
    o_ref,
    chosen_ref, chosen_s, tok_ref, wl_ref, wq_ref, vu_ref, w_ref, qgain_ref, kgain_ref, ogain_ref,
    tk_ref, wqs_ref, vus_ref, q_ref, lat_ref, out_ref, kvp_ref, kn_ref, vt_ref, bd_ref,
    map_ref, req_ref, chs_ref, map_s, chs_s,
    ho_ref, wc_ref, proj_ref, px_ref, ss_ref,
    in_s, lc, t_s, tf_s, t_r, tf_r, c_s, c_r, ch_s, ch_r, b_s, b_r, k_s, k_r, kf_r, kr_r,
    w_s, w_r, y_s, y_r, h_s, h_r, p_s, p_r, s_s, s_r,
):
    kv, tp = lax.axis_index("kv"), lax.axis_index("tp")
    core, x = lax.rem(tp, 2), tp // 2
    sib = tp + 1 - 2 * core
    blocks, _, xs, piece, feat = tok_ref.shape
    width = wl_ref.shape[1]
    heads = wq_ref.shape[1] // width
    vdim = vu_ref.shape[1]
    slots = kvp_ref.shape[1]
    picks = chosen_ref.shape[1]
    cols = o_ref.shape[1]
    half = BLOCK // 2
    mine = blocks * piece
    per_row = LANES // blocks
    wrows = w_ref.shape[0] // RING
    y = lax.rem(kv, RING)

    def at_kv(other):
        return {"kv": other, "tp": tp}

    def at_tp(other):
        return {"kv": kv, "tp": other}

    def other_tp(d):
        return lax.rem(tp + d + tp_n, tp_n)

    barrier = pltpu.get_barrier_semaphore()
    for d in range(1, kv_n):
        pl.semaphore_signal(barrier, inc=1, device_id=at_kv(lax.rem(kv + d, kv_n)), device_id_type=MESH)
    for d in range(1, tp_n):
        pl.semaphore_signal(barrier, inc=1, device_id=at_tp(other_tp(d)), device_id_type=MESH)

    loads = [
        pltpu.make_async_copy(a, b, in_s.at[i])
        for i, (a, b) in enumerate([
            (chosen_in, chosen_ref), (chosen_in, chosen_s), (tok_in, tok_ref), (wl_in, wl_ref), (wq_in, wq_ref),
            (vu_in, vu_ref), (w_in, w_ref), (qgain_in, qgain_ref), (kgain_in, kgain_ref), (ogain_in, ogain_ref),
        ])
    ]
    for load in loads:
        load.start()
    loads[0].wait()
    lane = lax.broadcasted_iota(jnp.int32, (blocks, LANES), 1)
    halves = map_ref.shape[0]
    table = chosen_ref[...]
    for g in range(halves):
        hit = jnp.zeros((blocks, LANES), jnp.int32)
        for c in range(picks):
            hit = jnp.where(table[:, c : c + 1] == lane + g * LANES, 1, hit)
        need = jnp.broadcast_to(jnp.max(hit, axis=0, keepdims=True), (blocks, LANES))
        rank = prefix_in_owner(need, lane, blocks, False)
        local = lane % blocks
        dist = kv - (lane // blocks + g * per_row)
        slot = jnp.where(dist == 0, local, blocks + (dist - 1) * PER_OWNER + rank)
        map_ref[g] = jnp.clip(slot, 0, slots - 1)[0:1]
        code = jnp.zeros((blocks, LANES), jnp.int32)
        for k in range(PER_OWNER):
            code = code + jnp.where((need > 0) & (rank == k), local * blocks**k, 0)
        req_ref[g] = prefix_in_owner(code, lane, blocks, True)[0:1]

    pltpu.make_async_copy(map_ref, map_s, lc.at[0]).start()
    for load in loads[1:]:
        load.wait()
    pl.semaphore_wait(barrier, kv_n - 1 + tp_n - 1)

    def chip(i):
        return lax.rem(x + i + xs, xs)

    def same_core(i):
        return 2 * chip(i) + core

    def tokens_to(e, j):
        c = 1 - core if e == 1 else e % 2
        part = chip(e // 2 + j)
        return send(
            tok_ref.at[:, c, part], tk_ref.at[tp, part], (t_s.at[j], t_r.at[j]), at_tp(2 * chip(e // 2) + c)
        )

    beside = [e for e in range(1, tp_n) if e // 2 != 2]

    def tokens_on(j, way):
        step = 1 - 2 * way
        part = tk_ref.at[2 * chip(-step) + way, chip(step + j)]
        return send(part, part, (tf_s.at[0], tf_r.at[j]), at_tp(same_core(step)))

    def ask(d):
        owner = lax.rem(kv - d + kv_n, kv_n)
        return send(
            req_ref.at[owner // per_row], chs_ref.at[d - 1],
            (ch_s.at[0], ch_r.at[0]), at_kv(owner),
        )

    def serves(d):
        return kv + d < kv_n

    def weights_to(d):
        other = other_tp(d)
        part = w_ref.at[
            pl.ds(pl.multiple_of(y * wrows, wrows), wrows),
            pl.ds(pl.multiple_of(other // 2 * 2 * cols, 2 * cols), 2 * cols),
        ]
        return send(part, wc_ref.at[tp, y], (w_s.at[0], w_r.at[0]), at_tp(other))

    def weights_on(e):
        part = wc_ref.at[:, y]
        other = kv - y + lax.rem(y + e, RING)
        return send(part, part, (y_s.at[0], y_r.at[0]), at_kv(other))

    to_sib = [
        send(wq_ref, wqs_ref, (c_s.at[0], c_r.at[0]), at_tp(sib)),
        send(vu_ref, vus_ref, (c_s.at[1], c_r.at[1]), at_tp(sib)),
    ]

    for e in (5, 4, 3, 2, 7, 6, 1):
        tokens_to(e, 0).start()
    for d in range(1, kv_n):

        @pl.when(kv - d >= 0)
        def _(d=d):
            ask(d).start()

    for j in range(1, xs):
        for e in beside:
            tokens_to(e, j).start()
    for copy in to_sib:
        copy.start()
    for p in range(xs):
        tk_ref[tp, p] = tok_ref[:, core, p]
    wc_ref[tp, y] = w_ref[
        pl.ds(pl.multiple_of(y * wrows, wrows), wrows), pl.ds(pl.multiple_of(x * 2 * cols, 2 * cols), 2 * cols)
    ]
    null = slots
    vt_ref[:, width:, :] = jnp.ones((slots + 1, ONES, BLOCK), jnp.bfloat16)
    kn_ref[null] = jnp.zeros((BLOCK, width), jnp.bfloat16)
    vt_ref[null] = jnp.zeros((width + ONES, BLOCK), jnp.bfloat16)
    bd_ref[...] = jnp.zeros_like(bd_ref)

    def features(p):
        return jnp.concatenate([tk_ref[t, p].reshape(mine, feat) for t in range(tp_n)], axis=1)

    def hand_tokens(j):
        if j:
            arrived(tk_ref.at[pl.ds(0, len(beside)), 0], t_r.at[j])
        if j != 1:
            tokens_on((j - 1) % xs, 0).start()
        if j < xs - 1:
            tokens_on(j + 1, 1).start()

    for n in range(1, kv_n):

        @pl.when(kv == kv_n - 1 - n)
        def _(n=n):
            arrived(chs_ref.at[pl.ds(0, n)], ch_r.at[0])

    to_smem = pltpu.make_async_copy(chs_ref, chs_s, lc.at[1])
    to_smem.start()
    arrived(tk_ref.at[pl.ds(0, tp_n - 1), 0], t_r.at[0])
    hand_tokens(0)
    lat = jnp.dot(features(x), wl_ref[...], preferred_element_type=jnp.float32).astype(jnp.bfloat16)
    lat_ref[...] = lat.reshape(blocks, piece, width)
    kvp_ref[tp, 0:blocks] = lat.reshape(blocks, piece, width)

    pltpu.make_async_copy(map_ref, map_s, lc.at[0]).wait()
    to_smem.wait()

    def slots_of(d):
        return pl.ds(blocks + (d - 1) * PER_OWNER, PER_OWNER)

    plans = owner_groups(kv_n)

    def span_of(d):
        index = 0
        for low, _, spans in plans:
            here = next((i for i, (a, b) in enumerate(spans) if a <= d < b), 0)
            index = jnp.where(kv + d >= low, here, index)
        return index

    def give(d):
        return send(
            out_ref.at[d - 1], kvp_ref.at[tp, slots_of(d)], (b_s.at[0], b_r.at[span_of(d)]), at_kv(lax.rem(kv + d, kv_n))
        )

    at_lane = lax.rem(kv, per_row) * blocks + blocks - 1
    for d in range(1, kv_n):

        @pl.when(serves(d))
        def _(d=d):
            code = chs_s[d - 1, 0, at_lane]
            for k in range(PER_OWNER):
                out_ref[d - 1, k] = lat_ref[(code >> (3 * k)) & (blocks - 1)]
            give(d).start()

    gain_k = kgain_ref[...]
    gain_q = qgain_ref[...] * (width**-0.5 * 1.4426950408889634)

    def project(j):
        if j:
            arrived(tk_ref.at[pl.ds(0, 2), 0], tf_r.at[j])
        p = lax.rem(x + j, xs)
        rows = features(p)
        for w, at in ((wq_ref, core), (wqs_ref, 1 - core)):
            qs = jnp.dot(rows, w[...], preferred_element_type=jnp.float32).astype(jnp.bfloat16)
            for h in range(heads):
                part = rms_scale(qs[:, h * width : (h + 1) * width], gain_q)
                q_ref[at * heads + h, p] = part.reshape(blocks, piece, width)

    def exchange(remote):
        groups = [(0, blocks)] + [
            (blocks + (a - 1) * PER_OWNER, (b - a) * PER_OWNER) for a, b in remote
        ]

        def direct(g):
            return g >= min(1, len(groups) - 1)

        def halves_of(g):
            first, size = groups[g]
            cut = (size + 1) // 2
            return [pl.ds(first, cut), pl.ds(first + cut, size - cut)]

        def spread(g, i):
            part = kvp_ref.at[tp, pl.ds(*groups[g])]
            where = sib if i == 2 else same_core((1, -1, 0, 2)[i])
            return send(part, part, (k_s.at[g], (kr_r if i == 2 else k_r).at[g]), at_tp(where))

        def pass_on(g, way):
            step = 1 - 2 * way
            part = kvp_ref.at[same_core(-step), halves_of(g)[way]]
            return send(part, part, (k_s.at[g], kf_r.at[g]), at_tp(same_core(step)))

        def relay(g, i):
            if i < 2 or direct(g):
                part = kvp_ref.at[same_core((-1, 1, 2)[i]), pl.ds(*groups[g])]
            else:
                part = kvp_ref.at[same_core(2), halves_of(g)[i - 2]]
            return send(part, part, (k_s.at[g], kr_r.at[g]), at_tp(sib))

        def when_group(g, body):
            if g == 0:
                body()
            else:
                pl.when(kv >= remote[g - 1][0])(body)

        def spread_group(g):
            def body():
                if g:
                    a, b = remote[g - 1]
                    for n in range(1, b - a + 1):

                        @pl.when((kv >= b - 1) if n == b - a else (kv == a + n - 1))
                        def _(n=n):
                            arrived(kvp_ref.at[tp, pl.ds(groups[g][0], n * PER_OWNER)], b_r.at[g - 1])

                for i in range(3 + direct(g)):
                    spread(g, i).start()

            when_group(g, body)

        def pass_group(g):
            def body():
                arrived(kvp_ref.at[pl.ds(0, 2 + direct(g)), pl.ds(*groups[g])], k_r.at[g])
                for i in range(2 + direct(g)):
                    if not direct(g):
                        pass_on(g, i).start()
                    relay(g, i).start()

            when_group(g, body)

        def relay_group(g):
            def body():
                if not direct(g):
                    arrived(kvp_ref.at[0, pl.ds(*groups[g])], kf_r.at[g])
                    for i in range(2):
                        relay(g, i + 2).start()

            when_group(g, body)

        def norm_group(g):
            def body():
                arrived(kvp_ref.at[pl.ds(0, 4), pl.ds(*groups[g])], kr_r.at[g])

                first, size = groups[g]
                each = next(n for n in (4, 2, 1) if size % n == 0)

                @pl.loop(0, size // each)
                def _(i):
                    for u in range(each):
                        slot = first + i * each + u
                        rows = jnp.concatenate(
                            [kvp_ref[p * 2 + c, slot] for c in range(2) for p in range(xs)], axis=0
                        )
                        kn_ref[slot] = rms_scale(rows, gain_k)
                        vt_ref[slot, 0:width, :] = rows.T

            when_group(g, body)

        spread_group(0)
        for copy in to_sib:
            copy.wait()
        for v, at in ((vu_ref, core), (vus_ref, 1 - core)):
            for h in range(heads):
                bd_ref[at, h * vdim : (h + 1) * vdim, h * width : (h + 1) * width] = v[h]
        count = len(groups)
        project(0)
        for j in range(1, xs):
            hand_tokens(j)
        def weights_step():
            arrived(wc_ref.at[pl.ds(0, tp_n - 1), 0], w_r.at[0])
            for e in range(1, RING):
                weights_on(e).start()

        for g in range(1, count):
            spread_group(g)
            if g == 1:
                pass_group(0)
        if count < 2:
            pass_group(0)
        for d in range(1, tp_n):
            weights_to(d).start()
        if not direct(0):
            relay_group(0)
        passed, normed = 1, 0
        for j in range(1, xs):
            project(j)
        norm_group(normed)
        normed += 1
        for g in range(passed, count):
            pass_group(g)
            if normed < g:
                norm_group(normed)
                normed += 1
        weights_step()
        for g in range(normed, count):
            norm_group(g)


    for low, high, spans in plans:

        @pl.when((kv >= low) & (kv < high))
        def _(spans=spans):
            exchange(spans)

    def listed(b, c):
        block = chosen_s[b, c]
        known = jnp.maximum(block, 0)
        return jnp.where(block < 0, null, map_s[known >> 7, 0, known & (LANES - 1)])

    def attend_block(b):
        q = jnp.concatenate([q_ref[h, p, b] for h in range(2 * heads) for p in range(xs)], axis=0)
        qt = q.T
        acc = jnp.zeros((width + ONES, 2 * heads * half), jnp.float32)
        for i in range(0, picks, STEP):
            at = [listed(b, i + k) for k in range(STEP)]
            keys = jnp.concatenate([kn_ref[s] for s in at], axis=0)
            s = jnp.dot(keys, qt, preferred_element_type=jnp.float32)
            if i == 0:
                key_row = lax.broadcasted_iota(jnp.int32, s.shape, 0)
                query_row = lax.broadcasted_iota(jnp.int32, s.shape, 1) % half + core * half
                s = jnp.where((key_row <= query_row) | (key_row >= BLOCK), s, masked_score)
            p = jnp.exp2(s).astype(jnp.bfloat16)
            values = jnp.concatenate([vt_ref[s] for s in at], axis=1)
            acc = acc + jnp.dot(values, p, preferred_element_type=jnp.float32)
        att = (acc[:width] / acc[width : width + 1]).astype(jnp.bfloat16).T
        out = []
        for h in range(0, 2 * heads, 2):
            two = jnp.concatenate([att[h * half : (h + 1) * half], att[(h + 1) * half : (h + 2) * half]], axis=1)
            out.append(
                lax.dot_general(two, bd_ref[h // 2], (((1,), (1,)), ((), ())), preferred_element_type=jnp.float32)
            )
        return jnp.concatenate(out, axis=1).astype(jnp.bfloat16)

    pairs = blocks // 2

    def heads_to(b, i):
        part = ho_ref.at[x, b]
        return send(part, part, (h_s.at[0], h_r.at[b // 2]), at_tp(same_core((2, 1, -1)[i])))

    def finish(g):
        arrived(ho_ref.at[pl.ds(0, xs - 1), pl.ds(0, 2)], h_r.at[g])
        total = jnp.zeros((BLOCK, 2 * cols), jnp.float32)
        for p in range(xs):
            rows = ho_ref[p, pl.ds(2 * g, 2)].reshape(BLOCK, 2 * cols)
            w = jnp.concatenate([wc_ref[2 * p + c].reshape(RING * wrows, 2 * cols) for c in range(2)], axis=0)
            total = total + jnp.dot(rows, w, preferred_element_type=jnp.float32)
        left, right = total[:, :cols], total[:, cols:]
        px_ref[g] = jnp.where(core == 0, right, left)
        proj_ref[g, core] = jnp.where(core == 0, left, right)
        squares = jnp.sum(total * total, axis=1, keepdims=True)
        ss_ref[tp, pl.ds(g, 1), :] = jnp.broadcast_to(squares, (BLOCK, BLOCK)).T[0:1]
        swap(g).start()

    def swap(g):
        return send(px_ref.at[g], proj_ref.at[g, core], (p_s.at[0], p_r.at[0]), at_tp(sib))

    @pl.loop(0, blocks)
    def _(b):
        ho_ref[x, b] = attend_block(b)
        for i in range(3):
            heads_to(b, i).start()

    arrived(wc_ref.at[:, pl.ds(0, RING - 1)], y_r.at[0])
    for g in range(pairs):
        finish(g)

    def sums(d):
        return send(ss_ref.at[tp], ss_ref.at[tp], (s_s.at[0], s_r.at[0]), at_tp(other_tp(d)))

    for d in range(1, tp_n):
        sums(d).start()

    for j in range(xs):
        arrived(tk_ref.at[pl.ds(0, len(beside) if j else tp_n - 1), 0], t_s.at[j])
    arrived(tk_ref.at[pl.ds(0, 2), pl.ds(0, xs - 1)], tf_s.at[0])
    for n in range(1, kv_n):

        @pl.when(kv == n)
        def _(n=n):
            arrived(chs_ref.at[pl.ds(0, n)], ch_s.at[0])

    arrived(wc_ref.at[pl.ds(0, tp_n - 1), 0], w_s.at[0])
    arrived(wc_ref.at[:, pl.ds(0, RING - 1)], y_s.at[0])
    for n in range(1, kv_n):

        @pl.when(kv == kv_n - 1 - n)
        def _(n=n):
            arrived(out_ref.at[pl.ds(0, n)], b_s.at[0])

    def drain(remote):
        arrived(kvp_ref.at[pl.ds(0, 7), pl.ds(0, blocks)], k_s.at[0])
        for g, (a, b) in enumerate(remote):

            @pl.when(kv >= a)
            def _(g=g, a=a, b=b):
                part = pl.ds(blocks + (a - 1) * PER_OWNER, (b - a) * PER_OWNER)
                arrived(kvp_ref.at[pl.ds(0, 7), part], k_s.at[g + 1])

    for low, high, spans in plans:

        @pl.when((kv >= low) & (kv < high))
        def _(spans=spans):
            drain(spans)

    arrived(ho_ref.at[pl.ds(0, xs - 1)], h_s.at[0])
    arrived(px_ref, p_s.at[0])
    arrived(ss_ref.at[pl.ds(0, tp_n - 1)], s_s.at[0])
    arrived(px_ref, p_r.at[0])
    arrived(ss_ref.at[pl.ds(0, tp_n - 1)], s_r.at[0])
    gains = ogain_ref[:, pl.ds(pl.multiple_of(tp * cols, cols), cols)]
    inverse = []
    for c in range(2):
        total = ss_ref[c]
        for p in range(1, xs):
            total = total + ss_ref[2 * p + c]
        inverse.append(lax.rsqrt(total / (cols * tp_n) + epsilon))

    for g in range(pairs):
        for c in range(2):
            scale = jnp.broadcast_to(inverse[c][g : g + 1], (BLOCK, BLOCK)).T
            scale = jnp.concatenate([scale] * (cols // BLOCK), axis=1)
            rows = (proj_ref[g, c] * scale * gains).astype(jnp.bfloat16)
            for u in range(2):
                o_ref[pl.ds((2 * g + u) * BLOCK + c * half, half), :] = rows[u * half : (u + 1) * half]


def on_device(
    tokens,
    query_weight,
    latent_weight,
    query_gain,
    key_gain,
    value_up,
    out_weight,
    out_gain,
    chosen,
):
    toks, feat = tokens.shape
    width = latent_weight.shape[1]
    heads = query_weight.shape[1] // width
    blocks = toks // BLOCK
    kv_n, tp_n = lax.axis_size("kv"), lax.axis_size("tp")
    cols = out_weight.shape[1] // tp_n
    hv = out_weight.shape[0]
    xs = tp_n // 2
    piece = BLOCK // tp_n
    slots = blocks + (kv_n - 1) * PER_OWNER
    halves = max(1, kv_n * blocks // LANES)
    near = max(len(spans) for _, _, spans in owner_groups(kv_n))
    count = near + 1
    bf, f32, i32 = jnp.bfloat16, jnp.float32, jnp.int32
    dma = pltpu.SemaphoreType.DMA
    vmem = pl.BlockSpec(memory_space=pltpu.VMEM)
    sems = [
        xs, 1, xs, xs, 2, 2, 1, 1, 1, near, count, count, count, count,
        1, 1, 1, 1, 1, blocks // 2, 1, 1, 1, 1,
    ]
    return pl.pallas_call(
        functools.partial(kernel, kv_n, tp_n),
        out_shape=jax.ShapeDtypeStruct((toks, cols), bf),
        in_specs=[pl.BlockSpec(memory_space=pltpu.HBM)] * 9,
        out_specs=vmem,
        scratch_shapes=[
            pltpu.VMEM(chosen.shape, i32),
            pltpu.SMEM(chosen.shape, i32),
            pltpu.VMEM((blocks, 2, xs, piece, feat), bf),
            pltpu.VMEM(latent_weight.shape, bf),
            pltpu.VMEM(query_weight.shape, bf),
            pltpu.VMEM((value_up.shape[0], value_up.shape[2], value_up.shape[1]), bf),
            pltpu.VMEM(out_weight.shape, bf),
            pltpu.VMEM((1, width), f32),
            pltpu.VMEM((1, width), f32),
            pltpu.VMEM((1, cols * tp_n), f32),
            pltpu.VMEM((tp_n, xs, blocks, piece, feat), bf),
            pltpu.VMEM(query_weight.shape, bf),
            pltpu.VMEM((value_up.shape[0], value_up.shape[2], value_up.shape[1]), bf),
            pltpu.VMEM((2 * heads, xs, blocks, piece, width), bf),
            pltpu.VMEM((blocks, piece, width), bf),
            pltpu.VMEM((kv_n - 1, PER_OWNER, piece, width), bf),
            pltpu.VMEM((tp_n, slots, piece, width), bf),
            pltpu.VMEM((slots + 1, BLOCK, width), bf),
            pltpu.VMEM((slots + 1, width + ONES, BLOCK), bf),
            pltpu.VMEM((2, hv, 2 * width), bf),
            pltpu.VMEM((halves, 1, LANES), i32),
            pltpu.VMEM((halves, 1, LANES), i32),
            pltpu.VMEM((kv_n - 1, 1, LANES), i32),
            pltpu.SMEM((halves, 1, LANES), i32),
            pltpu.SMEM((kv_n - 1, 1, LANES), i32),
            pltpu.VMEM((xs, blocks, BLOCK // 2, 2 * hv), bf),
            pltpu.VMEM((tp_n, RING, hv // RING, 2 * cols), bf),
            pltpu.VMEM((blocks // 2, 2, BLOCK, cols), f32),
            pltpu.VMEM((blocks // 2, BLOCK, cols), f32),
            pltpu.VMEM((tp_n, blocks // 2, BLOCK), f32),
            dma((10,)), dma((2,)), *[dma((n,)) for n in sems],
        ],
        compiler_params=pltpu.CompilerParams(
            collective_id=0, has_side_effects=True, vmem_limit_bytes=24 << 20
        ),
    )(*[
        pltpu.with_memory_space_constraint(a, pltpu.HBM)
        for a in (
            tokens.reshape(blocks, 2, xs, piece, feat), query_weight, latent_weight, query_gain[None, :],
            key_gain[None, :], jnp.swapaxes(value_up, 1, 2), out_weight, out_gain[None, :], chosen,
        )
    ])


def solution(mesh):
    in_specs = (
        P("kv", "tp"),
        P(None, "tp"),
        P(),
        P(),
        P(),
        P("tp", None, None),
        P("tp", None),
        P(),
        P("kv", None),
    )
    out_specs = P("kv", "tp")
    return jax.shard_map(
        on_device, mesh=mesh, in_specs=in_specs, out_specs=out_specs, check_vma=False
    )
```

```python
import functools

import jax
import jax.numpy as jnp
from jax import lax
from jax.experimental import pallas as pl
from jax.experimental.pallas import tpu as pltpu
from jax.sharding import PartitionSpec as P

BLOCK = 128
PER_OWNER = 2
RING = 4
OWNERS = 8
STEP = 8
LANES = 128
ONES = 16
MESH = pl.DeviceIdType.MESH

epsilon = 1e-06
masked_score = -1e30


def rms_scale(values, gain_row):
    widened = values.astype(jnp.float32)
    mean_sq = jnp.mean(widened * widened, axis=-1, keepdims=True)
    return (widened * lax.rsqrt(mean_sq + epsilon) * gain_row).astype(jnp.bfloat16)


def prefix_in_owner(values, lane, blocks, inclusive):
    total = values if inclusive else jnp.zeros_like(values)
    for s in range(1, blocks):
        total = total + jnp.where(lane % blocks >= s, pltpu.roll(values, s, 1), 0)
    return total


def send(src, dst, sems, where):
    return pltpu.make_async_remote_copy(
        src_ref=src, dst_ref=dst, send_sem=sems[0], recv_sem=sems[1], device_id=where, device_id_type=MESH
    )


def arrived(part, sem):
    pltpu.make_async_copy(part, part, sem).wait()


def owner_groups(kv_n):
    if kv_n != 8 * RING:
        return [(0, kv_n, [(d, min(d + OWNERS, kv_n)) for d in range(1, kv_n, OWNERS)])]
    return [
        (0, 8, [(1, 8)]),
        (8, 16, [(1, 7), (7, 12), (12, 16)]),
        (16, 20, [(1, 7), (7, 11), (11, 15), (15, 18), (18, 20)]),
        (20, 24, [(1, 9), (17, 24), (9, 13), (13, 17)]),
        (24, 28, [(1, 9), (20, 25), (25, 28), (9, 13), (13, 17), (17, 20)]),
        (28, 32, [(1, 6), (6, 11), (11, 16), (16, 21), (21, 25), (25, 29), (29, 32)]),
    ]


def kernel(
    kv_n, tp_n,
    tok_in, wq_in, wl_in, qgain_in, kgain_in, vu_in, w_in, ogain_in, chosen_in,
    o_ref,
    chosen_ref, chosen_s, tok_ref, wl_ref, wq_ref, vu_ref, w_ref, qgain_ref, kgain_ref, ogain_ref,
    tk_ref, wqs_ref, vus_ref, q_ref, lat_ref, out_ref, kvp_ref, kn_ref, vt_ref, bd_ref,
    map_ref, req_ref, chs_ref, map_s, chs_s,
    ho_ref, wc_ref, proj_ref, px_ref, ss_ref,
    in_s, lc, t_s, tf_s, t_r, tf_r, c_s, c_r, ch_s, ch_r, b_s, b_r, k_s, k_r, kf_r, kr_r,
    w_s, w_r, y_s, y_r, h_s, h_r, p_s, p_r, s_s, s_r,
):
    kv, tp = lax.axis_index("kv"), lax.axis_index("tp")
    core, x = lax.rem(tp, 2), tp // 2
    sib = tp + 1 - 2 * core
    blocks, _, xs, piece, feat = tok_ref.shape
    width = wl_ref.shape[1]
    heads = wq_ref.shape[1] // width
    vdim = vu_ref.shape[1]
    slots = kvp_ref.shape[1]
    picks = chosen_ref.shape[1]
    cols = o_ref.shape[1]
    half = BLOCK // 2
    mine = blocks * piece
    per_row = LANES // blocks
    wrows = w_ref.shape[0] // RING
    y = lax.rem(kv, RING)

    def at_kv(other):
        return {"kv": other, "tp": tp}

    def at_tp(other):
        return {"kv": kv, "tp": other}

    def other_tp(d):
        return lax.rem(tp + d + tp_n, tp_n)

    barrier = pltpu.get_barrier_semaphore()
    for d in range(1, kv_n):
        pl.semaphore_signal(barrier, inc=1, device_id=at_kv(lax.rem(kv + d, kv_n)), device_id_type=MESH)
    for d in range(1, tp_n):
        pl.semaphore_signal(barrier, inc=1, device_id=at_tp(other_tp(d)), device_id_type=MESH)

    loads = [
        pltpu.make_async_copy(a, b, in_s.at[i])
        for i, (a, b) in enumerate([
            (chosen_in, chosen_ref), (chosen_in, chosen_s), (tok_in, tok_ref), (wl_in, wl_ref), (wq_in, wq_ref),
            (vu_in, vu_ref), (w_in, w_ref), (qgain_in, qgain_ref), (kgain_in, kgain_ref), (ogain_in, ogain_ref),
        ])
    ]
    for load in loads:
        load.start()
    loads[0].wait()
    lane = lax.broadcasted_iota(jnp.int32, (blocks, LANES), 1)
    halves = map_ref.shape[0]
    table = chosen_ref[...]
    for g in range(halves):
        hit = jnp.zeros((blocks, LANES), jnp.int32)
        for c in range(picks):
            hit = jnp.where(table[:, c : c + 1] == lane + g * LANES, 1, hit)
        need = jnp.broadcast_to(jnp.max(hit, axis=0, keepdims=True), (blocks, LANES))
        rank = prefix_in_owner(need, lane, blocks, False)
        local = lane % blocks
        dist = kv - (lane // blocks + g * per_row)
        slot = jnp.where(dist == 0, local, blocks + (dist - 1) * PER_OWNER + rank)
        map_ref[g] = jnp.clip(slot, 0, slots - 1)[0:1]
        code = jnp.zeros((blocks, LANES), jnp.int32)
        for k in range(PER_OWNER):
            code = code + jnp.where((need > 0) & (rank == k), local * blocks**k, 0)
        req_ref[g] = prefix_in_owner(code, lane, blocks, True)[0:1]

    pltpu.make_async_copy(map_ref, map_s, lc.at[0]).start()
    for load in loads[1:]:
        load.wait()
    pl.semaphore_wait(barrier, kv_n - 1 + tp_n - 1)

    def chip(i):
        return lax.rem(x + i + xs, xs)

    def same_core(i):
        return 2 * chip(i) + core

    def tokens_to(e, j):
        c = 1 - core if e == 1 else e % 2
        part = chip(e // 2 + j)
        return send(
            tok_ref.at[:, c, part], tk_ref.at[tp, part], (t_s.at[j], t_r.at[j]), at_tp(2 * chip(e // 2) + c)
        )

    beside = [e for e in range(1, tp_n) if e // 2 != 2]

    def tokens_on(j, way):
        step = 1 - 2 * way
        part = tk_ref.at[2 * chip(-step) + way, chip(step + j)]
        return send(part, part, (tf_s.at[0], tf_r.at[j]), at_tp(same_core(step)))

    def ask(d):
        owner = lax.rem(kv - d + kv_n, kv_n)
        return send(
            req_ref.at[owner // per_row], chs_ref.at[d - 1],
            (ch_s.at[0], ch_r.at[0]), at_kv(owner),
        )

    def serves(d):
        return kv + d < kv_n

    def weights_to(d):
        other = other_tp(d)
        part = w_ref.at[
            pl.ds(pl.multiple_of(y * wrows, wrows), wrows),
            pl.ds(pl.multiple_of(other // 2 * 2 * cols, 2 * cols), 2 * cols),
        ]
        return send(part, wc_ref.at[tp, y], (w_s.at[0], w_r.at[0]), at_tp(other))

    def weights_on(e):
        part = wc_ref.at[:, y]
        other = kv - y + lax.rem(y + e, RING)
        return send(part, part, (y_s.at[0], y_r.at[0]), at_kv(other))

    to_sib = [
        send(wq_ref, wqs_ref, (c_s.at[0], c_r.at[0]), at_tp(sib)),
        send(vu_ref, vus_ref, (c_s.at[1], c_r.at[1]), at_tp(sib)),
    ]

    for e in (5, 4, 3, 2, 7, 6, 1):
        tokens_to(e, 0).start()
    for d in range(1, kv_n):

        @pl.when(kv - d >= 0)
        def _(d=d):
            ask(d).start()

    for j in range(1, xs):
        for e in beside:
            tokens_to(e, j).start()
    for copy in to_sib:
        copy.start()
    for p in range(xs):
        tk_ref[tp, p] = tok_ref[:, core, p]
    wc_ref[tp, y] = w_ref[
        pl.ds(pl.multiple_of(y * wrows, wrows), wrows), pl.ds(pl.multiple_of(x * 2 * cols, 2 * cols), 2 * cols)
    ]
    null = slots
    vt_ref[:, width:, :] = jnp.ones((slots + 1, ONES, BLOCK), jnp.bfloat16)
    kn_ref[null] = jnp.zeros((BLOCK, width), jnp.bfloat16)
    vt_ref[null] = jnp.zeros((width + ONES, BLOCK), jnp.bfloat16)
    bd_ref[...] = jnp.zeros_like(bd_ref)

    def features(p):
        return jnp.concatenate([tk_ref[t, p].reshape(mine, feat) for t in range(tp_n)], axis=1)

    def hand_tokens(j):
        if j:
            arrived(tk_ref.at[pl.ds(0, len(beside)), 0], t_r.at[j])
        if j != 1:
            tokens_on((j - 1) % xs, 0).start()
        if j < xs - 1:
            tokens_on(j + 1, 1).start()

    for n in range(1, kv_n):

        @pl.when(kv == kv_n - 1 - n)
        def _(n=n):
            arrived(chs_ref.at[pl.ds(0, n)], ch_r.at[0])

    to_smem = pltpu.make_async_copy(chs_ref, chs_s, lc.at[1])
    to_smem.start()
    arrived(tk_ref.at[pl.ds(0, tp_n - 1), 0], t_r.at[0])
    hand_tokens(0)
    lat = jnp.dot(features(x), wl_ref[...], preferred_element_type=jnp.float32).astype(jnp.bfloat16)
    lat_ref[...] = lat.reshape(blocks, piece, width)
    kvp_ref[tp, 0:blocks] = lat.reshape(blocks, piece, width)

    pltpu.make_async_copy(map_ref, map_s, lc.at[0]).wait()
    to_smem.wait()

    def slots_of(d):
        return pl.ds(blocks + (d - 1) * PER_OWNER, PER_OWNER)

    plans = owner_groups(kv_n)

    def span_of(d):
        index = 0
        for low, _, spans in plans:
            here = next((i for i, (a, b) in enumerate(spans) if a <= d < b), 0)
            index = jnp.where(kv + d >= low, here, index)
        return index

    def give(d):
        return send(
            out_ref.at[d - 1], kvp_ref.at[tp, slots_of(d)], (b_s.at[0], b_r.at[span_of(d)]), at_kv(lax.rem(kv + d, kv_n))
        )

    at_lane = lax.rem(kv, per_row) * blocks + blocks - 1
    for d in range(1, kv_n):

        @pl.when(serves(d))
        def _(d=d):
            code = chs_s[d - 1, 0, at_lane]
            for k in range(PER_OWNER):
                out_ref[d - 1, k] = lat_ref[(code >> (3 * k)) & (blocks - 1)]
            give(d).start()

    gain_k = kgain_ref[...]
    gain_q = qgain_ref[...] * (width**-0.5 * 1.4426950408889634)

    def project(j):
        if j:
            arrived(tk_ref.at[pl.ds(0, 2), 0], tf_r.at[j])
        p = lax.rem(x + j, xs)
        rows = features(p)
        for w, at in ((wq_ref, core), (wqs_ref, 1 - core)):
            qs = jnp.dot(rows, w[...], preferred_element_type=jnp.float32).astype(jnp.bfloat16)
            for h in range(heads):
                part = rms_scale(qs[:, h * width : (h + 1) * width], gain_q)
                q_ref[at * heads + h, p] = part.reshape(blocks, piece, width)

    def exchange(remote):
        groups = [(0, blocks)] + [
            (blocks + (a - 1) * PER_OWNER, (b - a) * PER_OWNER) for a, b in remote
        ]

        def direct(g):
            return g >= min(1, len(groups) - 1)

        def halves_of(g):
            first, size = groups[g]
            cut = (size + 1) // 2
            return [pl.ds(first, cut), pl.ds(first + cut, size - cut)]

        def spread(g, i):
            part = kvp_ref.at[tp, pl.ds(*groups[g])]
            where = sib if i == 2 else same_core((1, -1, 0, 2)[i])
            return send(part, part, (k_s.at[g], (kr_r if i == 2 else k_r).at[g]), at_tp(where))

        def pass_on(g, way):
            step = 1 - 2 * way
            part = kvp_ref.at[same_core(-step), halves_of(g)[way]]
            return send(part, part, (k_s.at[g], kf_r.at[g]), at_tp(same_core(step)))

        def relay(g, i):
            if i < 2 or direct(g):
                part = kvp_ref.at[same_core((-1, 1, 2)[i]), pl.ds(*groups[g])]
            else:
                part = kvp_ref.at[same_core(2), halves_of(g)[i - 2]]
            return send(part, part, (k_s.at[g], kr_r.at[g]), at_tp(sib))

        def when_group(g, body):
            if g == 0:
                body()
            else:
                pl.when(kv >= remote[g - 1][0])(body)

        def spread_group(g):
            def body():
                if g:
                    a, b = remote[g - 1]
                    for n in range(1, b - a + 1):

                        @pl.when((kv >= b - 1) if n == b - a else (kv == a + n - 1))
                        def _(n=n):
                            arrived(kvp_ref.at[tp, pl.ds(groups[g][0], n * PER_OWNER)], b_r.at[g - 1])

                for i in range(3 + direct(g)):
                    spread(g, i).start()

            when_group(g, body)

        def pass_group(g):
            def body():
                arrived(kvp_ref.at[pl.ds(0, 2 + direct(g)), pl.ds(*groups[g])], k_r.at[g])
                for i in range(2 + direct(g)):
                    if not direct(g):
                        pass_on(g, i).start()
                    relay(g, i).start()

            when_group(g, body)

        def relay_group(g):
            def body():
                if not direct(g):
                    arrived(kvp_ref.at[0, pl.ds(*groups[g])], kf_r.at[g])
                    for i in range(2):
                        relay(g, i + 2).start()

            when_group(g, body)

        def norm_group(g):
            def body():
                arrived(kvp_ref.at[pl.ds(0, 4), pl.ds(*groups[g])], kr_r.at[g])

                first, size = groups[g]
                each = next(n for n in (6, 5, 4, 7, 3, 2, 1) if size % n == 0)

                @pl.loop(0, size // each)
                def _(i):
                    for u in range(each):
                        slot = first + i * each + u
                        rows = jnp.concatenate(
                            [kvp_ref[p * 2 + c, slot] for c in range(2) for p in range(xs)], axis=0
                        )
                        kn_ref[slot] = rms_scale(rows, gain_k)
                        vt_ref[slot, 0:width, :] = rows.T

            when_group(g, body)

        spread_group(0)
        for copy in to_sib:
            copy.wait()
        for v, at in ((vu_ref, core), (vus_ref, 1 - core)):
            for h in range(heads):
                bd_ref[at, h * vdim : (h + 1) * vdim, h * width : (h + 1) * width] = v[h]
        count = len(groups)
        project(0)
        for j in range(1, xs):
            hand_tokens(j)
        def weights_step():
            arrived(wc_ref.at[pl.ds(0, tp_n - 1), 0], w_r.at[0])
            for e in range(1, RING):
                weights_on(e).start()

        for g in range(1, count):
            spread_group(g)
            if g == 1:
                pass_group(0)
        if count < 2:
            pass_group(0)
        for d in range(1, tp_n):
            weights_to(d).start()
        if not direct(0):
            relay_group(0)
        passed, normed = 1, 0
        for j in range(1, xs):
            project(j)
        norm_group(normed)
        normed += 1
        for g in range(passed, count):
            pass_group(g)
            if normed < g:
                norm_group(normed)
                normed += 1
        weights_step()
        for g in range(normed, count):
            norm_group(g)


    for low, high, spans in plans:

        @pl.when((kv >= low) & (kv < high))
        def _(spans=spans):
            exchange(spans)

    def listed(b, c):
        block = chosen_s[b, c]
        known = jnp.maximum(block, 0)
        return jnp.where(block < 0, null, map_s[known >> 7, 0, known & (LANES - 1)])

    def attend_block(b):
        q = jnp.concatenate([q_ref[h, p, b] for h in range(2 * heads) for p in range(xs)], axis=0)
        qt = q.T
        acc = jnp.zeros((width + ONES, 2 * heads * half), jnp.float32)
        for i in range(0, picks, STEP):
            at = [listed(b, i + k) for k in range(STEP)]
            keys = jnp.concatenate([kn_ref[s] for s in at], axis=0)
            s = jnp.dot(keys, qt, preferred_element_type=jnp.float32)
            if i == 0:
                key_row = lax.broadcasted_iota(jnp.int32, s.shape, 0)
                query_row = lax.broadcasted_iota(jnp.int32, s.shape, 1) % half + core * half
                s = jnp.where((key_row <= query_row) | (key_row >= BLOCK), s, masked_score)
            p = jnp.exp2(s).astype(jnp.bfloat16)
            values = jnp.concatenate([vt_ref[s] for s in at], axis=1)
            acc = acc + jnp.dot(values, p, preferred_element_type=jnp.float32)
        att = (acc[:width] / acc[width : width + 1]).astype(jnp.bfloat16).T
        out = []
        for h in range(0, 2 * heads, 2):
            two = jnp.concatenate([att[h * half : (h + 1) * half], att[(h + 1) * half : (h + 2) * half]], axis=1)
            out.append(
                lax.dot_general(two, bd_ref[h // 2], (((1,), (1,)), ((), ())), preferred_element_type=jnp.float32)
            )
        return jnp.concatenate(out, axis=1).astype(jnp.bfloat16)

    pairs = blocks // 2

    def heads_to(b, i):
        part = ho_ref.at[x, b]
        return send(part, part, (h_s.at[0], h_r.at[b // 2]), at_tp(same_core((2, 1, -1)[i])))

    def finish(g):
        arrived(ho_ref.at[pl.ds(0, xs - 1), pl.ds(0, 2)], h_r.at[g])
        total = jnp.zeros((BLOCK, 2 * cols), jnp.float32)
        for p in range(xs):
            rows = ho_ref[p, pl.ds(2 * g, 2)].reshape(BLOCK, 2 * cols)
            w = jnp.concatenate([wc_ref[2 * p + c].reshape(RING * wrows, 2 * cols) for c in range(2)], axis=0)
            total = total + jnp.dot(rows, w, preferred_element_type=jnp.float32)
        left, right = total[:, :cols], total[:, cols:]
        px_ref[g] = jnp.where(core == 0, right, left)
        proj_ref[g, core] = jnp.where(core == 0, left, right)
        squares = jnp.sum(total * total, axis=1, keepdims=True)
        ss_ref[tp, pl.ds(g, 1), :] = jnp.broadcast_to(squares, (BLOCK, BLOCK)).T[0:1]
        swap(g).start()

    def swap(g):
        return send(px_ref.at[g], proj_ref.at[g, core], (p_s.at[0], p_r.at[0]), at_tp(sib))

    @pl.loop(0, blocks)
    def _(b):
        ho_ref[x, b] = attend_block(b)
        for i in range(3):
            heads_to(b, i).start()

    arrived(wc_ref.at[:, pl.ds(0, RING - 1)], y_r.at[0])
    for g in range(pairs):
        finish(g)

    def sums(d):
        return send(ss_ref.at[tp], ss_ref.at[tp], (s_s.at[0], s_r.at[0]), at_tp(other_tp(d)))

    for d in range(1, tp_n):
        sums(d).start()

    for j in range(xs):
        arrived(tk_ref.at[pl.ds(0, len(beside) if j else tp_n - 1), 0], t_s.at[j])
    arrived(tk_ref.at[pl.ds(0, 2), pl.ds(0, xs - 1)], tf_s.at[0])
    for n in range(1, kv_n):

        @pl.when(kv == n)
        def _(n=n):
            arrived(chs_ref.at[pl.ds(0, n)], ch_s.at[0])

    arrived(wc_ref.at[pl.ds(0, tp_n - 1), 0], w_s.at[0])
    arrived(wc_ref.at[:, pl.ds(0, RING - 1)], y_s.at[0])
    for n in range(1, kv_n):

        @pl.when(kv == kv_n - 1 - n)
        def _(n=n):
            arrived(out_ref.at[pl.ds(0, n)], b_s.at[0])

    def drain(remote):
        arrived(kvp_ref.at[pl.ds(0, 7), pl.ds(0, blocks)], k_s.at[0])
        for g, (a, b) in enumerate(remote):

            @pl.when(kv >= a)
            def _(g=g, a=a, b=b):
                part = pl.ds(blocks + (a - 1) * PER_OWNER, (b - a) * PER_OWNER)
                arrived(kvp_ref.at[pl.ds(0, 7), part], k_s.at[g + 1])

    for low, high, spans in plans:

        @pl.when((kv >= low) & (kv < high))
        def _(spans=spans):
            drain(spans)

    arrived(ho_ref.at[pl.ds(0, xs - 1)], h_s.at[0])
    arrived(px_ref, p_s.at[0])
    arrived(ss_ref.at[pl.ds(0, tp_n - 1)], s_s.at[0])
    arrived(px_ref, p_r.at[0])
    arrived(ss_ref.at[pl.ds(0, tp_n - 1)], s_r.at[0])
    gains = ogain_ref[:, pl.ds(pl.multiple_of(tp * cols, cols), cols)]
    inverse = []
    for c in range(2):
        total = ss_ref[c]
        for p in range(1, xs):
            total = total + ss_ref[2 * p + c]
        inverse.append(lax.rsqrt(total / (cols * tp_n) + epsilon))

    for g in range(pairs):
        for c in range(2):
            scale = jnp.broadcast_to(inverse[c][g : g + 1], (BLOCK, BLOCK)).T
            scale = jnp.concatenate([scale] * (cols // BLOCK), axis=1)
            rows = (proj_ref[g, c] * scale * gains).astype(jnp.bfloat16)
            for u in range(2):
                o_ref[pl.ds((2 * g + u) * BLOCK + c * half, half), :] = rows[u * half : (u + 1) * half]


def on_device(
    tokens,
    query_weight,
    latent_weight,
    query_gain,
    key_gain,
    value_up,
    out_weight,
    out_gain,
    chosen,
):
    toks, feat = tokens.shape
    width = latent_weight.shape[1]
    heads = query_weight.shape[1] // width
    blocks = toks // BLOCK
    kv_n, tp_n = lax.axis_size("kv"), lax.axis_size("tp")
    cols = out_weight.shape[1] // tp_n
    hv = out_weight.shape[0]
    xs = tp_n // 2
    piece = BLOCK // tp_n
    slots = blocks + (kv_n - 1) * PER_OWNER
    halves = max(1, kv_n * blocks // LANES)
    near = max(len(spans) for _, _, spans in owner_groups(kv_n))
    count = near + 1
    bf, f32, i32 = jnp.bfloat16, jnp.float32, jnp.int32
    dma = pltpu.SemaphoreType.DMA
    vmem = pl.BlockSpec(memory_space=pltpu.VMEM)
    sems = [
        xs, 1, xs, xs, 2, 2, 1, 1, 1, near, count, count, count, count,
        1, 1, 1, 1, 1, blocks // 2, 1, 1, 1, 1,
    ]
    return pl.pallas_call(
        functools.partial(kernel, kv_n, tp_n),
        out_shape=jax.ShapeDtypeStruct((toks, cols), bf),
        in_specs=[pl.BlockSpec(memory_space=pltpu.HBM)] * 9,
        out_specs=vmem,
        scratch_shapes=[
            pltpu.VMEM(chosen.shape, i32),
            pltpu.SMEM(chosen.shape, i32),
            pltpu.VMEM((blocks, 2, xs, piece, feat), bf),
            pltpu.VMEM(latent_weight.shape, bf),
            pltpu.VMEM(query_weight.shape, bf),
            pltpu.VMEM((value_up.shape[0], value_up.shape[2], value_up.shape[1]), bf),
            pltpu.VMEM(out_weight.shape, bf),
            pltpu.VMEM((1, width), f32),
            pltpu.VMEM((1, width), f32),
            pltpu.VMEM((1, cols * tp_n), f32),
            pltpu.VMEM((tp_n, xs, blocks, piece, feat), bf),
            pltpu.VMEM(query_weight.shape, bf),
            pltpu.VMEM((value_up.shape[0], value_up.shape[2], value_up.shape[1]), bf),
            pltpu.VMEM((2 * heads, xs, blocks, piece, width), bf),
            pltpu.VMEM((blocks, piece, width), bf),
            pltpu.VMEM((kv_n - 1, PER_OWNER, piece, width), bf),
            pltpu.VMEM((tp_n, slots, piece, width), bf),
            pltpu.VMEM((slots + 1, BLOCK, width), bf),
            pltpu.VMEM((slots + 1, width + ONES, BLOCK), bf),
            pltpu.VMEM((2, hv, 2 * width), bf),
            pltpu.VMEM((halves, 1, LANES), i32),
            pltpu.VMEM((halves, 1, LANES), i32),
            pltpu.VMEM((kv_n - 1, 1, LANES), i32),
            pltpu.SMEM((halves, 1, LANES), i32),
            pltpu.SMEM((kv_n - 1, 1, LANES), i32),
            pltpu.VMEM((xs, blocks, BLOCK // 2, 2 * hv), bf),
            pltpu.VMEM((tp_n, RING, hv // RING, 2 * cols), bf),
            pltpu.VMEM((blocks // 2, 2, BLOCK, cols), f32),
            pltpu.VMEM((blocks // 2, BLOCK, cols), f32),
            pltpu.VMEM((tp_n, blocks // 2, BLOCK), f32),
            dma((10,)), dma((2,)), *[dma((n,)) for n in sems],
        ],
        compiler_params=pltpu.CompilerParams(
            collective_id=0, has_side_effects=True, vmem_limit_bytes=24 << 20
        ),
    )(*[
        pltpu.with_memory_space_constraint(a, pltpu.HBM)
        for a in (
            tokens.reshape(blocks, 2, xs, piece, feat), query_weight, latent_weight, query_gain[None, :],
            key_gain[None, :], jnp.swapaxes(value_up, 1, 2), out_weight, out_gain[None, :], chosen,
        )
    ])


def solution(mesh):
    in_specs = (
        P("kv", "tp"),
        P(None, "tp"),
        P(),
        P(),
        P(),
        P("tp", None, None),
        P("tp", None),
        P(),
        P("kv", None),
    )
    out_specs = P("kv", "tp")
    return jax.shard_map(
        on_device, mesh=mesh, in_specs=in_specs, out_specs=out_specs, check_vma=False
    )
```

```python
import functools

import jax
import jax.numpy as jnp
from jax import lax
from jax.experimental import pallas as pl
from jax.experimental.pallas import tpu as pltpu
from jax.sharding import PartitionSpec as P

BLOCK = 128
PER_OWNER = 2
RING = 4
OWNERS = 8
STEP = 8
LANES = 128
ONES = 16
MESH = pl.DeviceIdType.MESH

epsilon = 1e-06
masked_score = -1e30


def rms_scale(values, gain_row):
    widened = values.astype(jnp.float32)
    mean_sq = jnp.mean(widened * widened, axis=-1, keepdims=True)
    return (widened * lax.rsqrt(mean_sq + epsilon) * gain_row).astype(jnp.bfloat16)


def prefix_in_owner(values, lane, blocks, inclusive):
    total = values if inclusive else jnp.zeros_like(values)
    for s in range(1, blocks):
        total = total + jnp.where(lane % blocks >= s, pltpu.roll(values, s, 1), 0)
    return total


def send(src, dst, sems, where):
    return pltpu.make_async_remote_copy(
        src_ref=src, dst_ref=dst, send_sem=sems[0], recv_sem=sems[1], device_id=where, device_id_type=MESH
    )


def arrived(part, sem):
    pltpu.make_async_copy(part, part, sem).wait()


def owner_groups(kv_n):
    if kv_n != 8 * RING:
        return [(0, kv_n, [(d, min(d + OWNERS, kv_n)) for d in range(1, kv_n, OWNERS)])]
    return [
        (0, 8, [(1, 8)]),
        (8, 16, [(1, 7), (7, 12), (12, 16)]),
        (16, 20, [(1, 7), (7, 11), (11, 15), (15, 18), (18, 20)]),
        (20, 24, [(1, 9), (17, 24), (9, 13), (13, 17)]),
        (24, 28, [(1, 9), (20, 25), (25, 28), (9, 13), (13, 17), (17, 20)]),
        (28, 32, [(1, 6), (6, 11), (11, 16), (16, 21), (21, 25), (25, 29), (29, 32)]),
    ]


def kernel(
    kv_n, tp_n,
    tok_in, wq_in, wl_in, qgain_in, kgain_in, vu_in, w_in, ogain_in, chosen_in,
    o_ref,
    chosen_ref, chosen_s, tok_ref, wl_ref, wq_ref, vu_ref, w_ref, qgain_ref, kgain_ref, ogain_ref,
    tk_ref, wqs_ref, vus_ref, q_ref, lat_ref, out_ref, kvp_ref, kn_ref, vt_ref, bd_ref,
    map_ref, req_ref, chs_ref, map_s, chs_s,
    ho_ref, wc_ref, proj_ref, px_ref, ss_ref,
    in_s, lc, t_s, tf_s, t_r, tf_r, c_s, c_r, ch_s, ch_r, b_s, b_r, k_s, k_r, kf_r, kr_r,
    w_s, w_r, y_s, y_r, h_s, h_r, p_s, p_r, s_s, s_r,
):
    kv, tp = lax.axis_index("kv"), lax.axis_index("tp")
    core, x = lax.rem(tp, 2), tp // 2
    sib = tp + 1 - 2 * core
    blocks, _, xs, piece, feat = tok_ref.shape
    width = wl_ref.shape[1]
    heads = wq_ref.shape[1] // width
    vdim = vu_ref.shape[1]
    slots = kvp_ref.shape[1]
    picks = chosen_ref.shape[1]
    cols = o_ref.shape[1]
    half = BLOCK // 2
    mine = blocks * piece
    per_row = LANES // blocks
    wrows = w_ref.shape[0] // RING
    y = lax.rem(kv, RING)

    def at_kv(other):
        return {"kv": other, "tp": tp}

    def at_tp(other):
        return {"kv": kv, "tp": other}

    def other_tp(d):
        return lax.rem(tp + d + tp_n, tp_n)

    barrier = pltpu.get_barrier_semaphore()
    for d in range(1, kv_n):
        pl.semaphore_signal(barrier, inc=1, device_id=at_kv(lax.rem(kv + d, kv_n)), device_id_type=MESH)
    for d in range(1, tp_n):
        pl.semaphore_signal(barrier, inc=1, device_id=at_tp(other_tp(d)), device_id_type=MESH)

    loads = [
        pltpu.make_async_copy(a, b, in_s.at[i])
        for i, (a, b) in enumerate([
            (chosen_in, chosen_ref), (chosen_in, chosen_s), (tok_in, tok_ref), (wl_in, wl_ref), (wq_in, wq_ref),
            (vu_in, vu_ref), (w_in, w_ref), (qgain_in, qgain_ref), (kgain_in, kgain_ref), (ogain_in, ogain_ref),
        ])
    ]
    for load in loads:
        load.start()
    loads[0].wait()
    lane = lax.broadcasted_iota(jnp.int32, (blocks, LANES), 1)
    halves = map_ref.shape[0]
    table = chosen_ref[...]
    for g in range(halves):
        hit = jnp.zeros((blocks, LANES), jnp.int32)
        for c in range(picks):
            hit = jnp.where(table[:, c : c + 1] == lane + g * LANES, 1, hit)
        need = jnp.broadcast_to(jnp.max(hit, axis=0, keepdims=True), (blocks, LANES))
        rank = prefix_in_owner(need, lane, blocks, False)
        local = lane % blocks
        dist = kv - (lane // blocks + g * per_row)
        slot = jnp.where(dist == 0, local, blocks + (dist - 1) * PER_OWNER + rank)
        map_ref[g] = jnp.clip(slot, 0, slots - 1)[0:1]
        code = jnp.zeros((blocks, LANES), jnp.int32)
        for k in range(PER_OWNER):
            code = code + jnp.where((need > 0) & (rank == k), local * blocks**k, 0)
        req_ref[g] = prefix_in_owner(code, lane, blocks, True)[0:1]

    pltpu.make_async_copy(map_ref, map_s, lc.at[0]).start()
    for load in loads[1:]:
        load.wait()
    pl.semaphore_wait(barrier, kv_n - 1 + tp_n - 1)

    def chip(i):
        return lax.rem(x + i + xs, xs)

    def same_core(i):
        return 2 * chip(i) + core

    def tokens_to(e, j):
        c = 1 - core if e == 1 else e % 2
        part = chip(e // 2 + j)
        return send(
            tok_ref.at[:, c, part], tk_ref.at[tp, part], (t_s.at[j], t_r.at[j]), at_tp(2 * chip(e // 2) + c)
        )

    beside = [e for e in range(1, tp_n) if e // 2 != 2]

    def tokens_on(j, way):
        step = 1 - 2 * way
        part = tk_ref.at[2 * chip(-step) + way, chip(step + j)]
        return send(part, part, (tf_s.at[0], tf_r.at[j]), at_tp(same_core(step)))

    def ask(d):
        owner = lax.rem(kv - d + kv_n, kv_n)
        return send(
            req_ref.at[owner // per_row], chs_ref.at[d - 1],
            (ch_s.at[0], ch_r.at[0]), at_kv(owner),
        )

    def serves(d):
        return kv + d < kv_n

    def weights_to(d):
        other = other_tp(d)
        part = w_ref.at[
            pl.ds(pl.multiple_of(y * wrows, wrows), wrows),
            pl.ds(pl.multiple_of(other // 2 * 2 * cols, 2 * cols), 2 * cols),
        ]
        return send(part, wc_ref.at[tp, y], (w_s.at[0], w_r.at[0]), at_tp(other))

    def weights_on(e):
        part = wc_ref.at[:, y]
        other = kv - y + lax.rem(y + e, RING)
        return send(part, part, (y_s.at[0], y_r.at[0]), at_kv(other))

    to_sib = [
        send(wq_ref, wqs_ref, (c_s.at[0], c_r.at[0]), at_tp(sib)),
        send(vu_ref, vus_ref, (c_s.at[1], c_r.at[1]), at_tp(sib)),
    ]

    for e in (5, 4, 3, 2, 7, 6, 1):
        tokens_to(e, 0).start()
    for d in range(1, kv_n):

        @pl.when(kv - d >= 0)
        def _(d=d):
            ask(d).start()

    for j in range(1, xs):
        for e in beside:
            tokens_to(e, j).start()
    for p in range(xs):
        tk_ref[tp, p] = tok_ref[:, core, p]
    wc_ref[tp, y] = w_ref[
        pl.ds(pl.multiple_of(y * wrows, wrows), wrows), pl.ds(pl.multiple_of(x * 2 * cols, 2 * cols), 2 * cols)
    ]
    null = slots
    vt_ref[:, width:, :] = jnp.ones((slots + 1, ONES, BLOCK), jnp.bfloat16)
    kn_ref[null] = jnp.zeros((BLOCK, width), jnp.bfloat16)
    vt_ref[null] = jnp.zeros((width + ONES, BLOCK), jnp.bfloat16)
    bd_ref[...] = jnp.zeros_like(bd_ref)

    def features(p):
        return jnp.concatenate([tk_ref[t, p].reshape(mine, feat) for t in range(tp_n)], axis=1)

    def hand_tokens(j):
        if j:
            arrived(tk_ref.at[pl.ds(0, len(beside)), 0], t_r.at[j])
        if j != 1:
            tokens_on((j - 1) % xs, 0).start()
        if j < xs - 1:
            tokens_on(j + 1, 1).start()

    for n in range(1, kv_n):

        @pl.when(kv == kv_n - 1 - n)
        def _(n=n):
            arrived(chs_ref.at[pl.ds(0, n)], ch_r.at[0])

    to_smem = pltpu.make_async_copy(chs_ref, chs_s, lc.at[1])
    to_smem.start()
    arrived(tk_ref.at[pl.ds(0, tp_n - 1), 0], t_r.at[0])
    hand_tokens(0)
    lat = jnp.dot(features(x), wl_ref[...], preferred_element_type=jnp.float32).astype(jnp.bfloat16)
    lat_ref[...] = lat.reshape(blocks, piece, width)
    kvp_ref[tp, 0:blocks] = lat.reshape(blocks, piece, width)

    pltpu.make_async_copy(map_ref, map_s, lc.at[0]).wait()
    to_smem.wait()

    for copy in to_sib:
        copy.start()
    def slots_of(d):
        return pl.ds(blocks + (d - 1) * PER_OWNER, PER_OWNER)

    plans = owner_groups(kv_n)

    def span_of(d):
        index = 0
        for low, _, spans in plans:
            here = next((i for i, (a, b) in enumerate(spans) if a <= d < b), 0)
            index = jnp.where(kv + d >= low, here, index)
        return index

    def give(d):
        return send(
            out_ref.at[d - 1], kvp_ref.at[tp, slots_of(d)], (b_s.at[0], b_r.at[span_of(d)]), at_kv(lax.rem(kv + d, kv_n))
        )

    at_lane = lax.rem(kv, per_row) * blocks + blocks - 1
    for d in range(1, kv_n):

        @pl.when(serves(d))
        def _(d=d):
            code = chs_s[d - 1, 0, at_lane]
            for k in range(PER_OWNER):
                out_ref[d - 1, k] = lat_ref[(code >> (3 * k)) & (blocks - 1)]
            give(d).start()

    gain_k = kgain_ref[...]
    gain_q = qgain_ref[...] * (width**-0.5 * 1.4426950408889634)

    def project(j):
        if j:
            arrived(tk_ref.at[pl.ds(0, 2), 0], tf_r.at[j])
        p = lax.rem(x + j, xs)
        rows = features(p)
        for w, at in ((wq_ref, core), (wqs_ref, 1 - core)):
            qs = jnp.dot(rows, w[...], preferred_element_type=jnp.float32).astype(jnp.bfloat16)
            for h in range(heads):
                part = rms_scale(qs[:, h * width : (h + 1) * width], gain_q)
                q_ref[at * heads + h, p] = part.reshape(blocks, piece, width)

    def exchange(remote):
        groups = [(0, blocks)] + [
            (blocks + (a - 1) * PER_OWNER, (b - a) * PER_OWNER) for a, b in remote
        ]

        def direct(g):
            return g >= min(1, len(groups) - 1)

        def halves_of(g):
            first, size = groups[g]
            cut = (size + 1) // 2
            return [pl.ds(first, cut), pl.ds(first + cut, size - cut)]

        def spread(g, i):
            part = kvp_ref.at[tp, pl.ds(*groups[g])]
            where = sib if i == 2 else same_core((1, -1, 0, 2)[i])
            return send(part, part, (k_s.at[g], (kr_r if i == 2 else k_r).at[g]), at_tp(where))

        def pass_on(g, way):
            step = 1 - 2 * way
            part = kvp_ref.at[same_core(-step), halves_of(g)[way]]
            return send(part, part, (k_s.at[g], kf_r.at[g]), at_tp(same_core(step)))

        def relay(g, i):
            if i < 2 or direct(g):
                part = kvp_ref.at[same_core((-1, 1, 2)[i]), pl.ds(*groups[g])]
            else:
                part = kvp_ref.at[same_core(2), halves_of(g)[i - 2]]
            return send(part, part, (k_s.at[g], kr_r.at[g]), at_tp(sib))

        def when_group(g, body):
            if g == 0:
                body()
            else:
                pl.when(kv >= remote[g - 1][0])(body)

        def spread_group(g):
            def body():
                if g:
                    a, b = remote[g - 1]
                    for n in range(1, b - a + 1):

                        @pl.when((kv >= b - 1) if n == b - a else (kv == a + n - 1))
                        def _(n=n):
                            arrived(kvp_ref.at[tp, pl.ds(groups[g][0], n * PER_OWNER)], b_r.at[g - 1])

                for i in range(3 + direct(g)):
                    spread(g, i).start()

            when_group(g, body)

        def pass_group(g):
            def body():
                arrived(kvp_ref.at[pl.ds(0, 2 + direct(g)), pl.ds(*groups[g])], k_r.at[g])
                for i in range(2 + direct(g)):
                    if not direct(g):
                        pass_on(g, i).start()
                    relay(g, i).start()

            when_group(g, body)

        def relay_group(g):
            def body():
                if not direct(g):
                    arrived(kvp_ref.at[0, pl.ds(*groups[g])], kf_r.at[g])
                    for i in range(2):
                        relay(g, i + 2).start()

            when_group(g, body)

        def norm_group(g):
            def body():
                arrived(kvp_ref.at[pl.ds(0, 4), pl.ds(*groups[g])], kr_r.at[g])

                first, size = groups[g]
                each = next(n for n in (6, 5, 4, 7, 3, 2, 1) if size % n == 0)

                @pl.loop(0, size // each)
                def _(i):
                    for u in range(each):
                        slot = first + i * each + u
                        rows = jnp.concatenate(
                            [kvp_ref[p * 2 + c, slot] for c in range(2) for p in range(xs)], axis=0
                        )
                        kn_ref[slot] = rms_scale(rows, gain_k)
                        vt_ref[slot, 0:width, :] = rows.T

            when_group(g, body)

        spread_group(0)
        count = len(groups)
        for j in range(1, xs):
            hand_tokens(j)
        for copy in to_sib:
            copy.wait()
        for v, at in ((vu_ref, core), (vus_ref, 1 - core)):
            for h in range(heads):
                bd_ref[at, h * vdim : (h + 1) * vdim, h * width : (h + 1) * width] = v[h]
        project(0)
        def weights_step():
            arrived(wc_ref.at[pl.ds(0, tp_n - 1), 0], w_r.at[0])
            for e in range(1, RING):
                weights_on(e).start()

        for g in range(1, count):
            spread_group(g)
            if g == 1:
                pass_group(0)
        if count < 2:
            pass_group(0)
        for d in range(1, tp_n):
            weights_to(d).start()
        if not direct(0):
            relay_group(0)
        passed, normed = 1, 0
        for j in range(1, xs):
            project(j)
        norm_group(normed)
        normed += 1
        for g in range(passed, count):
            pass_group(g)
            if normed < g:
                norm_group(normed)
                normed += 1
        weights_step()
        for g in range(normed, count):
            norm_group(g)


    for low, high, spans in plans:

        @pl.when((kv >= low) & (kv < high))
        def _(spans=spans):
            exchange(spans)

    def listed(b, c):
        block = chosen_s[b, c]
        known = jnp.maximum(block, 0)
        return jnp.where(block < 0, null, map_s[known >> 7, 0, known & (LANES - 1)])

    def attend_block(b):
        q = jnp.concatenate([q_ref[h, p, b] for h in range(2 * heads) for p in range(xs)], axis=0)
        qt = q.T
        acc = jnp.zeros((width + ONES, 2 * heads * half), jnp.float32)
        for i in range(0, picks, STEP):
            at = [listed(b, i + k) for k in range(STEP)]
            keys = jnp.concatenate([kn_ref[s] for s in at], axis=0)
            s = jnp.dot(keys, qt, preferred_element_type=jnp.float32)
            if i == 0:
                key_row = lax.broadcasted_iota(jnp.int32, s.shape, 0)
                query_row = lax.broadcasted_iota(jnp.int32, s.shape, 1) % half + core * half
                s = jnp.where((key_row <= query_row) | (key_row >= BLOCK), s, masked_score)
            p = jnp.exp2(s).astype(jnp.bfloat16)
            values = jnp.concatenate([vt_ref[s] for s in at], axis=1)
            acc = acc + jnp.dot(values, p, preferred_element_type=jnp.float32)
        att = (acc[:width] / acc[width : width + 1]).astype(jnp.bfloat16).T
        out = []
        for h in range(0, 2 * heads, 2):
            two = jnp.concatenate([att[h * half : (h + 1) * half], att[(h + 1) * half : (h + 2) * half]], axis=1)
            out.append(
                lax.dot_general(two, bd_ref[h // 2], (((1,), (1,)), ((), ())), preferred_element_type=jnp.float32)
            )
        return jnp.concatenate(out, axis=1).astype(jnp.bfloat16)

    pairs = blocks // 2

    def heads_to(b, i):
        part = ho_ref.at[x, b]
        return send(part, part, (h_s.at[0], h_r.at[b // 2]), at_tp(same_core((2, 1, -1)[i])))

    def finish(g):
        arrived(ho_ref.at[pl.ds(0, xs - 1), pl.ds(0, 2)], h_r.at[g])
        total = jnp.zeros((BLOCK, 2 * cols), jnp.float32)
        for p in range(xs):
            rows = ho_ref[p, pl.ds(2 * g, 2)].reshape(BLOCK, 2 * cols)
            w = jnp.concatenate([wc_ref[2 * p + c].reshape(RING * wrows, 2 * cols) for c in range(2)], axis=0)
            total = total + jnp.dot(rows, w, preferred_element_type=jnp.float32)
        left, right = total[:, :cols], total[:, cols:]
        px_ref[g] = jnp.where(core == 0, right, left)
        proj_ref[g, core] = jnp.where(core == 0, left, right)
        squares = jnp.sum(total * total, axis=1, keepdims=True)
        ss_ref[tp, pl.ds(g, 1), :] = jnp.broadcast_to(squares, (BLOCK, BLOCK)).T[0:1]
        swap(g).start()

    def swap(g):
        return send(px_ref.at[g], proj_ref.at[g, core], (p_s.at[0], p_r.at[0]), at_tp(sib))

    @pl.loop(0, blocks)
    def _(b):
        ho_ref[x, b] = attend_block(b)
        for i in range(3):
            heads_to(b, i).start()

    arrived(wc_ref.at[:, pl.ds(0, RING - 1)], y_r.at[0])
    for g in range(pairs):
        finish(g)

    def sums(d):
        return send(ss_ref.at[tp], ss_ref.at[tp], (s_s.at[0], s_r.at[0]), at_tp(other_tp(d)))

    for d in range(1, tp_n):
        sums(d).start()

    for j in range(xs):
        arrived(tk_ref.at[pl.ds(0, len(beside) if j else tp_n - 1), 0], t_s.at[j])
    arrived(tk_ref.at[pl.ds(0, 2), pl.ds(0, xs - 1)], tf_s.at[0])
    for n in range(1, kv_n):

        @pl.when(kv == n)
        def _(n=n):
            arrived(chs_ref.at[pl.ds(0, n)], ch_s.at[0])

    arrived(wc_ref.at[pl.ds(0, tp_n - 1), 0], w_s.at[0])
    arrived(wc_ref.at[:, pl.ds(0, RING - 1)], y_s.at[0])
    for n in range(1, kv_n):

        @pl.when(kv == kv_n - 1 - n)
        def _(n=n):
            arrived(out_ref.at[pl.ds(0, n)], b_s.at[0])

    def drain(remote):
        arrived(kvp_ref.at[pl.ds(0, 7), pl.ds(0, blocks)], k_s.at[0])
        for g, (a, b) in enumerate(remote):

            @pl.when(kv >= a)
            def _(g=g, a=a, b=b):
                part = pl.ds(blocks + (a - 1) * PER_OWNER, (b - a) * PER_OWNER)
                arrived(kvp_ref.at[pl.ds(0, 7), part], k_s.at[g + 1])

    for low, high, spans in plans:

        @pl.when((kv >= low) & (kv < high))
        def _(spans=spans):
            drain(spans)

    arrived(ho_ref.at[pl.ds(0, xs - 1)], h_s.at[0])
    arrived(px_ref, p_s.at[0])
    arrived(ss_ref.at[pl.ds(0, tp_n - 1)], s_s.at[0])
    arrived(px_ref, p_r.at[0])
    arrived(ss_ref.at[pl.ds(0, tp_n - 1)], s_r.at[0])
    gains = ogain_ref[:, pl.ds(pl.multiple_of(tp * cols, cols), cols)]
    inverse = []
    for c in range(2):
        total = ss_ref[c]
        for p in range(1, xs):
            total = total + ss_ref[2 * p + c]
        inverse.append(lax.rsqrt(total / (cols * tp_n) + epsilon))

    for g in range(pairs):
        for c in range(2):
            scale = jnp.broadcast_to(inverse[c][g : g + 1], (BLOCK, BLOCK)).T
            scale = jnp.concatenate([scale] * (cols // BLOCK), axis=1)
            rows = (proj_ref[g, c] * scale * gains).astype(jnp.bfloat16)
            for u in range(2):
                o_ref[pl.ds((2 * g + u) * BLOCK + c * half, half), :] = rows[u * half : (u + 1) * half]


def on_device(
    tokens,
    query_weight,
    latent_weight,
    query_gain,
    key_gain,
    value_up,
    out_weight,
    out_gain,
    chosen,
):
    toks, feat = tokens.shape
    width = latent_weight.shape[1]
    heads = query_weight.shape[1] // width
    blocks = toks // BLOCK
    kv_n, tp_n = lax.axis_size("kv"), lax.axis_size("tp")
    cols = out_weight.shape[1] // tp_n
    hv = out_weight.shape[0]
    xs = tp_n // 2
    piece = BLOCK // tp_n
    slots = blocks + (kv_n - 1) * PER_OWNER
    halves = max(1, kv_n * blocks // LANES)
    near = max(len(spans) for _, _, spans in owner_groups(kv_n))
    count = near + 1
    bf, f32, i32 = jnp.bfloat16, jnp.float32, jnp.int32
    dma = pltpu.SemaphoreType.DMA
    vmem = pl.BlockSpec(memory_space=pltpu.VMEM)
    sems = [
        xs, 1, xs, xs, 2, 2, 1, 1, 1, near, count, count, count, count,
        1, 1, 1, 1, 1, blocks // 2, 1, 1, 1, 1,
    ]
    return pl.pallas_call(
        functools.partial(kernel, kv_n, tp_n),
        out_shape=jax.ShapeDtypeStruct((toks, cols), bf),
        in_specs=[pl.BlockSpec(memory_space=pltpu.HBM)] * 9,
        out_specs=vmem,
        scratch_shapes=[
            pltpu.VMEM(chosen.shape, i32),
            pltpu.SMEM(chosen.shape, i32),
            pltpu.VMEM((blocks, 2, xs, piece, feat), bf),
            pltpu.VMEM(latent_weight.shape, bf),
            pltpu.VMEM(query_weight.shape, bf),
            pltpu.VMEM((value_up.shape[0], value_up.shape[2], value_up.shape[1]), bf),
            pltpu.VMEM(out_weight.shape, bf),
            pltpu.VMEM((1, width), f32),
            pltpu.VMEM((1, width), f32),
            pltpu.VMEM((1, cols * tp_n), f32),
            pltpu.VMEM((tp_n, xs, blocks, piece, feat), bf),
            pltpu.VMEM(query_weight.shape, bf),
            pltpu.VMEM((value_up.shape[0], value_up.shape[2], value_up.shape[1]), bf),
            pltpu.VMEM((2 * heads, xs, blocks, piece, width), bf),
            pltpu.VMEM((blocks, piece, width), bf),
            pltpu.VMEM((kv_n - 1, PER_OWNER, piece, width), bf),
            pltpu.VMEM((tp_n, slots, piece, width), bf),
            pltpu.VMEM((slots + 1, BLOCK, width), bf),
            pltpu.VMEM((slots + 1, width + ONES, BLOCK), bf),
            pltpu.VMEM((2, hv, 2 * width), bf),
            pltpu.VMEM((halves, 1, LANES), i32),
            pltpu.VMEM((halves, 1, LANES), i32),
            pltpu.VMEM((kv_n - 1, 1, LANES), i32),
            pltpu.SMEM((halves, 1, LANES), i32),
            pltpu.SMEM((kv_n - 1, 1, LANES), i32),
            pltpu.VMEM((xs, blocks, BLOCK // 2, 2 * hv), bf),
            pltpu.VMEM((tp_n, RING, hv // RING, 2 * cols), bf),
            pltpu.VMEM((blocks // 2, 2, BLOCK, cols), f32),
            pltpu.VMEM((blocks // 2, BLOCK, cols), f32),
            pltpu.VMEM((tp_n, blocks // 2, BLOCK), f32),
            dma((10,)), dma((2,)), *[dma((n,)) for n in sems],
        ],
        compiler_params=pltpu.CompilerParams(
            collective_id=0, has_side_effects=True, vmem_limit_bytes=24 << 20
        ),
    )(*[
        pltpu.with_memory_space_constraint(a, pltpu.HBM)
        for a in (
            tokens.reshape(blocks, 2, xs, piece, feat), query_weight, latent_weight, query_gain[None, :],
            key_gain[None, :], jnp.swapaxes(value_up, 1, 2), out_weight, out_gain[None, :], chosen,
        )
    ])


def solution(mesh):
    in_specs = (
        P("kv", "tp"),
        P(None, "tp"),
        P(),
        P(),
        P(),
        P("tp", None, None),
        P("tp", None),
        P(),
        P("kv", None),
    )
    out_specs = P("kv", "tp")
    return jax.shard_map(
        on_device, mesh=mesh, in_specs=in_specs, out_specs=out_specs, check_vma=False
    )
```

```python
import functools

import jax
import jax.numpy as jnp
from jax import lax
from jax.experimental import pallas as pl
from jax.experimental.pallas import tpu as pltpu
from jax.sharding import PartitionSpec as P

BLOCK = 128
PER_OWNER = 2
RING = 4
OWNERS = 8
STEP = 8
LANES = 128
ONES = 16
MESH = pl.DeviceIdType.MESH

epsilon = 1e-06
masked_score = -1e30


def rms_scale(values, gain_row):
    widened = values.astype(jnp.float32)
    mean_sq = jnp.mean(widened * widened, axis=-1, keepdims=True)
    return (widened * lax.rsqrt(mean_sq + epsilon) * gain_row).astype(jnp.bfloat16)


def prefix_in_owner(values, lane, blocks, inclusive):
    total = values if inclusive else jnp.zeros_like(values)
    for s in range(1, blocks):
        total = total + jnp.where(lane % blocks >= s, pltpu.roll(values, s, 1), 0)
    return total


def send(src, dst, sems, where):
    return pltpu.make_async_remote_copy(
        src_ref=src, dst_ref=dst, send_sem=sems[0], recv_sem=sems[1], device_id=where, device_id_type=MESH
    )


def arrived(part, sem):
    pltpu.make_async_copy(part, part, sem).wait()


def owner_groups(kv_n):
    if kv_n != 8 * RING:
        return [(0, kv_n, [(d, min(d + OWNERS, kv_n)) for d in range(1, kv_n, OWNERS)])]
    return [
        (0, 8, [(1, 8)]),
        (8, 16, [(1, 7), (7, 12), (12, 16)]),
        (16, 20, [(1, 7), (7, 11), (11, 15), (15, 18), (18, 20)]),
        (20, 24, [(1, 9), (17, 24), (9, 13), (13, 17)]),
        (24, 28, [(1, 9), (20, 25), (25, 28), (9, 13), (13, 17), (17, 20)]),
        (28, 32, [(1, 6), (6, 11), (11, 16), (16, 21), (21, 25), (25, 28), (28, 30), (30, 32)]),
    ]


def kernel(
    kv_n, tp_n,
    tok_in, wq_in, wl_in, qgain_in, kgain_in, vu_in, w_in, ogain_in, chosen_in,
    o_ref,
    chosen_ref, chosen_s, tok_ref, wl_ref, wq_ref, vu_ref, w_ref, qgain_ref, kgain_ref, ogain_ref,
    tk_ref, wqs_ref, vus_ref, q_ref, lat_ref, out_ref, kvp_ref, kn_ref, vt_ref, bd_ref,
    map_ref, req_ref, chs_ref, map_s, chs_s,
    ho_ref, wc_ref, proj_ref, px_ref, ss_ref,
    in_s, lc, t_s, tf_s, t_r, tf_r, c_s, c_r, ch_s, ch_r, b_s, b_r, k_s, k_r, kf_r, kr_r,
    w_s, w_r, y_s, y_r, h_s, h_r, p_s, p_r, s_s, s_r,
):
    kv, tp = lax.axis_index("kv"), lax.axis_index("tp")
    core, x = lax.rem(tp, 2), tp // 2
    sib = tp + 1 - 2 * core
    blocks, _, xs, piece, feat = tok_ref.shape
    width = wl_ref.shape[1]
    heads = wq_ref.shape[1] // width
    vdim = vu_ref.shape[1]
    slots = kvp_ref.shape[1]
    picks = chosen_ref.shape[1]
    cols = o_ref.shape[1]
    half = BLOCK // 2
    mine = blocks * piece
    per_row = LANES // blocks
    wrows = w_ref.shape[0] // RING
    y = lax.rem(kv, RING)

    def at_kv(other):
        return {"kv": other, "tp": tp}

    def at_tp(other):
        return {"kv": kv, "tp": other}

    def other_tp(d):
        return lax.rem(tp + d + tp_n, tp_n)

    barrier = pltpu.get_barrier_semaphore()
    for d in range(1, kv_n):
        pl.semaphore_signal(barrier, inc=1, device_id=at_kv(lax.rem(kv + d, kv_n)), device_id_type=MESH)
    for d in range(1, tp_n):
        pl.semaphore_signal(barrier, inc=1, device_id=at_tp(other_tp(d)), device_id_type=MESH)

    loads = [
        pltpu.make_async_copy(a, b, in_s.at[i])
        for i, (a, b) in enumerate([
            (chosen_in, chosen_ref), (chosen_in, chosen_s), (tok_in, tok_ref), (wl_in, wl_ref), (wq_in, wq_ref),
            (vu_in, vu_ref), (w_in, w_ref), (qgain_in, qgain_ref), (kgain_in, kgain_ref), (ogain_in, ogain_ref),
        ])
    ]
    for load in loads:
        load.start()
    loads[0].wait()
    lane = lax.broadcasted_iota(jnp.int32, (blocks, LANES), 1)
    halves = map_ref.shape[0]
    table = chosen_ref[...]
    for g in range(halves):
        hit = jnp.zeros((blocks, LANES), jnp.int32)
        for c in range(picks):
            hit = jnp.where(table[:, c : c + 1] == lane + g * LANES, 1, hit)
        need = jnp.broadcast_to(jnp.max(hit, axis=0, keepdims=True), (blocks, LANES))
        rank = prefix_in_owner(need, lane, blocks, False)
        local = lane % blocks
        dist = kv - (lane // blocks + g * per_row)
        slot = jnp.where(dist == 0, local, blocks + (dist - 1) * PER_OWNER + rank)
        map_ref[g] = jnp.clip(slot, 0, slots - 1)[0:1]
        code = jnp.zeros((blocks, LANES), jnp.int32)
        for k in range(PER_OWNER):
            code = code + jnp.where((need > 0) & (rank == k), local * blocks**k, 0)
        req_ref[g] = prefix_in_owner(code, lane, blocks, True)[0:1]

    pltpu.make_async_copy(map_ref, map_s, lc.at[0]).start()
    for load in loads[1:]:
        load.wait()
    pl.semaphore_wait(barrier, kv_n - 1 + tp_n - 1)

    def chip(i):
        return lax.rem(x + i + xs, xs)

    def same_core(i):
        return 2 * chip(i) + core

    def tokens_to(e, j):
        c = 1 - core if e == 1 else e % 2
        part = chip(e // 2 + j)
        return send(
            tok_ref.at[:, c, part], tk_ref.at[tp, part], (t_s.at[j], t_r.at[j]), at_tp(2 * chip(e // 2) + c)
        )

    beside = [e for e in range(1, tp_n) if e // 2 != 2]

    def tokens_on(j, way):
        step = 1 - 2 * way
        part = tk_ref.at[2 * chip(-step) + way, chip(step + j)]
        return send(part, part, (tf_s.at[0], tf_r.at[j]), at_tp(same_core(step)))

    def ask(d):
        owner = lax.rem(kv - d + kv_n, kv_n)
        return send(
            req_ref.at[owner // per_row], chs_ref.at[d - 1],
            (ch_s.at[0], ch_r.at[0]), at_kv(owner),
        )

    def serves(d):
        return kv + d < kv_n

    def weights_to(d):
        other = other_tp(d)
        part = w_ref.at[
            pl.ds(pl.multiple_of(y * wrows, wrows), wrows),
            pl.ds(pl.multiple_of(other // 2 * 2 * cols, 2 * cols), 2 * cols),
        ]
        return send(part, wc_ref.at[tp, y], (w_s.at[0], w_r.at[0]), at_tp(other))

    def weights_on(e):
        part = wc_ref.at[:, y]
        other = kv - y + lax.rem(y + e, RING)
        return send(part, part, (y_s.at[0], y_r.at[0]), at_kv(other))

    to_sib = [
        send(wq_ref, wqs_ref, (c_s.at[0], c_r.at[0]), at_tp(sib)),
        send(vu_ref, vus_ref, (c_s.at[1], c_r.at[1]), at_tp(sib)),
    ]

    for e in (5, 4, 3, 2, 7, 6, 1):
        tokens_to(e, 0).start()
    for d in range(1, kv_n):

        @pl.when(kv - d >= 0)
        def _(d=d):
            ask(d).start()

    for j in range(1, xs):
        for e in beside:
            tokens_to(e, j).start()
    for p in range(xs):
        tk_ref[tp, p] = tok_ref[:, core, p]
    wc_ref[tp, y] = w_ref[
        pl.ds(pl.multiple_of(y * wrows, wrows), wrows), pl.ds(pl.multiple_of(x * 2 * cols, 2 * cols), 2 * cols)
    ]
    null = slots
    vt_ref[:, width:, :] = jnp.ones((slots + 1, ONES, BLOCK), jnp.bfloat16)
    kn_ref[null] = jnp.zeros((BLOCK, width), jnp.bfloat16)
    vt_ref[null] = jnp.zeros((width + ONES, BLOCK), jnp.bfloat16)
    bd_ref[...] = jnp.zeros_like(bd_ref)

    def features(p):
        return jnp.concatenate([tk_ref[t, p].reshape(mine, feat) for t in range(tp_n)], axis=1)

    def hand_tokens(j):
        if j:
            arrived(tk_ref.at[pl.ds(0, len(beside)), 0], t_r.at[j])
        if j != 1:
            tokens_on((j - 1) % xs, 0).start()
        if j < xs - 1:
            tokens_on(j + 1, 1).start()

    for n in range(1, kv_n):

        @pl.when(kv == kv_n - 1 - n)
        def _(n=n):
            arrived(chs_ref.at[pl.ds(0, n)], ch_r.at[0])

    to_smem = pltpu.make_async_copy(chs_ref, chs_s, lc.at[1])
    to_smem.start()
    arrived(tk_ref.at[pl.ds(0, tp_n - 1), 0], t_r.at[0])
    hand_tokens(0)
    lat = jnp.dot(features(x), wl_ref[...], preferred_element_type=jnp.float32).astype(jnp.bfloat16)
    lat_ref[...] = lat.reshape(blocks, piece, width)
    kvp_ref[tp, 0:blocks] = lat.reshape(blocks, piece, width)

    pltpu.make_async_copy(map_ref, map_s, lc.at[0]).wait()
    to_smem.wait()

    for copy in to_sib:
        copy.start()
    def slots_of(d):
        return pl.ds(blocks + (d - 1) * PER_OWNER, PER_OWNER)

    plans = owner_groups(kv_n)

    def span_of(d):
        index = 0
        for low, _, spans in plans:
            here = next((i for i, (a, b) in enumerate(spans) if a <= d < b), 0)
            index = jnp.where(kv + d >= low, here, index)
        return index

    def give(d):
        return send(
            out_ref.at[d - 1], kvp_ref.at[tp, slots_of(d)], (b_s.at[0], b_r.at[span_of(d)]), at_kv(lax.rem(kv + d, kv_n))
        )

    at_lane = lax.rem(kv, per_row) * blocks + blocks - 1
    for d in range(1, kv_n):

        @pl.when(serves(d))
        def _(d=d):
            code = chs_s[d - 1, 0, at_lane]
            for k in range(PER_OWNER):
                out_ref[d - 1, k] = lat_ref[(code >> (3 * k)) & (blocks - 1)]
            give(d).start()

    gain_k = kgain_ref[...]
    gain_q = qgain_ref[...] * (width**-0.5 * 1.4426950408889634)

    def project(j):
        if j:
            arrived(tk_ref.at[pl.ds(0, 2), 0], tf_r.at[j])
        p = lax.rem(x + j, xs)
        rows = features(p)
        for w, at in ((wq_ref, core), (wqs_ref, 1 - core)):
            qs = jnp.dot(rows, w[...], preferred_element_type=jnp.float32).astype(jnp.bfloat16)
            for h in range(heads):
                part = rms_scale(qs[:, h * width : (h + 1) * width], gain_q)
                q_ref[at * heads + h, p] = part.reshape(blocks, piece, width)

    def exchange(remote):
        groups = [(0, blocks)] + [
            (blocks + (a - 1) * PER_OWNER, (b - a) * PER_OWNER) for a, b in remote
        ]

        def direct(g):
            return g >= min(1, len(groups) - 1)

        def halves_of(g):
            first, size = groups[g]
            cut = (size + 1) // 2
            return [pl.ds(first, cut), pl.ds(first + cut, size - cut)]

        def spread(g, i):
            part = kvp_ref.at[tp, pl.ds(*groups[g])]
            where = sib if i == 2 else same_core((1, -1, 0, 2)[i])
            return send(part, part, (k_s.at[g], (kr_r if i == 2 else k_r).at[g]), at_tp(where))

        def pass_on(g, way):
            step = 1 - 2 * way
            part = kvp_ref.at[same_core(-step), halves_of(g)[way]]
            return send(part, part, (k_s.at[g], kf_r.at[g]), at_tp(same_core(step)))

        def relay(g, i):
            if i < 2 or direct(g):
                part = kvp_ref.at[same_core((-1, 1, 2)[i]), pl.ds(*groups[g])]
            else:
                part = kvp_ref.at[same_core(2), halves_of(g)[i - 2]]
            return send(part, part, (k_s.at[g], kr_r.at[g]), at_tp(sib))

        def when_group(g, body):
            if g == 0:
                body()
            else:
                pl.when(kv >= remote[g - 1][0])(body)

        def spread_group(g):
            def body():
                if g:
                    a, b = remote[g - 1]
                    for n in range(1, b - a + 1):

                        @pl.when((kv >= b - 1) if n == b - a else (kv == a + n - 1))
                        def _(n=n):
                            arrived(kvp_ref.at[tp, pl.ds(groups[g][0], n * PER_OWNER)], b_r.at[g - 1])

                for i in range(3 + direct(g)):
                    spread(g, i).start()

            when_group(g, body)

        def pass_group(g):
            def body():
                arrived(kvp_ref.at[pl.ds(0, 2 + direct(g)), pl.ds(*groups[g])], k_r.at[g])
                for i in range(2 + direct(g)):
                    if not direct(g):
                        pass_on(g, i).start()
                    relay(g, i).start()

            when_group(g, body)

        def relay_group(g):
            def body():
                if not direct(g):
                    arrived(kvp_ref.at[0, pl.ds(*groups[g])], kf_r.at[g])
                    for i in range(2):
                        relay(g, i + 2).start()

            when_group(g, body)

        def norm_group(g):
            def body():
                arrived(kvp_ref.at[pl.ds(0, 4), pl.ds(*groups[g])], kr_r.at[g])

                first, size = groups[g]
                each = next(n for n in (6, 5, 4, 7, 3, 2, 1) if size % n == 0)

                @pl.loop(0, size // each)
                def _(i):
                    for u in range(each):
                        slot = first + i * each + u
                        rows = jnp.concatenate(
                            [kvp_ref[p * 2 + c, slot] for c in range(2) for p in range(xs)], axis=0
                        )
                        kn_ref[slot] = rms_scale(rows, gain_k)
                        vt_ref[slot, 0:width, :] = rows.T

            when_group(g, body)

        spread_group(0)
        count = len(groups)
        for j in range(1, xs):
            hand_tokens(j)
        for copy in to_sib:
            copy.wait()
        for v, at in ((vu_ref, core), (vus_ref, 1 - core)):
            for h in range(heads):
                bd_ref[at, h * vdim : (h + 1) * vdim, h * width : (h + 1) * width] = v[h]
        project(0)
        def weights_step():
            arrived(wc_ref.at[pl.ds(0, tp_n - 1), 0], w_r.at[0])
            for e in range(1, RING):
                weights_on(e).start()

        for g in range(1, count):
            spread_group(g)
            if g == 1:
                pass_group(0)
        if count < 2:
            pass_group(0)
        for d in range(1, tp_n):
            weights_to(d).start()
        if not direct(0):
            relay_group(0)
        passed, normed = 1, 0
        for j in range(1, xs):
            project(j)
        norm_group(normed)
        normed += 1
        for g in range(passed, count):
            pass_group(g)
            if normed < g:
                norm_group(normed)
                normed += 1
        weights_step()
        for g in range(normed, count):
            norm_group(g)


    for low, high, spans in plans:

        @pl.when((kv >= low) & (kv < high))
        def _(spans=spans):
            exchange(spans)

    def listed(b, c):
        block = chosen_s[b, c]
        known = jnp.maximum(block, 0)
        return jnp.where(block < 0, null, map_s[known >> 7, 0, known & (LANES - 1)])

    def attend_block(b):
        q = jnp.concatenate([q_ref[h, p, b] for h in range(2 * heads) for p in range(xs)], axis=0)
        qt = q.T
        acc = jnp.zeros((width + ONES, 2 * heads * half), jnp.float32)
        for i in range(0, picks, STEP):
            at = [listed(b, i + k) for k in range(STEP)]
            keys = jnp.concatenate([kn_ref[s] for s in at], axis=0)
            s = jnp.dot(keys, qt, preferred_element_type=jnp.float32)
            if i == 0:
                key_row = lax.broadcasted_iota(jnp.int32, s.shape, 0)
                query_row = lax.broadcasted_iota(jnp.int32, s.shape, 1) % half + core * half
                s = jnp.where((key_row <= query_row) | (key_row >= BLOCK), s, masked_score)
            p = jnp.exp2(s).astype(jnp.bfloat16)
            values = jnp.concatenate([vt_ref[s] for s in at], axis=1)
            acc = acc + jnp.dot(values, p, preferred_element_type=jnp.float32)
        att = (acc[:width] / acc[width : width + 1]).astype(jnp.bfloat16).T
        out = []
        for h in range(0, 2 * heads, 2):
            two = jnp.concatenate([att[h * half : (h + 1) * half], att[(h + 1) * half : (h + 2) * half]], axis=1)
            out.append(
                lax.dot_general(two, bd_ref[h // 2], (((1,), (1,)), ((), ())), preferred_element_type=jnp.float32)
            )
        return jnp.concatenate(out, axis=1).astype(jnp.bfloat16)

    pairs = blocks // 2

    def heads_to(b, i):
        part = ho_ref.at[x, b]
        return send(part, part, (h_s.at[0], h_r.at[b // 2]), at_tp(same_core((2, 1, -1)[i])))

    def finish(g):
        arrived(ho_ref.at[pl.ds(0, xs - 1), pl.ds(0, 2)], h_r.at[g])
        total = jnp.zeros((BLOCK, 2 * cols), jnp.float32)
        for p in range(xs):
            rows = ho_ref[p, pl.ds(2 * g, 2)].reshape(BLOCK, 2 * cols)
            w = jnp.concatenate([wc_ref[2 * p + c].reshape(RING * wrows, 2 * cols) for c in range(2)], axis=0)
            total = total + jnp.dot(rows, w, preferred_element_type=jnp.float32)
        left, right = total[:, :cols], total[:, cols:]
        px_ref[g] = jnp.where(core == 0, right, left)
        proj_ref[g, core] = jnp.where(core == 0, left, right)
        squares = jnp.sum(total * total, axis=1, keepdims=True)
        ss_ref[tp, pl.ds(g, 1), :] = jnp.broadcast_to(squares, (BLOCK, BLOCK)).T[0:1]
        swap(g).start()

    def swap(g):
        return send(px_ref.at[g], proj_ref.at[g, core], (p_s.at[0], p_r.at[0]), at_tp(sib))

    @pl.loop(0, blocks)
    def _(b):
        ho_ref[x, b] = attend_block(b)
        for i in range(3):
            heads_to(b, i).start()

    arrived(wc_ref.at[:, pl.ds(0, RING - 1)], y_r.at[0])
    for g in range(pairs):
        finish(g)

    def sums(d):
        return send(ss_ref.at[tp], ss_ref.at[tp], (s_s.at[0], s_r.at[0]), at_tp(other_tp(d)))

    for d in range(1, tp_n):
        sums(d).start()

    for j in range(xs):
        arrived(tk_ref.at[pl.ds(0, len(beside) if j else tp_n - 1), 0], t_s.at[j])
    arrived(tk_ref.at[pl.ds(0, 2), pl.ds(0, xs - 1)], tf_s.at[0])
    for n in range(1, kv_n):

        @pl.when(kv == n)
        def _(n=n):
            arrived(chs_ref.at[pl.ds(0, n)], ch_s.at[0])

    arrived(wc_ref.at[pl.ds(0, tp_n - 1), 0], w_s.at[0])
    arrived(wc_ref.at[:, pl.ds(0, RING - 1)], y_s.at[0])
    for n in range(1, kv_n):

        @pl.when(kv == kv_n - 1 - n)
        def _(n=n):
            arrived(out_ref.at[pl.ds(0, n)], b_s.at[0])

    def drain(remote):
        arrived(kvp_ref.at[pl.ds(0, 7), pl.ds(0, blocks)], k_s.at[0])
        for g, (a, b) in enumerate(remote):

            @pl.when(kv >= a)
            def _(g=g, a=a, b=b):
                part = pl.ds(blocks + (a - 1) * PER_OWNER, (b - a) * PER_OWNER)
                arrived(kvp_ref.at[pl.ds(0, 7), part], k_s.at[g + 1])

    for low, high, spans in plans:

        @pl.when((kv >= low) & (kv < high))
        def _(spans=spans):
            drain(spans)

    arrived(ho_ref.at[pl.ds(0, xs - 1)], h_s.at[0])
    arrived(px_ref, p_s.at[0])
    arrived(ss_ref.at[pl.ds(0, tp_n - 1)], s_s.at[0])
    arrived(px_ref, p_r.at[0])
    arrived(ss_ref.at[pl.ds(0, tp_n - 1)], s_r.at[0])
    gains = ogain_ref[:, pl.ds(pl.multiple_of(tp * cols, cols), cols)]
    inverse = []
    for c in range(2):
        total = ss_ref[c]
        for p in range(1, xs):
            total = total + ss_ref[2 * p + c]
        inverse.append(lax.rsqrt(total / (cols * tp_n) + epsilon))

    for g in range(pairs):
        for c in range(2):
            scale = jnp.broadcast_to(inverse[c][g : g + 1], (BLOCK, BLOCK)).T
            scale = jnp.concatenate([scale] * (cols // BLOCK), axis=1)
            rows = (proj_ref[g, c] * scale * gains).astype(jnp.bfloat16)
            for u in range(2):
                o_ref[pl.ds((2 * g + u) * BLOCK + c * half, half), :] = rows[u * half : (u + 1) * half]


def on_device(
    tokens,
    query_weight,
    latent_weight,
    query_gain,
    key_gain,
    value_up,
    out_weight,
    out_gain,
    chosen,
):
    toks, feat = tokens.shape
    width = latent_weight.shape[1]
    heads = query_weight.shape[1] // width
    blocks = toks // BLOCK
    kv_n, tp_n = lax.axis_size("kv"), lax.axis_size("tp")
    cols = out_weight.shape[1] // tp_n
    hv = out_weight.shape[0]
    xs = tp_n // 2
    piece = BLOCK // tp_n
    slots = blocks + (kv_n - 1) * PER_OWNER
    halves = max(1, kv_n * blocks // LANES)
    near = max(len(spans) for _, _, spans in owner_groups(kv_n))
    count = near + 1
    bf, f32, i32 = jnp.bfloat16, jnp.float32, jnp.int32
    dma = pltpu.SemaphoreType.DMA
    vmem = pl.BlockSpec(memory_space=pltpu.VMEM)
    sems = [
        xs, 1, xs, xs, 2, 2, 1, 1, 1, near, count, count, count, count,
        1, 1, 1, 1, 1, blocks // 2, 1, 1, 1, 1,
    ]
    return pl.pallas_call(
        functools.partial(kernel, kv_n, tp_n),
        out_shape=jax.ShapeDtypeStruct((toks, cols), bf),
        in_specs=[pl.BlockSpec(memory_space=pltpu.HBM)] * 9,
        out_specs=vmem,
        scratch_shapes=[
            pltpu.VMEM(chosen.shape, i32),
            pltpu.SMEM(chosen.shape, i32),
            pltpu.VMEM((blocks, 2, xs, piece, feat), bf),
            pltpu.VMEM(latent_weight.shape, bf),
            pltpu.VMEM(query_weight.shape, bf),
            pltpu.VMEM((value_up.shape[0], value_up.shape[2], value_up.shape[1]), bf),
            pltpu.VMEM(out_weight.shape, bf),
            pltpu.VMEM((1, width), f32),
            pltpu.VMEM((1, width), f32),
            pltpu.VMEM((1, cols * tp_n), f32),
            pltpu.VMEM((tp_n, xs, blocks, piece, feat), bf),
            pltpu.VMEM(query_weight.shape, bf),
            pltpu.VMEM((value_up.shape[0], value_up.shape[2], value_up.shape[1]), bf),
            pltpu.VMEM((2 * heads, xs, blocks, piece, width), bf),
            pltpu.VMEM((blocks, piece, width), bf),
            pltpu.VMEM((kv_n - 1, PER_OWNER, piece, width), bf),
            pltpu.VMEM((tp_n, slots, piece, width), bf),
            pltpu.VMEM((slots + 1, BLOCK, width), bf),
            pltpu.VMEM((slots + 1, width + ONES, BLOCK), bf),
            pltpu.VMEM((2, hv, 2 * width), bf),
            pltpu.VMEM((halves, 1, LANES), i32),
            pltpu.VMEM((halves, 1, LANES), i32),
            pltpu.VMEM((kv_n - 1, 1, LANES), i32),
            pltpu.SMEM((halves, 1, LANES), i32),
            pltpu.SMEM((kv_n - 1, 1, LANES), i32),
            pltpu.VMEM((xs, blocks, BLOCK // 2, 2 * hv), bf),
            pltpu.VMEM((tp_n, RING, hv // RING, 2 * cols), bf),
            pltpu.VMEM((blocks // 2, 2, BLOCK, cols), f32),
            pltpu.VMEM((blocks // 2, BLOCK, cols), f32),
            pltpu.VMEM((tp_n, blocks // 2, BLOCK), f32),
            dma((10,)), dma((2,)), *[dma((n,)) for n in sems],
        ],
        compiler_params=pltpu.CompilerParams(
            collective_id=0, has_side_effects=True, vmem_limit_bytes=24 << 20
        ),
    )(*[
        pltpu.with_memory_space_constraint(a, pltpu.HBM)
        for a in (
            tokens.reshape(blocks, 2, xs, piece, feat), query_weight, latent_weight, query_gain[None, :],
            key_gain[None, :], jnp.swapaxes(value_up, 1, 2), out_weight, out_gain[None, :], chosen,
        )
    ])


def solution(mesh):
    in_specs = (
        P("kv", "tp"),
        P(None, "tp"),
        P(),
        P(),
        P(),
        P("tp", None, None),
        P("tp", None),
        P(),
        P("kv", None),
    )
    out_specs = P("kv", "tp")
    return jax.shard_map(
        on_device, mesh=mesh, in_specs=in_specs, out_specs=out_specs, check_vma=False
    )
```
